256 devices in a mesh: ep: 16 (over y, x), tp: 16 (over z, core).
Axes of the slice: x: 4, y: 4, z: 8, core: 2. Of those that a mesh axis runs over, the one named last changes fastest.
Arguments:
- tokens: bfloat16 [512, 4096], P('ep'), may hold values from -6 to 6
- state_matrix: float32 [512, 16, 128, 128], P('ep', 'tp'), may hold values from -1.5 to 1.5
- state_norm: float32 [512, 16, 128], P('ep', 'tp'), may hold values from -4 to 4
- state_max: float32 [512, 16], P('ep', 'tp'), may hold values from -5 to 5
- mixer_gain: float32 [4096], replicated, may hold values from 0.1 to 1.9
- w_query: bfloat16 [4096, 2048], P('ep', 'tp'), may hold values from -0.09375 to 0.09375
- w_key: bfloat16 [4096, 2048], P('ep', 'tp'), may hold values from -0.09375 to 0.09375
- w_value: bfloat16 [4096, 2048], P('ep', 'tp'), may hold values from -0.09375 to 0.09375
- w_outgate: bfloat16 [4096, 2048], P('ep', 'tp'), may hold values from -0.09375 to 0.09375
- w_ingate: bfloat16 [4096, 16], replicated, may hold values from -0.09375 to 0.09375
- w_forget: bfloat16 [4096, 16], replicated, may hold values from -0.09375 to 0.09375
- forget_bias: float32 [16], replicated, may hold values from -2 to 4
- w_proj: bfloat16 [2048, 4096], P('tp', 'ep'), may hold values from -0.125 to 0.125
- ffn_gain: float32 [4096], replicated, may hold values from 0.1 to 1.9
- w_branch: bfloat16 [4096], replicated, may hold values from -0.09375 to 0.09375
- routes: int32 [512, 2], P('ep'), may hold values from 0 to 15, all different within a row; in each aligned block of 32 rows (0 to 31, 32 to 63, ...) at most 6 rows name the same one
- route_weight: float32 [512, 2], P('ep'), may hold values from 0.2 to 1
- expert_gate: bfloat16 [16, 4096, 4096], P('ep', None, 'tp'), may hold values from -0.09375 to 0.09375
- expert_up: bfloat16 [16, 4096, 4096], P('ep', None, 'tp'), may hold values from -0.09375 to 0.09375
- expert_down: bfloat16 [16, 4096, 4096], P('ep', 'tp'), may hold values from -0.09375 to 0.09375
- dense_gate: bfloat16 [4096, 8192], P('ep', 'tp'), may hold values from -0.09375 to 0.09375
- dense_up: bfloat16 [4096, 8192], P('ep', 'tp'), may hold values from -0.09375 to 0.09375
- dense_down: bfloat16 [8192, 4096], P('tp', 'ep'), may hold values from -0.0625 to 0.0625
Outputs:
- layer_out: bfloat16 [512, 4096], P('ep')
- new_matrix: float32 [512, 16, 128, 128], P('ep', 'tp')
- new_norm: float32 [512, 16, 128], P('ep', 'tp')
- new_max: float32 [512, 16], P('ep', 'tp')
The draws below stay inside these ranges and needn't reach their ends.
Inputs may be any that keep to these rules, and one draw needn't show every extreme that they name: `routes`: each row names 2 different experts. Among the rows of one index of ep (32 sequences) no expert is named more than 6 times, and in some such group one expert is named exactly 6 times.
All inputs are finite; a program needn't handle non-finite values.
Results may differ from the reference program's by a relative error of at most 0.012.
Values may be sent and summed in bfloat16 or wider, within the bound.
A program may use at most 64 MiB of HBM per device.

```python
import math
import jax
import jax.numpy as jnp
import numpy as np
from jax import lax

D = 4096
HEADS = 16
HDIM = 128
MW = 2048
FFD = 8192
FFE = 4096
TOPK = 2
SEQS = 32
BATCH = 512
EXPERTS = 16
CAP = 6
N_EP = 16


def shard_levels(stream_key, shape, pieces, low, high):
    def one(axis_at, parts):
        draws = jax.random.uniform(jax.random.fold_in(jax.random.fold_in(stream_key, 6), axis_at), (parts,), jnp.float32, low / len(pieces), high / len(pieces))
        return jnp.repeat(jnp.exp(draws), shape[axis_at] // parts).reshape((-1,) + (1,) * (len(shape) - axis_at - 1))

    level = one(*pieces[0])
    for cut in pieces[1:]:
        level = level * one(*cut)
    return level


def shared_out(key, own, number, rows, amount, top, limit, slope):
    ranking = jax.random.permutation(key, amount)
    crowded, usual = load_shares(amount, rows * top, limit, slope, True), load_shares(amount, rows * top, limit, slope, False)
    places = jnp.arange(amount)

    def named(lengths, turn):
        used = int((lengths > 0).sum())
        fixed = max(1, used // 4)
        shifted = fixed + (places - fixed + turn * (used - fixed)) % max(1, amount - fixed)
        return jnp.zeros((amount,), jnp.int32).at[ranking[jnp.where(places < fixed, places, shifted)]].set(jnp.asarray(lengths, jnp.int32))

    lengths = jnp.where(number % 4 == 0, named(crowded, number // 4), named(usual, number - number // 4 - 1))
    mixed = jax.random.permutation(jax.random.fold_in(own, 3), amount)
    giver, receiver = mixed[0:amount // 2 * 2:2], mixed[1:amount // 2 * 2:2]
    slack = jnp.minimum(lengths[giver] - 1, limit - lengths[receiver]) // 2
    slack = jnp.where((giver == ranking[0]) | (receiver == ranking[0]) | (lengths[receiver] == 0), 0, jnp.maximum(slack, 0))
    shifted = jax.random.randint(jax.random.fold_in(own, 4), (amount // 2,), 0, 1 << 20) % (slack + 1)
    lengths = lengths.at[giver].add(-shifted).at[receiver].add(shifted)
    members = jnp.searchsorted(jnp.cumsum(lengths), jnp.arange(rows * top), side="right").astype(jnp.int32)
    grid = members.reshape(top, rows).T
    grid = grid[jax.random.permutation(jax.random.fold_in(own, 1), rows)]
    turn = jax.random.randint(jax.random.fold_in(own, 2), (rows, 1), 0, top)
    return jnp.take_along_axis(grid, (jnp.arange(top)[None, :] + turn) % top, axis=1)


def load_shares(number_of, total, limit, lean, full):
    portions = [(1 << 20) // math.isqrt(standing ** lean) + 1 for standing in range(1, number_of + 1)]
    largest = limit if full else min(limit, max(-(-total // number_of), total * portions[0] // sum(portions)))
    least = 1 if total - largest >= number_of - 1 else 0
    given, surplus = [largest] + [least] * (number_of - 1), total - largest - least * (number_of - 1)
    while surplus > 0:
        movable = [i for i in range(1, number_of) if given[i] < largest] or [i for i in range(1, number_of) if given[i] < limit]
        pool, left = sum([portions[i] for i in movable]), surplus
        for i in movable:
            addition = min(limit - given[i], max(1, left * portions[i] // pool), surplus)
            given[i] = given[i] + addition
            surplus = surplus - addition
    return np.array(given)


def bell_draw(stream_key, extent, spread, reach, pieces=(), held_as=jnp.bfloat16):
    result = spread * jax.random.normal(stream_key, extent, jnp.float32)
    if pieces:
        result = result * shard_levels(stream_key, extent, pieces, -0.22, 0.18)
    return jnp.clip(result, -reach, reach).astype(held_as)


def setup_inputs(seed: int = 0) -> dict:
    key_of = jax.random.split(jax.random.key(seed), 24)
    tokens = bell_draw(key_of[0], (BATCH, D), 1.0, 6.0, ((0, 16),))
    state_matrix = bell_draw(key_of[1], (BATCH, HEADS, HDIM, HDIM), 0.1, 1.5, ((0, 16), (1, 16)), jnp.float32)
    state_norm = bell_draw(key_of[2], (BATCH, HEADS, HDIM), 0.3, 4.0, ((0, 16), (1, 16)), jnp.float32)
    state_max = bell_draw(key_of[3], (BATCH, HEADS), 1.0, 5.0, ((0, 16), (1, 16)), jnp.float32)
    mixer_gain = jnp.clip(1.0 + 0.18 * jax.random.normal(key_of[4], (D,), jnp.float32), 0.1, 1.9)
    w_query = bell_draw(key_of[5], (D, MW), D ** -0.5, 0.09375, ((0, 16), (1, 16)))
    w_key = bell_draw(key_of[6], (D, MW), D ** -0.5, 0.09375, ((0, 16), (1, 16)))
    w_value = bell_draw(key_of[7], (D, MW), D ** -0.5, 0.09375, ((0, 16), (1, 16)))
    w_outgate = bell_draw(key_of[8], (D, MW), D ** -0.5, 0.09375, ((0, 16), (1, 16)))
    w_ingate = bell_draw(key_of[9], (D, HEADS), D ** -0.5, 0.09375)
    w_forget = bell_draw(key_of[10], (D, HEADS), D ** -0.5, 0.09375)
    forget_bias = jnp.clip(jax.random.uniform(key_of[11], (HEADS,), jnp.float32, -2.0, 4.0), -2.0, 4.0)
    w_proj = bell_draw(key_of[12], (MW, D), MW ** -0.5, 0.125, ((0, 16), (1, 16)))
    ffn_gain = jnp.clip(1.0 + 0.18 * jax.random.normal(key_of[13], (D,), jnp.float32), 0.1, 1.9)
    w_branch = bell_draw(key_of[14], (D,), D ** -0.5, 0.09375)
    routes_keys = jax.random.split(jax.random.fold_in(key_of[15], 1), BATCH // SEQS)
    routes_turns = jax.random.permutation(jax.random.fold_in(key_of[15], 3), BATCH // SEQS)
    routes = jax.vmap(lambda own, number: shared_out(jax.random.fold_in(key_of[15], 2), own, number, SEQS, EXPERTS, TOPK, CAP, 2))(routes_keys, routes_turns).reshape((BATCH, TOPK))
    route_weight = jnp.clip(jnp.exp(math.log(1.0) - 1.609438 * jax.random.uniform(key_of[16], (BATCH, TOPK), jnp.float32) ** shard_levels(key_of[16], (BATCH, TOPK), ((0, 16),), -0.2, 0.2)), 0.2, 1.0)
    expert_gate = bell_draw(key_of[17], (EXPERTS, D, FFE), D ** -0.5, 0.09375, ((0, 16), (2, 16)))
    expert_up = bell_draw(key_of[18], (EXPERTS, D, FFE), D ** -0.5, 0.09375, ((0, 16), (2, 16)))
    expert_down = bell_draw(key_of[19], (EXPERTS, FFE, D), FFE ** -0.5, 0.09375, ((0, 16), (1, 16)))
    dense_gate = bell_draw(key_of[20], (D, FFD), D ** -0.5, 0.09375, ((0, 16), (1, 16)))
    dense_up = bell_draw(key_of[21], (D, FFD), D ** -0.5, 0.09375, ((0, 16), (1, 16)))
    dense_down = bell_draw(key_of[22], (FFD, D), FFD ** -0.5, 0.0625, ((0, 16), (1, 16)))
    return dict(tokens=tokens, state_matrix=state_matrix, state_norm=state_norm, state_max=state_max, mixer_gain=mixer_gain, w_query=w_query, w_key=w_key, w_value=w_value, w_outgate=w_outgate, w_ingate=w_ingate, w_forget=w_forget, forget_bias=forget_bias, w_proj=w_proj, ffn_gain=ffn_gain, w_branch=w_branch, routes=routes, route_weight=route_weight, expert_gate=expert_gate, expert_up=expert_up, expert_down=expert_down, dense_gate=dense_gate, dense_up=dense_up, dense_down=dense_down)


EPS = 1e-06

def rms_scale(values, gain):
    wide = values.astype(jnp.float32)
    return wide * lax.rsqrt(lax.optimization_barrier(jnp.mean(wide * wide, axis=-1, keepdims=True)) + EPS) * gain.astype(jnp.float32)

def slot_numbers(flat_routes, experts_all):
    onehot = (flat_routes[:, None] == jnp.arange(experts_all, dtype=jnp.int32)[None, :]).astype(jnp.int32)
    before = jnp.cumsum(onehot, axis=0) - onehot
    return lax.optimization_barrier(jnp.sum(before * onehot, axis=1)).astype(jnp.int32)

def memory_step(query_all, key_all, value_all, outgate, gate_in, gate_forget, state_matrix, state_norm, state_max):
    row_count, head_count = gate_in.shape
    head_size = state_matrix.shape[-1]
    heads_q = query_all.reshape(row_count, head_count, head_size)
    heads_k = key_all.reshape(row_count, head_count, head_size) * head_size ** (-0.5)
    heads_v = value_all.reshape(row_count, head_count, head_size)
    log_keep = jax.nn.log_sigmoid(gate_forget)
    new_max = jnp.maximum(log_keep + state_max, gate_in)
    keep_factor = jnp.exp(log_keep + state_max - new_max)
    write_factor = jnp.exp(gate_in - new_max)
    new_matrix = keep_factor[:, :, None, None] * state_matrix + write_factor[:, :, None, None] * heads_k[:, :, :, None] * heads_v[:, :, None, :]
    new_norm = keep_factor[:, :, None] * state_norm + write_factor[:, :, None] * heads_k
    numer = jnp.einsum('bhk,bhkv->bhv', heads_q, new_matrix, precision=lax.Precision.HIGHEST)
    denom = lax.optimization_barrier(jnp.sum(heads_q * new_norm, axis=-1))
    cell = numer / jnp.maximum(jnp.abs(denom), 1.0)[:, :, None]
    gated = jax.nn.sigmoid(outgate.reshape(row_count, head_count, head_size)) * cell
    mixed_heads = gated.reshape(row_count, head_count * head_size).astype(jnp.bfloat16)
    return (mixed_heads, new_matrix, new_norm, new_max)

def reference(tokens, state_matrix, state_norm, state_max, mixer_gain, w_query, w_key, w_value, w_outgate, w_ingate, w_forget, forget_bias, w_proj, ffn_gain, w_branch, routes, route_weight, expert_gate, expert_up, expert_down, dense_gate, dense_up, dense_down):
    normed = rms_scale(tokens, mixer_gain).astype(jnp.bfloat16)
    query_all = jnp.dot(normed, w_query, preferred_element_type=jnp.float32)
    key_all = jnp.dot(normed, w_key, preferred_element_type=jnp.float32)
    value_all = jnp.dot(normed, w_value, preferred_element_type=jnp.float32)
    outgate = jnp.dot(normed, w_outgate, preferred_element_type=jnp.float32)
    gate_in = jnp.dot(normed, w_ingate, preferred_element_type=jnp.float32)
    gate_forget = jnp.dot(normed, w_forget, preferred_element_type=jnp.float32) + forget_bias
    mixed_heads, new_matrix, new_norm, new_max = memory_step(query_all, key_all, value_all, outgate, gate_in, gate_forget, state_matrix, state_norm, state_max)
    mixer_out = jnp.dot(mixed_heads, w_proj, preferred_element_type=jnp.float32)
    residual = (tokens.astype(jnp.float32) + mixer_out).astype(jnp.bfloat16)
    ffn_in = rms_scale(residual, ffn_gain).astype(jnp.bfloat16)
    branch_share = jax.nn.sigmoid(jnp.dot(ffn_in, w_branch, preferred_element_type=jnp.float32))
    dense_hidden = (jax.nn.silu(jnp.dot(ffn_in, dense_gate, preferred_element_type=jnp.float32)) * jnp.dot(ffn_in, dense_up, preferred_element_type=jnp.float32)).astype(jnp.bfloat16)
    dense_out = jnp.dot(dense_hidden, dense_down, preferred_element_type=jnp.float32)
    group_routes = routes.reshape(N_EP, SEQS * TOPK)
    slots = jax.vmap(lambda group_row: slot_numbers(group_row, EXPERTS))(group_routes)
    group_ids = jnp.broadcast_to(jnp.arange(N_EP, dtype=jnp.int32)[:, None], group_routes.shape)
    repeated = jnp.repeat(ffn_in, TOPK, axis=0).reshape(N_EP, SEQS * TOPK, D)
    buffers = jnp.zeros((EXPERTS, N_EP, CAP, D), jnp.bfloat16).at[group_routes, group_ids, slots].set(repeated)

    def one_expert(index):
        rows_in = buffers[index].reshape(N_EP * CAP, D)
        hidden = (jax.nn.silu(jnp.dot(rows_in, expert_gate[index], preferred_element_type=jnp.float32)) * jnp.dot(rows_in, expert_up[index], preferred_element_type=jnp.float32)).astype(jnp.bfloat16)
        return jnp.dot(hidden, expert_down[index], preferred_element_type=jnp.float32).reshape(N_EP, CAP, D)
    results = lax.map(one_expert, jnp.arange(EXPERTS, dtype=jnp.int32))
    picked = results[group_routes, group_ids, slots].reshape(N_EP * SEQS, TOPK, D)
    shares = route_weight / lax.optimization_barrier(jnp.sum(route_weight, axis=1, keepdims=True))
    expert_rows = lax.optimization_barrier(jnp.sum(shares[:, :, None] * picked, axis=1))
    total_ffn = expert_rows + branch_share[:, None] * dense_out
    layer_out = (residual.astype(jnp.float32) + total_ffn).astype(jnp.bfloat16)
    return (layer_out, new_matrix, new_norm, new_max)
```

```python
import functools

import jax
import jax.numpy as jnp
from jax import lax
from jax.experimental import pallas as pl
from jax.experimental.pallas import tpu as pltpu
from jax.sharding import PartitionSpec as P

EPS = 1e-06
MESH = pl.DeviceIdType.MESH
CAP = 6
SLOT = 8
F32 = jnp.float32
BF16 = jnp.bfloat16
HIGHEST = lax.Precision.HIGHEST
NT = (((1,), (1,)), ((), ()))


def iota(shape, dim):
    return lax.broadcasted_iota(jnp.int32, shape, dim)


def to_column(row, rows):
    diag = iota((rows, row.shape[1]), 0) == iota((rows, row.shape[1]), 1)
    return jnp.sum(jnp.where(diag, row, 0.0), axis=1, keepdims=True)


def to_row(column, lanes):
    rows = column.shape[0]
    diag = iota((rows, lanes), 0) == iota((rows, lanes), 1)
    return jnp.sum(jnp.where(diag, column, 0.0), axis=0, keepdims=True)


TOK, KEY, QKV, MIX, PRJ, RES, ROW, STA, DEN, HID, DWN, EXP, RET, OUT = range(14)
PHASES = 14


def layer_kernel(
    n,
    tok_h, sm_h, sn_h, smax_h, mgain_h, wq_h, wk_h, wv_h, wo_h, win_h, wfo_h, fbias_h,
    wproj_h, fgain_h, wbr_h, routes_h, rw_h, eg_h, eu_h, ed_h, dg_h, du_h, dd_h,
    out_h, nm_h, nn_h, nmax_h,
    tok, sm, sn, smax, mgain, wqkv, wgates, fbias, wproj, fgain, wbr, routes, rw,
    eg, eu, ed, dgu, dd,
    tok_all, key_all, qkv_part, qkv_in, mix_all, prj_part, prj_in, res_all,
    row_out, row_in, sta_out, sta_in, den_part, den_in, hid_all, dwn_part, dwn_in,
    exp_part, exp_in, ret_out, ret_in, fin_out, fin_in, out_own,
    nm, nn, nmax, pick, gu_acc, gates, wkt, qt, vrow, keep_rows, numer, ret_w,
    load_sem, send_sem, recv_sem, fin_sem, store_sem, out_sem,
):
    me_e, me_t = lax.axis_index("ep"), lax.axis_index("tp")
    rows = tok.shape[0]
    width = tok.shape[1]
    block = width // n
    head = sn.shape[1]
    hid_e = eg.shape[1]
    hid_d = dd.shape[0]
    cap_rows = CAP * n

    loads = [
        (tok_h, tok), (mgain_h, mgain), (fgain_h, fgain), (wbr_h, wbr), (routes_h, routes),
        (rw_h, rw), (win_h, wgates.at[pl.ds(0, n), :]), (wfo_h, wgates.at[pl.ds(n, n), :]),
        (fbias_h, fbias), (smax_h, smax), (sn_h, sn),
        (wq_h, wqkv.at[:, pl.ds(0, head)]), (wk_h, wqkv.at[:, pl.ds(head, head)]),
        (wv_h, wqkv.at[:, pl.ds(2 * head, head)]), (wo_h, wqkv.at[:, pl.ds(3 * head, head)]),
        (sm_h, sm), (wproj_h, wproj), (dg_h, dgu.at[:, pl.ds(0, hid_d)]),
        (du_h, dgu.at[:, pl.ds(hid_d, hid_d)]), (eg_h, eg), (eu_h, eu), (ed_h, ed), (dd_h, dd),
    ]
    loads = [pltpu.make_async_copy(a, b, load_sem.at[k]) for k, (a, b) in enumerate(loads)]
    for copy in loads:
        copy.start()

    barrier = pltpu.get_barrier_semaphore()

    def greet(d, _):
        pl.semaphore_signal(barrier, 1, device_id=(lax.rem(me_e + d, n), me_t), device_id_type=MESH)
        pl.semaphore_signal(barrier, 1, device_id=(me_e, lax.rem(me_t + d, n)), device_id_type=MESH)
        return 0

    lax.fori_loop(1, n, greet, 0)

    @pl.when(me_e != me_t)
    def _():
        pl.semaphore_signal(barrier, 1, device_id=(me_t, me_e), device_id_type=MESH)

    @pl.when(me_e != me_t)
    def _():
        pl.semaphore_wait(barrier, 2 * n - 1)

    @pl.when(me_e == me_t)
    def _():
        pl.semaphore_wait(barrier, 2 * n - 2)

    def ep_copy(phase, src, dst, peer, landing):
        return pltpu.make_async_remote_copy(
            src_ref=src, dst_ref=dst, send_sem=send_sem.at[phase],
            recv_sem=recv_sem.at[phase, landing], device_id=(peer, me_t), device_id_type=MESH)

    def tp_copy(phase, src, dst, peer, landing):
        return pltpu.make_async_remote_copy(
            src_ref=src, dst_ref=dst, send_sem=send_sem.at[phase],
            recv_sem=recv_sem.at[phase, landing], device_id=(me_e, peer), device_id_type=MESH)

    def to_peers(copy, me, phase, src_of, dst):
        def one(d, _):
            peer = lax.rem(me + d, n)
            copy(phase, src_of(peer), dst, peer, me).start()
            return 0

        lax.fori_loop(1, n, one, 0)

    def await_peers(copy, me, phase, buffer, use=None, carry=0):
        def one(d, carry):
            peer = lax.rem(me + n - d, n)
            copy(phase, buffer.at[peer], buffer.at[peer], peer, peer).wait_recv()
            return carry if use is None else use(peer, carry)

        return lax.fori_loop(1, n, one, carry)

    def sent(copy, phase, many):
        copy(phase, many, many, 0, 0).wait_send()

    loads[0].wait()
    to_peers(ep_copy, me_e, TOK,
             lambda peer: tok.at[:, pl.ds(pl.multiple_of(peer * block, block), block)],
             tok_all.at[me_e])
    tok_all[me_e] = tok[:, pl.ds(pl.multiple_of(me_e * block, block), block)]

    loads[4].wait()
    loads[5].wait()
    route_rows = [routes[pl.ds(k, 1), :] for k in range(2)]
    lanes_e = iota((128, rows), 0)
    named = sum(jnp.where(lanes_e == r, 1.0, 0.0) for r in route_rows)
    earlier = jnp.where(iota((rows, rows), 0) < iota((rows, rows), 1), 1.0, 0.0)
    before = jnp.dot(named.astype(BF16), earlier.astype(BF16), preferred_element_type=F32)
    base = (CAP * me_e).astype(F32)
    key = jnp.where(named > 0.0, before + base, -1.0)
    eye = jnp.where(iota((rows, rows), 0) == iota((rows, rows), 1), 1.0, 0.0)
    key_all[me_e] = lax.dot_general(
        eye.astype(BF16), key.astype(BF16), NT, preferred_element_type=F32).astype(BF16)
    to_peers(ep_copy, me_e, KEY, lambda peer: key_all.at[me_e], key_all.at[me_e])
    weights = [rw[pl.ds(k, 1), :] for k in range(2)]
    total = weights[0] + weights[1]
    spots = iota((n * SLOT, rows), 0)
    share_t = jnp.zeros((n * SLOT, rows), F32)
    for r, w in zip(route_rows, weights):
        slot = jnp.sum(jnp.where(lanes_e == r, before, 0.0), axis=0, keepdims=True)
        hit = (spots.astype(F32) == r.astype(F32) * SLOT + slot)
        share_t = share_t + jnp.where(hit, w / total, 0.0)
    ret_w[...] = lax.dot_general(eye, share_t, NT, precision=HIGHEST, preferred_element_type=F32)

    loads[1].wait()
    squares = jnp.zeros((rows, block), F32)
    for k in range(n):
        part = tok[:, k * block:(k + 1) * block].astype(F32)
        squares = squares + part * part
    scale = lax.rsqrt(jnp.sum(squares, axis=1, keepdims=True) / width + EPS)
    loads[6].wait()
    loads[7].wait()
    gate = jnp.zeros((rows, 2 * n), F32)
    for k in range(n):
        cols = slice(k * block, (k + 1) * block)
        gain = mgain[:, cols]
        normed = (tok[:, cols].astype(F32) * scale * gain).astype(BF16)
        gate = gate + lax.dot_general(normed, wgates[:, cols], NT, preferred_element_type=F32)
    for k in range(8, 11):
        loads[k].wait()
    lane = iota((rows, 2 * n), 1)
    gate_in = jnp.sum(jnp.where(lane == me_t, gate, 0.0), axis=1, keepdims=True)
    gate_forget = jnp.sum(jnp.where(lane == me_t + n, gate, 0.0), axis=1, keepdims=True)
    bias = jnp.sum(jnp.where(iota((1, n), 1) == me_t, fbias[...], 0.0), axis=1, keepdims=True)
    gate_forget = gate_forget + bias
    log_keep = jnp.minimum(gate_forget, 0.0) - jnp.log1p(jnp.exp(-jnp.abs(gate_forget)))
    old_max = to_column(smax[...], rows)
    new_max = jnp.maximum(log_keep + old_max, gate_in)
    keep = jnp.exp(log_keep + old_max - new_max)
    write = jnp.exp(gate_in - new_max)
    nmax[...] = to_row(new_max, rows)

    await_peers(ep_copy, me_e, TOK, tok_all)
    for k in range(11, 15):
        loads[k].wait()
    gain_m = mgain[:, pl.ds(pl.multiple_of(me_e * block, block), block)]
    group = 4
    big = group * rows

    def project(c, _):
        at = pl.multiple_of(c * group, group)
        x = tok_all[pl.ds(at, group)].reshape(big, block).astype(F32) * gain_m
        y = jnp.dot(x.astype(BF16), wqkv[...], preferred_element_type=F32)
        qkv_part[pl.ds(at, group)] = y.astype(BF16).reshape(group, rows, 4 * head)

        def one(k, _):
            peer = at + k

            @pl.when(peer != me_e)
            def _():
                ep_copy(QKV, qkv_part.at[peer], qkv_in.at[me_e], peer, me_e).start()

            return 0

        return lax.fori_loop(0, group, one, 0)

    lax.fori_loop(0, n // group, project, 0)

    loads[15].wait()
    y = await_peers(ep_copy, me_e, QKV, qkv_in,
                    lambda peer, acc: acc + qkv_in[peer].astype(F32),
                    qkv_part[me_e].astype(F32)) * scale
    query = y[:, :head]
    keys = y[:, head:2 * head] * head ** (-0.5)
    value = y[:, 2 * head:3 * head]
    outgate = y[:, 3 * head:]
    written = write * keys
    new_norm = keep * sn[...] + written
    nn[...] = new_norm
    denom = jnp.sum(query * new_norm, axis=1, keepdims=True)
    qt[...] = query.T
    wkt[...] = written.T
    vrow[...] = value
    keep_rows[...] = jnp.broadcast_to(keep, (rows, head))
    for b in range(rows):
        numer[pl.ds(b, 1), :] = jnp.sum(qt[:, b:b + 1] * sm[b], axis=0, keepdims=True)
    dots = jnp.sum(query * written, axis=1, keepdims=True)
    num = keep * numer[...] + dots * value
    cell = num / jnp.maximum(jnp.abs(denom), 1.0)
    mix_all[me_e] = (jax.nn.sigmoid(outgate) * cell).astype(BF16)
    to_peers(ep_copy, me_e, MIX, lambda peer: mix_all.at[me_e], mix_all.at[me_e])
    for b in range(rows):
        nm[b] = keep_rows[pl.ds(b, 1), :] * sm[b] + wkt[:, b:b + 1] * vrow[pl.ds(b, 1), :]
    stores = [
        pltpu.make_async_copy(a, b, store_sem.at[k])
        for k, (a, b) in enumerate([(nm, nm_h), (nn, nn_h), (nmax, nmax_h)])
    ]
    for copy in stores:
        copy.start()

    await_peers(ep_copy, me_e, KEY, key_all)
    key_t = lax.dot_general(
        jnp.where(iota((n, 128), 0) == iota((n, 128), 1), 1.0, 0.0).astype(BF16),
        key_all[...].reshape(n * rows, 128), NT, preferred_element_type=F32)
    places = iota((cap_rows, n * rows), 0).astype(F32)
    for e in range(n):
        pick[pl.ds(e * cap_rows, cap_rows), :] = jnp.where(
            places == key_t[e:e + 1, :], 1.0, 0.0).astype(BF16)

    await_peers(ep_copy, me_e, MIX, mix_all)
    loads[16].wait()
    y = jnp.dot(mix_all[...].reshape(n * rows, head), wproj[...], preferred_element_type=F32)
    prj_part[...] = y.astype(BF16).reshape(n, rows, block)
    to_peers(tp_copy, me_t, PRJ, lambda peer: prj_part.at[peer], prj_in.at[me_t])
    mixed = await_peers(tp_copy, me_t, PRJ, prj_in,
                        lambda peer, acc: acc + prj_in[peer].astype(F32),
                        prj_part[me_t].astype(F32))
    residual = (tok_all[me_t].astype(F32) + mixed).astype(BF16)
    res_all[me_t] = residual
    to_peers(tp_copy, me_t, RES, lambda peer: res_all.at[me_t], res_all.at[me_t])
    loads[2].wait()
    loads[3].wait()
    await_peers(tp_copy, me_t, RES, res_all)

    res_flat = res_all[...].reshape(n * rows, block)

    def dispatch(c, _):
        at = pl.multiple_of(c * group, group)
        y = jnp.dot(pick[pl.ds(pl.multiple_of(at * cap_rows, group * cap_rows), group * cap_rows), :],
                    res_flat, preferred_element_type=F32)
        row_out[pl.ds(at, group)] = y.astype(BF16).reshape(group, cap_rows, block)

        def one(k, _):
            peer = at + k

            @pl.when(peer != me_e)
            def _():
                ep_copy(ROW, row_out.at[peer], row_in.at[me_e], peer, me_e).start()

            return 0

        return lax.fori_loop(0, group, one, 0)

    lax.fori_loop(0, n // group, dispatch, 0)
    row_in[me_e] = row_out[me_e]

    mine = pl.multiple_of(me_e * block, block)
    gain_f = fgain[:, pl.ds(mine, block)]
    gain_b = gain_f * wbr[:, pl.ds(mine, block)].astype(F32)

    def stats(b, _):
        r = res_all[b].astype(F32)
        ss = to_row(jnp.sum(r * r, axis=1, keepdims=True), 128)
        br = to_row(jnp.sum(r * gain_b, axis=1, keepdims=True), 128)
        sta_out[b] = jnp.where(iota((8, 128), 0) == 0, ss, br)
        return 0

    lax.fori_loop(0, n, stats, 0)
    to_peers(ep_copy, me_e, STA, lambda peer: sta_out.at[peer], sta_in.at[me_e])
    loads[17].wait()
    loads[18].wait()

    def dense(c, _):
        at = pl.multiple_of(c * group, group)
        x = res_all[pl.ds(at, group)].reshape(big, block).astype(F32) * gain_f
        y = jnp.dot(x.astype(BF16), dgu[...], preferred_element_type=F32)
        den_part[pl.ds(at, group)] = y.astype(BF16).reshape(group, rows, 2 * hid_d)

        def one(k, _):
            peer = at + k

            @pl.when(peer != me_e)
            def _():
                ep_copy(DEN, den_part.at[peer], den_in.at[me_e], peer, me_e).start()

            return 0

        return lax.fori_loop(0, group, one, 0)

    lax.fori_loop(0, n // group, dense, 0)

    loads[19].wait()
    loads[20].wait()

    def expert_in(peer, ss):
        x = row_in[peer].astype(F32)
        at = pl.multiple_of(peer * block, block)
        xg = (x * fgain[:, pl.ds(at, block)]).astype(BF16)
        gu_acc[:, pl.ds(0, hid_e)] += jnp.dot(xg, eg[pl.ds(at, block), :], preferred_element_type=F32)
        gu_acc[:, pl.ds(hid_e, hid_e)] += jnp.dot(xg, eu[pl.ds(at, block), :], preferred_element_type=F32)
        return ss + jnp.sum(x * x, axis=1, keepdims=True)

    gu_acc[...] = jnp.zeros_like(gu_acc)
    ss = expert_in(me_e, jnp.zeros((cap_rows, 1), F32))
    ss = await_peers(ep_copy, me_e, ROW, row_in, expert_in, ss)
    row_scale = lax.rsqrt(ss / width + EPS)
    g = gu_acc[:, :hid_e] * row_scale
    u = gu_acc[:, hid_e:] * row_scale
    hidden = (g / (1.0 + jnp.exp(-g)) * u).astype(BF16)
    loads[21].wait()
    for k in range(n):
        exp_part[k] = jnp.dot(hidden, ed[:, k * block:(k + 1) * block],
                              preferred_element_type=F32).astype(BF16)
    to_peers(tp_copy, me_t, EXP, lambda peer: exp_part.at[peer], exp_in.at[me_t])

    sums = await_peers(ep_copy, me_e, STA, sta_in, lambda peer, acc: acc + sta_in[peer], sta_out[me_e])
    dense_scale = lax.rsqrt(to_column(sums[0:1, :], rows) / width + EPS)
    branch = jax.nn.sigmoid(to_column(sums[1:2, :], rows) * dense_scale)
    y = await_peers(ep_copy, me_e, DEN, den_in,
                    lambda peer, acc: acc + den_in[peer].astype(F32),
                    den_part[me_e].astype(F32)) * dense_scale
    g, u = y[:, :hid_d], y[:, hid_d:]
    hid_all[me_e] = (g / (1.0 + jnp.exp(-g)) * u * branch).astype(BF16)
    to_peers(ep_copy, me_e, HID, lambda peer: hid_all.at[me_e], hid_all.at[me_e])

    y = await_peers(tp_copy, me_t, EXP, exp_in,
                    lambda peer, acc: acc + exp_in[peer].astype(F32),
                    exp_part[me_t].astype(F32))
    spot, col = iota((n * SLOT, cap_rows), 0), iota((n * SLOT, cap_rows), 1)
    within = jnp.bitwise_and(spot, SLOT - 1)
    source = CAP * jnp.right_shift(spot, SLOT.bit_length() - 1) + within
    spread = jnp.where((source == col) & (within < CAP), 1.0, 0.0).astype(BF16)
    ret_out[...] = jnp.dot(spread, y.astype(BF16), preferred_element_type=F32).reshape(n, SLOT, block)
    to_peers(ep_copy, me_e, RET, lambda peer: ret_out.at[peer], ret_in.at[me_e])
    ret_in[me_e] = ret_out[me_e]

    await_peers(ep_copy, me_e, HID, hid_all)
    loads[22].wait()
    y = jnp.dot(hid_all[...].reshape(n * rows, hid_d), dd[...], preferred_element_type=F32)
    dwn_part[...] = y.astype(BF16).reshape(n, rows, block)
    to_peers(tp_copy, me_t, DWN, lambda peer: dwn_part.at[peer], dwn_in.at[me_t])

    await_peers(ep_copy, me_e, RET, ret_in)
    routed = jnp.dot(ret_w[...], ret_in[...].reshape(n * SLOT, block), precision=HIGHEST,
                     preferred_element_type=F32)

    y = await_peers(tp_copy, me_t, DWN, dwn_in,
                    lambda peer, acc: acc + dwn_in[peer].astype(F32),
                    dwn_part[me_t].astype(F32))
    fin_out[...] = res_all[me_t].astype(F32) + y

    def crossing():
        return pltpu.make_async_remote_copy(
            src_ref=fin_out, dst_ref=fin_in, send_sem=fin_sem.at[0], recv_sem=fin_sem.at[1],
            device_id=(me_t, me_e), device_id_type=MESH)

    @pl.when(me_e != me_t)
    def _():
        crossing().start()
        crossing().wait()

    @pl.when(me_e == me_t)
    def _():
        fin_in[...] = fin_out[...]

    out_own[...] = (fin_in[...] + routed).astype(BF16)
    place = out_h.at[:, pl.ds(pl.multiple_of(me_t * block, block), block)]
    to_peers(tp_copy, me_t, OUT, lambda peer: out_own, place)
    own = pltpu.make_async_copy(out_own, place, out_sem)
    own.start()

    def landed(d, _):
        peer = lax.rem(me_t + n - d, n)
        spot = out_h.at[:, pl.ds(pl.multiple_of(peer * block, block), block)]
        tp_copy(OUT, out_own, spot, peer, peer).wait_recv()
        return 0

    lax.fori_loop(1, n, landed, 0)
    own.wait()
    for copy in stores:
        copy.wait()
    rest = pl.ds(0, n - 1)
    sent(ep_copy, TOK, tok_all.at[rest])
    sent(ep_copy, KEY, key_all.at[rest])
    sent(ep_copy, QKV, qkv_part.at[rest])
    sent(ep_copy, MIX, mix_all.at[rest])
    sent(tp_copy, PRJ, prj_part.at[rest])
    sent(tp_copy, RES, res_all.at[rest])
    sent(ep_copy, ROW, row_out.at[rest])
    sent(ep_copy, STA, sta_out.at[rest])
    sent(ep_copy, DEN, den_part.at[rest])
    sent(ep_copy, HID, hid_all.at[rest])
    sent(tp_copy, DWN, dwn_part.at[rest])
    sent(tp_copy, EXP, exp_part.at[rest])
    sent(ep_copy, RET, ret_out.at[rest])
    sent(tp_copy, OUT, res_all.at[rest])


def on_device(
    n, tokens, state_matrix, state_norm, state_max, mixer_gain, w_query, w_key, w_value, w_outgate,
    w_ingate, w_forget, forget_bias, w_proj, ffn_gain, w_branch, routes, route_weight,
    expert_gate, expert_up, expert_down, dense_gate, dense_up, dense_down,
):
    rows, width = tokens.shape
    head = state_norm.shape[-1]
    block = width // n
    hid_e, hid_d = expert_gate.shape[2], dense_gate.shape[1]
    cap_rows = CAP * n
    args = (
        tokens,
        state_matrix.reshape(rows, head, head),
        state_norm.reshape(rows, head),
        state_max.T,
        mixer_gain.reshape(1, width),
        w_query, w_key, w_value, w_outgate,
        w_ingate.T, w_forget.T,
        forget_bias.reshape(1, n),
        w_proj,
        ffn_gain.reshape(1, width),
        w_branch.reshape(1, width),
        routes.T, route_weight.T,
        expert_gate.reshape(width, hid_e), expert_up.reshape(width, hid_e),
        expert_down.reshape(hid_e, width),
        dense_gate, dense_up, dense_down,
    )
    vm = pltpu.VMEM
    dma = pltpu.SemaphoreType.DMA
    scratch = [
        vm((rows, width), BF16), vm((rows, head, head), F32), vm((rows, head), F32), vm((1, rows), F32),
        vm((1, width), F32), vm((block, 4 * head), BF16), vm((2 * n, width), BF16), vm((1, n), F32),
        vm((head, block), BF16), vm((1, width), F32), vm((1, width), BF16), vm((2, rows), jnp.int32),
        vm((2, rows), F32), vm((width, hid_e), BF16), vm((width, hid_e), BF16), vm((hid_e, width), BF16),
        vm((block, 2 * hid_d), BF16), vm((hid_d, block), BF16),
        vm((n, rows, block), BF16), vm((n, rows, 128), BF16),
        vm((n, rows, 4 * head), BF16), vm((n, rows, 4 * head), BF16),
        vm((n, rows, head), BF16), vm((n, rows, block), BF16), vm((n, rows, block), BF16),
        vm((n, rows, block), BF16),
        vm((n, cap_rows, block), BF16), vm((n, cap_rows, block), BF16),
        vm((n, 8, 128), F32), vm((n, 8, 128), F32),
        vm((n, rows, 2 * hid_d), BF16), vm((n, rows, 2 * hid_d), BF16),
        vm((n, rows, hid_d), BF16), vm((n, rows, block), BF16), vm((n, rows, block), BF16),
        vm((n, cap_rows, block), BF16), vm((n, cap_rows, block), BF16),
        vm((n, SLOT, block), F32), vm((n, SLOT, block), F32),
        vm((rows, block), F32), vm((rows, block), F32), vm((rows, block), BF16),
        vm((rows, head, head), F32), vm((rows, head), F32), vm((1, rows), F32),
        vm((n * cap_rows, n * rows), BF16), vm((cap_rows, 2 * hid_e), F32), vm((rows, 2 * n), F32),
        vm((head, rows), F32), vm((head, rows), F32), vm((rows, head), F32), vm((rows, head), F32),
        vm((rows, head), F32), vm((rows, n * SLOT), F32),
        dma((len(args),)), dma((PHASES,)), dma((PHASES, n)), dma((2,)), dma((3,)), dma,
    ]
    any_space = pl.BlockSpec(memory_space=pl.ANY)
    out, new_matrix, new_norm, new_max = pl.pallas_call(
        functools.partial(layer_kernel, n),
        out_shape=(
            jax.ShapeDtypeStruct((rows, width), BF16),
            jax.ShapeDtypeStruct((rows, head, head), F32),
            jax.ShapeDtypeStruct((rows, head), F32),
            jax.ShapeDtypeStruct((1, rows), F32),
        ),
        in_specs=[any_space] * len(args),
        out_specs=[any_space] * 4,
        scratch_shapes=scratch,
        compiler_params=pltpu.CompilerParams(
            collective_id=0, has_side_effects=True, vmem_limit_bytes=56 * 1024 * 1024),
        name="layer",
    )(*args)
    return (out, new_matrix.reshape(rows, 1, head, head), new_norm.reshape(rows, 1, head), new_max.T)


def solution(mesh):
    n = mesh.shape["ep"]
    in_specs = (
        P("ep", None),
        P("ep", "tp", None, None),
        P("ep", "tp", None),
        P("ep", "tp"),
        P(),
        P("ep", "tp"),
        P("ep", "tp"),
        P("ep", "tp"),
        P("ep", "tp"),
        P(),
        P(),
        P(),
        P("tp", "ep"),
        P(),
        P(),
        P("ep", None),
        P("ep", None),
        P("ep", None, "tp"),
        P("ep", None, "tp"),
        P("ep", "tp", None),
        P("ep", "tp"),
        P("ep", "tp"),
        P("tp", "ep"),
    )
    out_specs = (P("ep", None), P("ep", "tp", None, None), P("ep", "tp", None), P("ep", "tp"))
    return jax.shard_map(
        functools.partial(on_device, n), mesh=mesh, in_specs=in_specs, out_specs=out_specs,
        check_vma=False)
```

```python
import functools

import jax
import jax.numpy as jnp
from jax import lax
from jax.experimental import pallas as pl
from jax.experimental.pallas import tpu as pltpu
from jax.sharding import PartitionSpec as P

EPS = 1e-06
MESH = pl.DeviceIdType.MESH
CAP = 6
SLOT = 8
F32 = jnp.float32
BF16 = jnp.bfloat16
HIGHEST = lax.Precision.HIGHEST
NT = (((1,), (1,)), ((), ()))


def iota(shape, dim):
    return lax.broadcasted_iota(jnp.int32, shape, dim)


def to_column(row, rows):
    diag = iota((rows, row.shape[1]), 0) == iota((rows, row.shape[1]), 1)
    return jnp.sum(jnp.where(diag, row, 0.0), axis=1, keepdims=True)


def to_row(column, lanes):
    rows = column.shape[0]
    diag = iota((rows, lanes), 0) == iota((rows, lanes), 1)
    return jnp.sum(jnp.where(diag, column, 0.0), axis=0, keepdims=True)


(TOK, KEY, QKV, MIX, PRJ_PAIR, PRJ, RES, ROW, STA, DEN, HID, DWN_PAIR, DWN, EXP_PAIR, EXP, RET,
 OUT) = range(17)
PHASES = 17


def layer_kernel(
    n,
    tok_h, sm_h, sn_h, smax_h, mgain_h, wq_h, wk_h, wv_h, wo_h, win_h, wfo_h, fbias_h,
    wproj_h, fgain_h, wbr_h, routes_h, rw_h, eg_h, eu_h, ed_h, dg_h, du_h, dd_h,
    out_h, nm_h, nn_h, nmax_h,
    tok, sm, sn, smax, mgain, wqkv, wgates, fbias, wproj, fgain, wbr, routes, rw,
    eg, eu, ed, dgu, dd,
    tok_all, key_all, qkv_part, qkv_in, mix_all, prj_part, prj_pair, prj_sum, prj_in, res_all,
    row_out, row_in, sta_out, sta_in, den_part, den_in, hid_all, dwn_part, dwn_pair, dwn_sum, dwn_in,
    exp_part, exp_pair, exp_sum, exp_in, ret_out, ret_in, ret_w_in, out_own, out_all,
    wbr_wide, nm, nn, nmax, pick, gu_acc, gates, wkt, qt, vrow, keep_rows, numer, ret_w,
    load_sem, send_sem, recv_sem, share_sem, store_sem, out_sem,
):
    me_e, me_t = lax.axis_index("ep"), lax.axis_index("tp")
    chips = n // 2
    me_z, core = lax.div(me_t, 2), lax.rem(me_t, 2)
    partner = me_t + 1 - 2 * core
    owned = lax.rem(me_t - me_e + n, n)
    rows = tok.shape[0]
    width = tok.shape[1]
    block = width // n
    head = sn.shape[1]
    hid_e = eg.shape[1]
    hid_d = dd.shape[0]
    cap_rows = CAP * n
    half_rows = cap_rows // 2

    loads = [
        (tok_h, tok), (mgain_h, mgain), (fgain_h, fgain), (wbr_h, wbr), (routes_h, routes),
        (rw_h, rw), (win_h, wgates.at[pl.ds(0, n), :]), (wfo_h, wgates.at[pl.ds(n, n), :]),
        (fbias_h, fbias), (smax_h, smax), (sn_h, sn),
        (wq_h, wqkv.at[:, pl.ds(0, head)]), (wk_h, wqkv.at[:, pl.ds(head, head)]),
        (wv_h, wqkv.at[:, pl.ds(2 * head, head)]), (wo_h, wqkv.at[:, pl.ds(3 * head, head)]),
        (sm_h, sm), (wproj_h, wproj), (dg_h, dgu.at[:, pl.ds(0, hid_d)]),
        (du_h, dgu.at[:, pl.ds(hid_d, hid_d)]), (eg_h, eg), (eu_h, eu), (ed_h, ed), (dd_h, dd),
    ]
    loads = [pltpu.make_async_copy(a, b, load_sem.at[k]) for k, (a, b) in enumerate(loads)]
    for copy in loads:
        copy.start()

    barrier = pltpu.get_barrier_semaphore()

    def greet(d, _):
        pl.semaphore_signal(barrier, 1, device_id=(lax.rem(me_e + d, n), me_t), device_id_type=MESH)
        pl.semaphore_signal(barrier, 1, device_id=(me_e, lax.rem(me_t + d, n)), device_id_type=MESH)
        return 0

    lax.fori_loop(1, n, greet, 0)
    pl.semaphore_wait(barrier, 2 * n - 2)

    def ep_copy(phase, src, dst, peer, landing):
        return pltpu.make_async_remote_copy(
            src_ref=src, dst_ref=dst, send_sem=send_sem.at[phase],
            recv_sem=recv_sem.at[phase, landing], device_id=(peer, me_t), device_id_type=MESH)

    def tp_copy(phase, src, dst, peer, landing):
        return pltpu.make_async_remote_copy(
            src_ref=src, dst_ref=dst, send_sem=send_sem.at[phase],
            recv_sem=recv_sem.at[phase, landing], device_id=(me_e, peer), device_id_type=MESH)

    def over(peer_e, peer_t, phase, src, dst, landing):
        return pltpu.make_async_remote_copy(
            src_ref=src, dst_ref=dst, send_sem=send_sem.at[phase],
            recv_sem=recv_sem.at[phase, landing], device_id=(peer_e, peer_t), device_id_type=MESH)

    def chip(k):
        k = chips - k
        return lax.rem(me_z + chips + lax.div(k + 1, 2) * (2 * lax.rem(k, 2) - 1), chips)

    def sum_over_tp(pair_phase, phase, part, place, pair, summed, arrived):
        def give(k, _):
            z = lax.rem(me_z + k, chips)
            tp_copy(pair_phase, part.at[place(2 * z + 1 - core)], pair.at[z], partner, z).start()
            return 0

        lax.fori_loop(1, chips + 1, give, 0)

        def add(z):
            tp_copy(pair_phase, pair.at[z], pair.at[z], partner, z).wait_recv()
            return part[place(2 * z + core)].astype(F32) + pair[z].astype(F32)

        def pass_on(k, _):
            z = chip(k)
            summed[z] = add(z).astype(BF16)
            tp_copy(phase, summed.at[z], arrived.at[me_z], 2 * z + core, me_z).start()
            return 0

        lax.fori_loop(1, chips, pass_on, 0)
        return add(me_z)

    def summed_over_tp(phase, arrived, acc):
        def one(k, acc):
            z = chip(chips - k)
            tp_copy(phase, arrived.at[z], arrived.at[z], 2 * z + core, z).wait_recv()
            return acc + arrived[z].astype(F32)

        return lax.fori_loop(1, chips, one, acc)

    def gather_over_tp(phase, blocks, place):
        mine = blocks.at[place(me_t)]
        tp_copy(phase, mine, mine, partner, place(me_t)).start()

        def give(k, _):
            tp_copy(phase, mine, mine, 2 * chip(k) + core, place(me_t)).start()
            return 0

        lax.fori_loop(1, chips, give, 0)

        def pass_on(k, _):
            z = chip(chips - k)
            block = blocks.at[place(2 * z + core)]
            tp_copy(phase, block, block, 2 * z + core, place(2 * z + core)).wait_recv()
            tp_copy(phase, block, block, partner, place(2 * z + core)).start()
            return 0

        lax.fori_loop(1, chips, pass_on, 0)

        def take(z, _):
            at = place(2 * z + 1 - core)
            tp_copy(phase, blocks.at[at], blocks.at[at], partner, at).wait_recv()
            return 0

        lax.fori_loop(0, chips, take, 0)

    def row_place(t):
        return lax.rem(t - me_e + n, n)

    def to_peers(copy, me, phase, src_of, dst):
        def one(d, _):
            peer = lax.rem(me + d, n)
            copy(phase, src_of(peer), dst, peer, me).start()
            return 0

        lax.fori_loop(1, n, one, 0)

    def await_peers(copy, me, phase, buffer, use=None, carry=0):
        def one(d, carry):
            peer = lax.rem(me + n - d, n)
            copy(phase, buffer.at[peer], buffer.at[peer], peer, peer).wait_recv()
            return carry if use is None else use(peer, carry)

        return lax.fori_loop(1, n, one, carry)

    def sent(copy, phase, many):
        copy(phase, many, many, 0, 0).wait_send()

    loads[0].wait()
    to_peers(ep_copy, me_e, TOK,
             lambda peer: tok.at[:, pl.ds(pl.multiple_of(peer * block, block), block)],
             tok_all.at[me_e])
    tok_all[me_e] = tok[:, pl.ds(pl.multiple_of(me_e * block, block), block)]

    loads[4].wait()
    loads[5].wait()
    route_rows = [routes[pl.ds(k, 1), :] for k in range(2)]
    lanes_e = iota((128, rows), 0)
    named = sum(jnp.where(lanes_e == r, 1.0, 0.0) for r in route_rows)
    earlier = jnp.where(iota((rows, rows), 0) < iota((rows, rows), 1), 1.0, 0.0)
    before = jnp.dot(named.astype(BF16), earlier.astype(BF16), preferred_element_type=F32)
    base = (CAP * me_e).astype(F32)
    key = jnp.where(named > 0.0, before + base, -1.0)
    eye = jnp.where(iota((rows, rows), 0) == iota((rows, rows), 1), 1.0, 0.0)
    key_all[me_e] = lax.dot_general(
        eye.astype(BF16), key.astype(BF16), NT, preferred_element_type=F32).astype(BF16)
    to_peers(ep_copy, me_e, KEY, lambda peer: key_all.at[me_e], key_all.at[me_e])
    weights = [rw[pl.ds(k, 1), :] for k in range(2)]
    total = weights[0] + weights[1]
    spots = iota((n * SLOT, rows), 0)
    share_t = jnp.zeros((n * SLOT, rows), F32)
    for r, w in zip(route_rows, weights):
        slot = jnp.sum(jnp.where(lanes_e == r, before, 0.0), axis=0, keepdims=True)
        hit = (spots.astype(F32) == r.astype(F32) * SLOT + slot)
        share_t = share_t + jnp.where(hit, w / total, 0.0)
    ret_w[...] = lax.dot_general(eye, share_t, NT, precision=HIGHEST, preferred_element_type=F32)

    def shares():
        return pltpu.make_async_remote_copy(
            src_ref=ret_w, dst_ref=ret_w_in, send_sem=share_sem.at[0], recv_sem=share_sem.at[1],
            device_id=(owned, me_t), device_id_type=MESH)

    @pl.when(owned != me_e)
    def _():
        shares().start()

    @pl.when(owned == me_e)
    def _():
        ret_w_in[...] = ret_w[...]

    loads[1].wait()
    squares = jnp.zeros((rows, block), F32)
    for k in range(n):
        part = tok[:, k * block:(k + 1) * block].astype(F32)
        squares = squares + part * part
    scale = lax.rsqrt(jnp.sum(squares, axis=1, keepdims=True) / width + EPS)
    loads[6].wait()
    loads[7].wait()
    gate = jnp.zeros((rows, 2 * n), F32)
    for k in range(n):
        cols = slice(k * block, (k + 1) * block)
        gain = mgain[:, cols]
        normed = (tok[:, cols].astype(F32) * scale * gain).astype(BF16)
        gate = gate + lax.dot_general(normed, wgates[:, cols], NT, preferred_element_type=F32)
    for k in range(8, 11):
        loads[k].wait()
    lane = iota((rows, 2 * n), 1)
    gate_in = jnp.sum(jnp.where(lane == me_t, gate, 0.0), axis=1, keepdims=True)
    gate_forget = jnp.sum(jnp.where(lane == me_t + n, gate, 0.0), axis=1, keepdims=True)
    bias = jnp.sum(jnp.where(iota((1, n), 1) == me_t, fbias[...], 0.0), axis=1, keepdims=True)
    gate_forget = gate_forget + bias
    log_keep = jnp.minimum(gate_forget, 0.0) - jnp.log1p(jnp.exp(-jnp.abs(gate_forget)))
    old_max = to_column(smax[...], rows)
    new_max = jnp.maximum(log_keep + old_max, gate_in)
    keep = jnp.exp(log_keep + old_max - new_max)
    write = jnp.exp(gate_in - new_max)
    nmax[...] = to_row(new_max, rows)

    await_peers(ep_copy, me_e, TOK, tok_all)
    for k in range(11, 15):
        loads[k].wait()
    gain_m = mgain[:, pl.ds(pl.multiple_of(me_e * block, block), block)]
    group = 4
    big = group * rows

    def project(c, _):
        at = pl.multiple_of(c * group, group)
        x = tok_all[pl.ds(at, group)].reshape(big, block).astype(F32) * gain_m
        y = jnp.dot(x.astype(BF16), wqkv[...], preferred_element_type=F32)
        qkv_part[pl.ds(at, group)] = y.astype(BF16).reshape(group, rows, 4 * head)

        def one(k, _):
            peer = at + k

            @pl.when(peer != me_e)
            def _():
                ep_copy(QKV, qkv_part.at[peer], qkv_in.at[me_e], peer, me_e).start()

            return 0

        return lax.fori_loop(0, group, one, 0)

    lax.fori_loop(0, n // group, project, 0)

    loads[15].wait()
    y = await_peers(ep_copy, me_e, QKV, qkv_in,
                    lambda peer, acc: acc + qkv_in[peer].astype(F32),
                    qkv_part[me_e].astype(F32)) * scale
    query = y[:, :head]
    keys = y[:, head:2 * head] * head ** (-0.5)
    value = y[:, 2 * head:3 * head]
    outgate = y[:, 3 * head:]
    written = write * keys
    new_norm = keep * sn[...] + written
    nn[...] = new_norm
    denom = jnp.sum(query * new_norm, axis=1, keepdims=True)
    qt[...] = query.T
    wkt[...] = written.T
    vrow[...] = value
    keep_rows[...] = jnp.broadcast_to(keep, (rows, head))
    for b in range(rows):
        numer[pl.ds(b, 1), :] = jnp.sum(qt[:, b:b + 1] * sm[b], axis=0, keepdims=True)
    dots = jnp.sum(query * written, axis=1, keepdims=True)
    num = keep * numer[...] + dots * value
    cell = num / jnp.maximum(jnp.abs(denom), 1.0)
    mix_all[me_e] = (jax.nn.sigmoid(outgate) * cell).astype(BF16)
    to_peers(ep_copy, me_e, MIX, lambda peer: mix_all.at[me_e], mix_all.at[me_e])
    for b in range(rows):
        nm[b] = keep_rows[pl.ds(b, 1), :] * sm[b] + wkt[:, b:b + 1] * vrow[pl.ds(b, 1), :]
    stores = [
        pltpu.make_async_copy(a, b, store_sem.at[k])
        for k, (a, b) in enumerate([(nm, nm_h), (nn, nn_h), (nmax, nmax_h)])
    ]
    for copy in stores:
        copy.start()

    await_peers(ep_copy, me_e, KEY, key_all)
    key_t = lax.dot_general(
        jnp.where(iota((n, 128), 0) == iota((n, 128), 1), 1.0, 0.0).astype(BF16),
        key_all[...].reshape(n * rows, 128), NT, preferred_element_type=F32)
    places = (iota((half_rows, n * rows), 0) + core * half_rows).astype(F32)
    for e in range(n):
        pick[pl.ds(e * half_rows, half_rows), :] = jnp.where(
            places == key_t[e:e + 1, :], 1.0, 0.0).astype(BF16)

    await_peers(ep_copy, me_e, MIX, mix_all)
    loads[16].wait()
    y = jnp.dot(mix_all[...].reshape(n * rows, head), wproj[...], preferred_element_type=F32)
    prj_part[...] = y.astype(BF16).reshape(n, rows, block)
    mixed = sum_over_tp(PRJ_PAIR, PRJ, prj_part, row_place, prj_pair, prj_sum, prj_in)
    mixed = summed_over_tp(PRJ, prj_in, mixed)
    residual = (tok_all[owned].astype(F32) + mixed).astype(BF16)
    res_all[owned] = residual
    gather_over_tp(RES, res_all, row_place)
    loads[2].wait()
    loads[3].wait()

    def pass_rows(peer):
        spot = core * n + peer
        tp_copy(ROW, row_in.at[spot], row_in.at[spot], partner, spot).start()

    res_flat = res_all[...].reshape(n * rows, block)

    def dispatch(c, _):
        at = pl.multiple_of(c * group, group)
        y = jnp.dot(pick[pl.ds(pl.multiple_of(at * half_rows, group * half_rows), group * half_rows), :],
                    res_flat, preferred_element_type=F32)
        row_out[pl.ds(at, group)] = y.astype(BF16).reshape(group, half_rows, block)

        def one(k, _):
            peer = at + k

            @pl.when(peer != me_e)
            def _():
                spot = core * n + me_e
                ep_copy(ROW, row_out.at[peer], row_in.at[spot], peer, spot).start()

            return 0

        return lax.fori_loop(0, group, one, 0)

    lax.fori_loop(0, n // group, dispatch, 0)
    row_in[core * n + me_e] = row_out[me_e]
    pass_rows(me_e)

    mine = pl.multiple_of(me_e * block, block)
    gain_f = fgain[:, pl.ds(mine, block)]
    wbr_wide[...] = wbr[...].astype(F32)
    lines = block // 128
    gain_b = gain_f * jnp.concatenate(
        [wbr_wide[pl.ds(me_e * lines + k, 1), :] for k in range(lines)], axis=1)

    def stats(b, _):
        r = res_all[b].astype(F32)
        ss = to_row(jnp.sum(r * r, axis=1, keepdims=True), 128)
        br = to_row(jnp.sum(r * gain_b, axis=1, keepdims=True), 128)
        sta_out[b] = jnp.where(iota((8, 128), 0) == 0, ss, br)
        return 0

    lax.fori_loop(0, n, stats, 0)
    to_peers(ep_copy, me_e, STA, lambda peer: sta_out.at[peer], sta_in.at[me_e])
    loads[17].wait()
    loads[18].wait()

    def dense(c, _):
        at = pl.multiple_of(c * group, group)
        x = res_all[pl.ds(at, group)].reshape(big, block).astype(F32) * gain_f
        y = jnp.dot(x.astype(BF16), dgu[...], preferred_element_type=F32)
        den_part[pl.ds(at, group)] = y.astype(BF16).reshape(group, rows, 2 * hid_d)

        def one(k, _):
            peer = at + k

            @pl.when(peer != me_e)
            def _():
                ep_copy(DEN, den_part.at[peer], den_in.at[me_e], peer, me_e).start()

            return 0

        return lax.fori_loop(0, group, one, 0)

    lax.fori_loop(0, n // group, dense, 0)

    loads[19].wait()
    loads[20].wait()

    def expert_in(peer, ss):
        other = (1 - core) * n + peer
        tp_copy(ROW, row_in.at[other], row_in.at[other], partner, other).wait_recv()
        x = jnp.concatenate([row_in[peer], row_in[n + peer]], axis=0).astype(F32)
        at = pl.multiple_of(peer * block, block)
        xg = (x * fgain[:, pl.ds(at, block)]).astype(BF16)
        gu_acc[:, pl.ds(0, hid_e)] += jnp.dot(xg, eg[pl.ds(at, block), :], preferred_element_type=F32)
        gu_acc[:, pl.ds(hid_e, hid_e)] += jnp.dot(xg, eu[pl.ds(at, block), :], preferred_element_type=F32)
        return ss + jnp.sum(x * x, axis=1, keepdims=True)

    def expert_next(d, ss):
        peer = lax.rem(me_e + n - d, n)
        spot = core * n + peer
        ep_copy(ROW, row_in.at[spot], row_in.at[spot], peer, spot).wait_recv()
        pass_rows(peer)
        return expert_in(lax.rem(peer + 1, n), ss)

    gu_acc[...] = jnp.zeros_like(gu_acc)
    ss = lax.fori_loop(1, n, expert_next, jnp.zeros((cap_rows, 1), F32))
    ss = expert_in(lax.rem(me_e + 1, n), ss)
    row_scale = lax.rsqrt(ss / width + EPS)
    g = gu_acc[:, :hid_e] * row_scale
    u = gu_acc[:, hid_e:] * row_scale
    hidden = (g / (1.0 + jnp.exp(-g)) * u).astype(BF16)
    loads[21].wait()
    for k in range(n):
        exp_part[k] = jnp.dot(hidden, ed[:, k * block:(k + 1) * block],
                              preferred_element_type=F32).astype(BF16)
    routed_sum = sum_over_tp(EXP_PAIR, EXP, exp_part, row_place, exp_pair, exp_sum, exp_in)

    sums = await_peers(ep_copy, me_e, STA, sta_in, lambda peer, acc: acc + sta_in[peer], sta_out[me_e])
    dense_scale = lax.rsqrt(to_column(sums[0:1, :], rows) / width + EPS)
    branch = jax.nn.sigmoid(to_column(sums[1:2, :], rows) * dense_scale)
    y = await_peers(ep_copy, me_e, DEN, den_in,
                    lambda peer, acc: acc + den_in[peer].astype(F32),
                    den_part[me_e].astype(F32)) * dense_scale
    g, u = y[:, :hid_d], y[:, hid_d:]
    hid_all[me_e] = (g / (1.0 + jnp.exp(-g)) * u * branch).astype(BF16)
    to_peers(ep_copy, me_e, HID, lambda peer: hid_all.at[me_e], hid_all.at[me_e])

    y = summed_over_tp(EXP, exp_in, routed_sum)
    spot, col = iota((n * SLOT, cap_rows), 0), iota((n * SLOT, cap_rows), 1)
    within = jnp.bitwise_and(spot, SLOT - 1)
    source = CAP * jnp.right_shift(spot, SLOT.bit_length() - 1) + within
    spread = jnp.where((source == col) & (within < CAP), 1.0, 0.0).astype(BF16)
    ret_out[...] = jnp.dot(spread, y.astype(BF16), preferred_element_type=F32).reshape(n, SLOT, block)

    def give_back(i, _):
        place = lax.rem(i + owned, n)
        own = (owned == me_e) & (place == me_t)

        @pl.when(jnp.logical_not(own))
        def _():
            over(owned, place, RET, ret_out.at[i], ret_in.at[me_e], me_e).start()

        @pl.when(own)
        def _():
            ret_in[me_e] = ret_out[i]

        return 0

    lax.fori_loop(0, n, give_back, 0)

    await_peers(ep_copy, me_e, HID, hid_all)
    loads[22].wait()
    y = jnp.dot(hid_all[...].reshape(n * rows, hid_d), dd[...], preferred_element_type=F32)
    dwn_part[...] = y.astype(BF16).reshape(n, rows, block)
    dense_sum = sum_over_tp(DWN_PAIR, DWN, dwn_part, row_place, dwn_pair, dwn_sum, dwn_in)

    def returned(e, _):
        source = lax.rem(e + me_e, n)

        @pl.when((e != me_e) | (source != me_t))
        def _():
            over(e, source, RET, ret_in.at[e], ret_in.at[e], e).wait_recv()

        return 0

    lax.fori_loop(0, n, returned, 0)

    @pl.when(owned != me_e)
    def _():
        shares().wait()

    routed = jnp.dot(ret_w_in[...], ret_in[...].reshape(n * SLOT, block), precision=HIGHEST,
                     preferred_element_type=F32)
    known = res_all[owned].astype(F32) + routed

    y = summed_over_tp(DWN, dwn_in, dense_sum)
    out_own[...] = (known + y).astype(BF16)

    def publish(k, _):
        z = chip(k)
        over(owned, 2 * z + core, OUT, out_own, out_all.at[me_e], me_e).start()
        return 0

    lax.fori_loop(1, chips, publish, 0)

    @pl.when(owned != me_e)
    def _():
        over(owned, me_t, OUT, out_own, out_all.at[me_e], me_e).start()

    @pl.when(owned == me_e)
    def _():
        out_all[me_e] = out_own[...]

    def write(j, where):
        return pltpu.make_async_copy(
            out_all.at[j], out_h.at[:, pl.ds(pl.multiple_of(j * block, block), block)], out_sem.at[where])

    def forward(k, _):
        j = lax.rem(2 * k + lax.rem(me_e + core, 2), n)
        source = lax.rem(me_e + j, n)

        @pl.when((j != me_e) | (source != me_t))
        def _():
            over(j, source, OUT, out_all.at[j], out_all.at[j], j).wait_recv()

        over(me_e, partner, OUT, out_all.at[j], out_all.at[j], j).start()
        write(j, j).start()
        return 0

    lax.fori_loop(0, chips, forward, 0)

    def finish(k, _):
        j = lax.rem(2 * k + lax.rem(me_e + core + 1, 2), n)
        over(me_e, partner, OUT, out_all.at[j], out_all.at[j], j).wait_recv()
        write(j, j).start()
        return 0

    lax.fori_loop(0, chips, finish, 0)

    def written_out(j, _):
        write(j, j).wait()
        return 0

    lax.fori_loop(0, n, written_out, 0)
    for copy in stores:
        copy.wait()
    rest = pl.ds(0, n - 1)
    sent(ep_copy, TOK, tok_all.at[rest])
    sent(ep_copy, KEY, key_all.at[rest])
    sent(ep_copy, QKV, qkv_part.at[rest])
    sent(ep_copy, MIX, mix_all.at[rest])
    some = pl.ds(0, chips - 1)
    sent(tp_copy, PRJ_PAIR, prj_pair)
    sent(tp_copy, PRJ, prj_sum.at[some])
    sent(tp_copy, RES, res_all.at[rest])
    sent(ep_copy, ROW, row_in.at[pl.ds(0, 2 * n - 1)])
    sent(ep_copy, STA, sta_out.at[rest])
    sent(ep_copy, DEN, den_part.at[rest])
    sent(ep_copy, HID, hid_all.at[rest])
    sent(tp_copy, EXP_PAIR, exp_pair)
    sent(tp_copy, EXP, exp_sum.at[some])
    sent(tp_copy, DWN_PAIR, dwn_pair)
    sent(tp_copy, DWN, dwn_sum.at[some])

    @pl.when(owned != me_e)
    def _():
        sent(ep_copy, RET, ret_out)
        sent(ep_copy, OUT, out_all)

    @pl.when(owned == me_e)
    def _():
        sent(ep_copy, RET, ret_out.at[rest])
        sent(ep_copy, OUT, out_all.at[rest])


def on_device(
    n, tokens, state_matrix, state_norm, state_max, mixer_gain, w_query, w_key, w_value, w_outgate,
    w_ingate, w_forget, forget_bias, w_proj, ffn_gain, w_branch, routes, route_weight,
    expert_gate, expert_up, expert_down, dense_gate, dense_up, dense_down,
):
    rows, width = tokens.shape
    head = state_norm.shape[-1]
    block = width // n
    hid_e, hid_d = expert_gate.shape[2], dense_gate.shape[1]
    cap_rows = CAP * n
    args = (
        tokens,
        state_matrix.reshape(rows, head, head),
        state_norm.reshape(rows, head),
        state_max.T,
        mixer_gain.reshape(1, width),
        w_query, w_key, w_value, w_outgate,
        w_ingate.T, w_forget.T,
        forget_bias.reshape(1, n),
        w_proj,
        ffn_gain.reshape(1, width),
        w_branch.reshape(width // 128, 128),
        routes.T, route_weight.T,
        expert_gate.reshape(width, hid_e), expert_up.reshape(width, hid_e),
        expert_down.reshape(hid_e, width),
        dense_gate, dense_up, dense_down,
    )
    vm = pltpu.VMEM
    dma = pltpu.SemaphoreType.DMA
    half_rows = cap_rows // 2

    def hier(tall):
        return [vm((n, tall, block), BF16)] + [vm((n // 2, tall, block), BF16)] * 3

    scratch = [
        vm((rows, width), BF16), vm((rows, head, head), F32), vm((rows, head), F32), vm((1, rows), F32),
        vm((1, width), F32), vm((block, 4 * head), BF16), vm((2 * n, width), BF16), vm((1, n), F32),
        vm((head, block), BF16), vm((1, width), F32), vm((width // 128, 128), BF16), vm((2, rows), jnp.int32),
        vm((2, rows), F32), vm((width, hid_e), BF16), vm((width, hid_e), BF16), vm((hid_e, width), BF16),
        vm((block, 2 * hid_d), BF16), vm((hid_d, block), BF16),
        vm((n, rows, block), BF16), vm((n, rows, 128), BF16),
        vm((n, rows, 4 * head), BF16), vm((n, rows, 4 * head), BF16),
        vm((n, rows, head), BF16), *hier(rows), vm((n, rows, block), BF16),
        vm((n, half_rows, block), BF16), vm((2 * n, half_rows, block), BF16),
        vm((n, 8, 128), F32), vm((n, 8, 128), F32),
        vm((n, rows, 2 * hid_d), BF16), vm((n, rows, 2 * hid_d), BF16),
        vm((n, rows, hid_d), BF16), *hier(rows), *hier(cap_rows),
        vm((n, SLOT, block), F32), vm((n, SLOT, block), F32), vm((rows, n * SLOT), F32),
        vm((rows, block), BF16), vm((n, rows, block), BF16),
        vm((width // 128, 128), F32), vm((rows, head, head), F32), vm((rows, head), F32), vm((1, rows), F32),
        vm((n * half_rows, n * rows), BF16), vm((cap_rows, 2 * hid_e), F32), vm((rows, 2 * n), F32),
        vm((head, rows), F32), vm((head, rows), F32), vm((rows, head), F32), vm((rows, head), F32),
        vm((rows, head), F32), vm((rows, n * SLOT), F32),
        dma((len(args),)), dma((PHASES,)), dma((PHASES, 2 * n)), dma((2,)), dma((3,)), dma((n,)),
    ]
    any_space = pl.BlockSpec(memory_space=pl.ANY)
    out, new_matrix, new_norm, new_max = pl.pallas_call(
        functools.partial(layer_kernel, n),
        out_shape=(
            jax.ShapeDtypeStruct((rows, width), BF16),
            jax.ShapeDtypeStruct((rows, head, head), F32),
            jax.ShapeDtypeStruct((rows, head), F32),
            jax.ShapeDtypeStruct((1, rows), F32),
        ),
        in_specs=[any_space] * len(args),
        out_specs=[any_space] * 4,
        scratch_shapes=scratch,
        compiler_params=pltpu.CompilerParams(
            collective_id=0, has_side_effects=True, vmem_limit_bytes=56 * 1024 * 1024),
        name="layer",
    )(*args)
    return (out, new_matrix.reshape(rows, 1, head, head), new_norm.reshape(rows, 1, head), new_max.T)


def solution(mesh):
    n = mesh.shape["ep"]
    in_specs = (
        P("ep", None),
        P("ep", "tp", None, None),
        P("ep", "tp", None),
        P("ep", "tp"),
        P(),
        P("ep", "tp"),
        P("ep", "tp"),
        P("ep", "tp"),
        P("ep", "tp"),
        P(),
        P(),
        P(),
        P("tp", "ep"),
        P(),
        P(),
        P("ep", None),
        P("ep", None),
        P("ep", None, "tp"),
        P("ep", None, "tp"),
        P("ep", "tp", None),
        P("ep", "tp"),
        P("ep", "tp"),
        P("tp", "ep"),
    )
    out_specs = (P("ep", None), P("ep", "tp", None, None), P("ep", "tp", None), P("ep", "tp"))
    return jax.shard_map(
        functools.partial(on_device, n), mesh=mesh, in_specs=in_specs, out_specs=out_specs,
        check_vma=False)
```

```python
import functools
import math

import jax
import jax.numpy as jnp
from jax import lax
from jax.experimental import pallas as pl
from jax.experimental.pallas import tpu as pltpu
from jax.sharding import PartitionSpec as P

EPS = 1e-06
MESH = pl.DeviceIdType.MESH
CAP = 6
SLOT = 8
F32 = jnp.float32
BF16 = jnp.bfloat16
HIGHEST = lax.Precision.HIGHEST
NT = (((1,), (1,)), ((), ()))


def iota(shape, dim):
    return lax.broadcasted_iota(jnp.int32, shape, dim)


def to_column(row, rows):
    diag = iota((rows, row.shape[1]), 0) == iota((rows, row.shape[1]), 1)
    return jnp.sum(jnp.where(diag, row, 0.0), axis=1, keepdims=True)


def to_row(column, lanes):
    rows = column.shape[0]
    diag = iota((rows, lanes), 0) == iota((rows, lanes), 1)
    return jnp.sum(jnp.where(diag, column, 0.0), axis=0, keepdims=True)


(TOK, KEY, QKV, MIX, PRJ_PAIR, PRJ, RES, ROW, STA, DEN, HID, DWN_PAIR, DWN, EXP_PAIR, EXP, RET,
 OUT, NEAR, FAR, NEAR_DOWN, FAR_DOWN) = range(21)
PHASES = 21
EARLY = 96


def layer_kernel(
    n,
    tok_h, sm_h, sn_h, smax_h, mgain_h, wq_h, wk_h, wv_h, wo_h, win_h, wfo_h, fbias_h,
    wproj_h, fgain_h, wbr_h, routes_h, rw_h, eg_h, eu_h, ed_h, dg_h, du_h, dd_h,
    out, nm, nn, nmax,
    tok, sm, sn, smax, mgain, wqkv, wgates, fbias, wproj, fgain, wbr, routes, rw,
    eg, eu, ed, dgu_all, dd_all,
    tok_all, key_all, qkv_part, qkv_in, mix_all, prj_part, prj_pair, prj_sum, prj_in, res_own, res_all, res_fin,
    row_out, row_in, sta_out, sta_in, den_part, den_in, hid_all, dwn_part, dwn_pair, dwn_sum, dwn_in,
    exp_part, exp_pair, exp_sum, exp_in, ret_out, ret_in, ret_w_in, out_own,
    wbr_wide, pick, x_cat, gu_acc, gates, wkt, qt, vrow, keep_rows, numer, ret_w,
    load_sem, send_sem, recv_sem, share_sem, res_sem,
):
    me_e, me_t = lax.axis_index("ep"), lax.axis_index("tp")
    chips = n // 2
    side = math.isqrt(n)
    me_y, me_x = lax.div(me_e, side), lax.rem(me_e, side)
    me_z, core = lax.div(me_t, 2), lax.rem(me_t, 2)
    partner = me_t + 1 - 2 * core
    owned = lax.rem(me_t - me_e + n, n)
    final_rows = side * me_y + lax.rem(owned, side)
    final_cols = side * lax.div(owned, side) + me_x
    rows = tok.shape[0]
    width = tok.shape[1]
    block = width // n
    head = sn.shape[1]
    hid_e = eg.shape[1]
    hid_d = dd_all.shape[1]
    quarter = rows * side
    cap_rows = CAP * n
    few_rows = CAP * side
    dgu, dd = dgu_all.at[me_x], dd_all.at[me_y]

    loads = [
        (tok_h, tok), (mgain_h, mgain), (fgain_h, fgain), (wbr_h, wbr), (routes_h, routes),
        (rw_h, rw), (win_h, wgates.at[pl.ds(0, n), :]), (wfo_h, wgates.at[pl.ds(n, n), :]),
        (fbias_h, fbias), (smax_h, smax), (sn_h, sn),
        (wq_h, wqkv.at[:, pl.ds(0, head)]), (wk_h, wqkv.at[:, pl.ds(head, head)]),
        (wv_h, wqkv.at[:, pl.ds(2 * head, head)]), (wo_h, wqkv.at[:, pl.ds(3 * head, head)]),
        (sm_h, sm), (wproj_h, wproj), (dg_h, dgu_all.at[me_x, :, pl.ds(0, hid_d)]),
        (du_h, dgu_all.at[me_x, :, pl.ds(hid_d, hid_d)]), (eg_h, eg), (eu_h, eu), (ed_h, ed), (dd_h, dd),
    ]
    loads = [pltpu.make_async_copy(a, b, load_sem.at[k]) for k, (a, b) in enumerate(loads)]
    for copy in loads:
        copy.start()

    barrier = pltpu.get_barrier_semaphore()

    def greet(d, _):
        pl.semaphore_signal(barrier, 1, device_id=(lax.rem(me_e + d, n), me_t), device_id_type=MESH)
        pl.semaphore_signal(barrier, 1, device_id=(me_e, lax.rem(me_t + d, n)), device_id_type=MESH)
        return 0

    lax.fori_loop(1, n, greet, 0)
    pl.semaphore_wait(barrier, 2 * n - 2)

    def ep_copy(phase, src, dst, peer, landing):
        return pltpu.make_async_remote_copy(
            src_ref=src, dst_ref=dst, send_sem=send_sem.at[phase],
            recv_sem=recv_sem.at[phase, landing], device_id=(peer, me_t), device_id_type=MESH)

    def tp_copy(phase, src, dst, peer, landing):
        return pltpu.make_async_remote_copy(
            src_ref=src, dst_ref=dst, send_sem=send_sem.at[phase],
            recv_sem=recv_sem.at[phase, landing], device_id=(me_e, peer), device_id_type=MESH)

    def over(peer_e, peer_t, phase, src, dst, landing):
        return pltpu.make_async_remote_copy(
            src_ref=src, dst_ref=dst, send_sem=send_sem.at[phase],
            recv_sem=recv_sem.at[phase, landing], device_id=(peer_e, peer_t), device_id_type=MESH)

    def chip(k):
        k = chips - k
        return lax.rem(me_z + chips + lax.div(k + 1, 2) * (2 * lax.rem(k, 2) - 1), chips)

    def sum_over_tp(pair_phase, phase, part, place, pair, summed, arrived):
        def give(k, _):
            z = lax.rem(me_z + k, chips)
            tp_copy(pair_phase, part.at[place(2 * z + 1 - core)], pair.at[z], partner, z).start()
            return 0

        lax.fori_loop(1, chips + 1, give, 0)

        def add(z):
            tp_copy(pair_phase, pair.at[z], pair.at[z], partner, z).wait_recv()
            return part[place(2 * z + core)].astype(F32) + pair[z].astype(F32)

        def pass_on(k, _):
            z = chip(k)
            summed[z] = add(z).astype(BF16)
            tp_copy(phase, summed.at[z], arrived.at[me_z], 2 * z + core, me_z).start()
            return 0

        lax.fori_loop(1, chips, pass_on, 0)
        return add(me_z)

    def summed_over_tp(phase, arrived, acc):
        def one(k, acc):
            z = chip(chips - k)
            tp_copy(phase, arrived.at[z], arrived.at[z], 2 * z + core, z).wait_recv()
            return acc + arrived[z].astype(F32)

        return lax.fori_loop(1, chips, one, acc)

    def gather_quarter():
        to_e = side * me_y + lax.rem(owned, side)
        spot = me_x * side + lax.div(owned, side)

        def give(k, _):
            over(to_e, 2 * chip(k) + core, RES, res_own, res_all.at[spot], spot).start()
            return 0

        lax.fori_loop(1, chips, give, 0)

        @pl.when(to_e != me_e)
        def _():
            over(to_e, me_t, RES, res_own, res_all.at[spot], spot).start()

        @pl.when(to_e == me_e)
        def _():
            res_all[spot] = res_own[...]

        def source(spot):
            o = side * lax.rem(spot, side) + me_x
            j = side * me_y + lax.div(spot, side)
            return j, lax.rem(o + j, n)

        def spot_of(k, parity):
            return (2 * lax.rem(k, 2) + parity) * side + lax.div(k, 2)

        def pass_on(k, _):
            spot = spot_of(k, lax.rem(core + me_x, 2))
            j, t = source(spot)

            @pl.when((j != me_e) | (t != me_t))
            def _():
                over(j, t, RES, res_all.at[spot], res_all.at[spot], spot).wait_recv()

            over(me_e, partner, RES, res_all.at[spot], res_all.at[spot], spot).start()
            return 0

        lax.fori_loop(0, n // 2, pass_on, 0)

        def take(k, _):
            spot = spot_of(k, lax.rem(core + me_x + 1, 2))
            over(me_e, partner, RES, res_all.at[spot], res_all.at[spot], spot).wait_recv()
            return 0

        lax.fori_loop(0, n // 2, take, 0)

    def along_x(step):
        return side * me_y + lax.rem(me_x + step + side, side)

    def along_y(step):
        return side * lax.rem(me_y + step + side, side) + me_x

    def weight_copy(phase, buffer, block_of, peer, first, many, landing):
        part = buffer.at[block_of, pl.ds(first, many), :]
        return over(peer, me_t, phase, part, part, landing)

    def near(phase, buffer, me, along, first, many, part):
        for way, step in enumerate((1, -1)):
            weight_copy(phase, buffer, me, along(step), first, many, 2 * part + way).start()

    def arrived_near(phase, buffer, me, along, first, many, part):
        for way, step in enumerate((-1, 1)):
            owner = lax.rem(me + step + side, side)
            weight_copy(phase, buffer, owner, along(step), first, many, 2 * part + way).wait_recv()

    def far(phase, buffer, me, along, first, many, part, act):
        half = many // 2
        for way, step in enumerate((1, -1)):
            if act == "start":
                owner = lax.rem(me - step + side, side)
                weight_copy(phase, buffer, owner, along(step), first + way * half, half, 2 * part + way).start()
            else:
                owner = lax.rem(me + 2, side)
                weight_copy(phase, buffer, owner, along(-step), first + way * half, half, 2 * part + way).wait_recv()

    late = block - EARLY

    def row_place(t):
        return lax.rem(t - me_e + n, n)

    def to_peers(copy, me, phase, src_of, dst):
        def one(d, _):
            peer = lax.rem(me + d, n)
            copy(phase, src_of(peer), dst, peer, me).start()
            return 0

        lax.fori_loop(1, n, one, 0)

    def await_peers(copy, me, phase, buffer, use=None, carry=0):
        def one(d, carry):
            peer = lax.rem(me + n - d, n)
            copy(phase, buffer.at[peer], buffer.at[peer], peer, peer).wait_recv()
            return carry if use is None else use(peer, carry)

        return lax.fori_loop(1, n, one, carry)

    def to_y_peers(phase, src_of, dst):
        def one(d, _):
            y = lax.rem(me_y + d, side)
            over(side * y + me_x, me_t, phase, src_of(y), dst, me_y).start()
            return 0

        lax.fori_loop(1, side, one, 0)

    def await_y_peers(phase, buffer, use=None, carry=0):
        def one(d, carry):
            y = lax.rem(me_y + side - d, side)
            over(side * y + me_x, me_t, phase, buffer.at[y], buffer.at[y], y).wait_recv()
            return carry if use is None else use(y, carry)

        return lax.fori_loop(1, side, one, carry)

    def sent(copy, phase, many):
        copy(phase, many, many, 0, 0).wait_send()

    loads[0].wait()
    to_peers(ep_copy, me_e, TOK,
             lambda peer: tok.at[:, pl.ds(pl.multiple_of(peer * block, block), block)],
             tok_all.at[me_e])
    tok_all[me_e] = tok[:, pl.ds(pl.multiple_of(me_e * block, block), block)]

    loads[17].wait()
    loads[18].wait()
    near(NEAR, dgu_all, me_x, along_x, 0, EARLY, 0)

    loads[4].wait()
    loads[5].wait()
    route_rows = [routes[pl.ds(k, 1), :] for k in range(2)]
    lanes_e = iota((128, rows), 0)
    named = sum(jnp.where(lanes_e == r, 1.0, 0.0) for r in route_rows)
    earlier = jnp.where(iota((rows, rows), 0) < iota((rows, rows), 1), 1.0, 0.0)
    before = jnp.dot(named.astype(BF16), earlier.astype(BF16), preferred_element_type=F32)
    base = (CAP * me_y).astype(F32)
    key = jnp.where(named > 0.0, before + base, -1.0)
    eye = jnp.where(iota((rows, rows), 0) == iota((rows, rows), 1), 1.0, 0.0)
    key_all[me_y] = lax.dot_general(
        eye.astype(BF16), key.astype(BF16), NT, preferred_element_type=F32).astype(BF16)
    to_y_peers(KEY, lambda y: key_all.at[me_y], key_all.at[me_y])
    weights = [rw[pl.ds(k, 1), :] for k in range(2)]
    total = weights[0] + weights[1]
    spots = iota((n * SLOT, rows), 0)
    share_t = jnp.zeros((n * SLOT, rows), F32)
    for r, w in zip(route_rows, weights):
        slot = jnp.sum(jnp.where(lanes_e == r, before, 0.0), axis=0, keepdims=True)
        hit = (spots.astype(F32) == r.astype(F32) * SLOT + slot)
        share_t = share_t + jnp.where(hit, w / total, 0.0)
    ret_w[...] = lax.dot_general(eye, share_t, NT, precision=HIGHEST, preferred_element_type=F32)

    def shares():
        return pltpu.make_async_remote_copy(
            src_ref=ret_w, dst_ref=ret_w_in, send_sem=share_sem.at[0], recv_sem=share_sem.at[1],
            device_id=(final_rows, me_t), device_id_type=MESH)

    @pl.when(final_rows != me_e)
    def _():
        shares().start()

    @pl.when(final_rows == me_e)
    def _():
        ret_w_in[...] = ret_w[...]

    loads[1].wait()
    squares = jnp.zeros((rows, block), F32)
    for k in range(n):
        part = tok[:, k * block:(k + 1) * block].astype(F32)
        squares = squares + part * part
    scale = lax.rsqrt(jnp.sum(squares, axis=1, keepdims=True) / width + EPS)
    loads[6].wait()
    loads[7].wait()
    gate = jnp.zeros((rows, 2 * n), F32)
    for k in range(n):
        cols = slice(k * block, (k + 1) * block)
        gain = mgain[:, cols]
        normed = (tok[:, cols].astype(F32) * scale * gain).astype(BF16)
        gate = gate + lax.dot_general(normed, wgates[:, cols], NT, preferred_element_type=F32)
    for k in range(8, 11):
        loads[k].wait()
    lane = iota((rows, 2 * n), 1)
    gate_in = jnp.sum(jnp.where(lane == me_t, gate, 0.0), axis=1, keepdims=True)
    gate_forget = jnp.sum(jnp.where(lane == me_t + n, gate, 0.0), axis=1, keepdims=True)
    bias = jnp.sum(jnp.where(iota((1, n), 1) == me_t, fbias[...], 0.0), axis=1, keepdims=True)
    gate_forget = gate_forget + bias
    log_keep = jnp.minimum(gate_forget, 0.0) - jnp.log1p(jnp.exp(-jnp.abs(gate_forget)))
    old_max = to_column(smax[...], rows)
    new_max = jnp.maximum(log_keep + old_max, gate_in)
    keep = jnp.exp(log_keep + old_max - new_max)
    write = jnp.exp(gate_in - new_max)
    nmax[...] = to_row(new_max, rows)

    await_peers(ep_copy, me_e, TOK, tok_all)
    for k in range(11, 15):
        loads[k].wait()
    gain_m = mgain[:, pl.ds(pl.multiple_of(me_e * block, block), block)]
    group = 4
    big = group * rows

    def project(c, _):
        at = pl.multiple_of(c * group, group)
        x = tok_all[pl.ds(at, group)].reshape(big, block).astype(F32) * gain_m
        y = jnp.dot(x.astype(BF16), wqkv[...], preferred_element_type=F32)
        qkv_part[pl.ds(at, group)] = y.astype(BF16).reshape(group, rows, 4 * head)

        def one(k, _):
            peer = at + k

            @pl.when(peer != me_e)
            def _():
                ep_copy(QKV, qkv_part.at[peer], qkv_in.at[me_e], peer, me_e).start()

            return 0

        return lax.fori_loop(0, group, one, 0)

    lax.fori_loop(0, n // group, project, 0)

    loads[15].wait()
    y = await_peers(ep_copy, me_e, QKV, qkv_in,
                    lambda peer, acc: acc + qkv_in[peer].astype(F32),
                    qkv_part[me_e].astype(F32)) * scale
    query = y[:, :head]
    keys = y[:, head:2 * head] * head ** (-0.5)
    value = y[:, 2 * head:3 * head]
    outgate = y[:, 3 * head:]
    written = write * keys
    new_norm = keep * sn[...] + written
    nn[...] = new_norm
    denom = jnp.sum(query * new_norm, axis=1, keepdims=True)
    qt[...] = query.T
    wkt[...] = written.T
    vrow[...] = value
    keep_rows[...] = jnp.broadcast_to(keep, (rows, head))
    for b in range(rows):
        numer[pl.ds(b, 1), :] = jnp.sum(qt[:, b:b + 1] * sm[b], axis=0, keepdims=True)
    dots = jnp.sum(query * written, axis=1, keepdims=True)
    num = keep * numer[...] + dots * value
    cell = num / jnp.maximum(jnp.abs(denom), 1.0)
    mix_all[me_e] = (jax.nn.sigmoid(outgate) * cell).astype(BF16)
    to_peers(ep_copy, me_e, MIX, lambda peer: mix_all.at[me_e], mix_all.at[me_e])
    arrived_near(NEAR, dgu_all, me_x, along_x, 0, EARLY, 0)
    far(FAR, dgu_all, me_x, along_x, 0, EARLY, 0, "start")
    near(NEAR, dgu_all, me_x, along_x, EARLY, late, 1)
    loads[22].wait()
    near(NEAR_DOWN, dd_all, me_y, along_y, 0, hid_d, 0)
    for b in range(rows):
        nm[b] = keep_rows[pl.ds(b, 1), :] * sm[b] + wkt[:, b:b + 1] * vrow[pl.ds(b, 1), :]

    await_y_peers(KEY, key_all)
    key_t = lax.dot_general(
        jnp.where(iota((n, 128), 0) == iota((n, 128), 1), 1.0, 0.0).astype(BF16),
        key_all[...].reshape(quarter, 128), NT, preferred_element_type=F32)
    places = iota((few_rows, quarter), 0).astype(F32)
    for e in range(0, n, 2):
        both = [jnp.where(places == key_t[k:k + 1, :], 1.0, 0.0) for k in (e, e + 1)]
        pick[pl.ds(e * few_rows, 2 * few_rows), :] = jnp.concatenate(both, axis=0).astype(BF16)

    await_peers(ep_copy, me_e, MIX, mix_all)
    loads[16].wait()
    y = jnp.dot(mix_all[...].reshape(n * rows, head), wproj[...], preferred_element_type=F32)
    prj_part[...] = y.astype(BF16).reshape(n, rows, block)
    mixed = sum_over_tp(PRJ_PAIR, PRJ, prj_part, row_place, prj_pair, prj_sum, prj_in)
    mixed = summed_over_tp(PRJ, prj_in, mixed)
    residual = (tok_all[owned].astype(F32) + mixed).astype(BF16)
    res_own[...] = residual

    def to_final():
        return pltpu.make_async_remote_copy(
            src_ref=res_own, dst_ref=res_fin, send_sem=res_sem.at[0], recv_sem=res_sem.at[1],
            device_id=(final_cols, me_t), device_id_type=MESH)

    gather_quarter()

    @pl.when(final_cols != me_e)
    def _():
        to_final().start()

    @pl.when(final_cols == me_e)
    def _():
        res_fin[...] = res_own[...]

    loads[2].wait()
    loads[3].wait()

    def pass_rows(peer):
        spot = core * n + peer
        tp_copy(ROW, row_in.at[spot], row_in.at[spot], partner, spot).start()

    half_side = side // 2
    res_half = jnp.concatenate(
        [res_all[pl.ds((core * half_side + k) * side, side)].reshape(quarter, block)
         for k in range(half_side)], axis=1)

    def dispatch(c, _):
        at = pl.multiple_of(c * group, group)
        y = jnp.dot(pick[pl.ds(pl.multiple_of(at * few_rows, group * few_rows), group * few_rows), :],
                    res_half, preferred_element_type=F32)
        row_out[pl.ds(at, group)] = y.reshape(group, few_rows, half_side * block).astype(BF16)

        def one(k, _):
            peer = at + k

            @pl.when(peer != me_e)
            def _():
                spot = core * n + me_e
                ep_copy(ROW, row_out.at[peer], row_in.at[spot], peer, spot).start()

            return 0

        return lax.fori_loop(0, group, one, 0)

    lax.fori_loop(0, n // group, dispatch, 0)
    row_in[core * n + me_e] = row_out[me_e]
    pass_rows(me_e)

    arrived_near(NEAR, dgu_all, me_x, along_x, EARLY, late, 1)
    far(FAR, dgu_all, me_x, along_x, EARLY, late, 1, "start")
    arrived_near(NEAR_DOWN, dd_all, me_y, along_y, 0, hid_d, 0)
    far(FAR_DOWN, dd_all, me_y, along_y, 0, hid_d, 0, "start")

    wbr_wide[...] = wbr[...].astype(F32)
    lines = block // 128
    squares = [jnp.zeros((rows, 1), F32)] * side
    branches = [jnp.zeros((rows, 1), F32)] * side
    for k in range(side):
        j = side * me_y + k
        gain_f = fgain[:, pl.ds(pl.multiple_of(j * block, block), block)]
        gain_b = gain_f * jnp.concatenate(
            [wbr_wide[pl.ds(j * lines + i, 1), :] for i in range(lines)], axis=1)
        for g in range(side):
            r = res_all[k * side + g].astype(F32)
            squares[g] = squares[g] + jnp.sum(r * r, axis=1, keepdims=True)
            branches[g] = branches[g] + jnp.sum(r * gain_b, axis=1, keepdims=True)
            x_cat[pl.ds(g * rows, rows), k * block:(k + 1) * block] = (r * gain_f).astype(BF16)
    for g in range(side):
        sta_out[g] = jnp.where(iota((8, 128), 0) == 0, to_row(squares[g], 128), to_row(branches[g], 128))
    to_y_peers(STA, lambda y: sta_out.at[y], sta_in.at[me_y])

    loads[19].wait()
    loads[20].wait()

    deep = half_side * block

    def expert_in(y, half, ss):
        x = row_in[pl.ds(half * n + y * side, side)].astype(F32).reshape(cap_rows, deep)
        at = pl.multiple_of(y * side * block + half * deep, deep)
        xg = (x * fgain[:, pl.ds(at, deep)]).astype(BF16)
        gu_acc[:, pl.ds(0, hid_e)] += jnp.dot(xg, eg[pl.ds(at, deep), :], preferred_element_type=F32)
        gu_acc[:, pl.ds(hid_e, hid_e)] += jnp.dot(xg, eu[pl.ds(at, deep), :], preferred_element_type=F32)
        return ss + jnp.sum(x * x, axis=1, keepdims=True)

    def expert_first(d, ss):
        y = lax.rem(me_y + side - d, side)

        def one(k, _):
            peer = side * y + lax.rem(me_x + k, side)
            spot = core * n + peer

            @pl.when(peer != me_e)
            def _():
                ep_copy(ROW, row_in.at[spot], row_in.at[spot], peer, spot).wait_recv()
                pass_rows(peer)

            return 0

        lax.fori_loop(0, side, one, 0)
        return expert_in(y, core, ss)

    def expert_second(d, ss):
        y = lax.rem(me_y + side - d, side)

        def one(k, _):
            other = (1 - core) * n + side * y + k
            tp_copy(ROW, row_in.at[other], row_in.at[other], partner, other).wait_recv()
            return 0

        lax.fori_loop(0, side, one, 0)
        return expert_in(y, 1 - core, ss)

    gu_acc[...] = jnp.zeros_like(gu_acc)
    ss = expert_first(0, jnp.zeros((cap_rows, 1), F32))
    ss = lax.fori_loop(1, side, lambda d, ss: expert_second(d - 1, expert_first(d, ss)), ss)
    ss = expert_second(side - 1, ss)
    row_scale = lax.rsqrt(ss / width + EPS)
    g = gu_acc[:, :hid_e] * row_scale
    u = gu_acc[:, hid_e:] * row_scale
    hidden = (g / (1.0 + jnp.exp(-g)) * u).astype(BF16)
    loads[21].wait()
    for k in range(n):
        exp_part[k] = jnp.dot(hidden, ed[:, k * block:(k + 1) * block],
                              preferred_element_type=F32).astype(BF16)
    routed_sum = sum_over_tp(EXP_PAIR, EXP, exp_part, row_place, exp_pair, exp_sum, exp_in)

    far(FAR, dgu_all, me_x, along_x, 0, EARLY, 0, "wait")
    far(FAR, dgu_all, me_x, along_x, EARLY, late, 1, "wait")
    weights = dgu_all[...].reshape(side * block, 2 * hid_d)
    x = x_cat[...]
    for k in range(2 * hid_d // block):
        y = jnp.dot(x, weights[:, k * block:(k + 1) * block], preferred_element_type=F32)
        den_part[:, :, k * block:(k + 1) * block] = y.astype(BF16).reshape(side, rows, block)
    to_y_peers(DEN, lambda y: den_part.at[y], den_in.at[me_y])

    sums = await_y_peers(STA, sta_in, lambda y, acc: acc + sta_in[y], sta_out[me_y])
    dense_scale = lax.rsqrt(to_column(sums[0:1, :], rows) / width + EPS)
    branch = jax.nn.sigmoid(to_column(sums[1:2, :], rows) * dense_scale)
    y = await_y_peers(DEN, den_in, lambda y, acc: acc + den_in[y].astype(F32),
                      den_part[me_y].astype(F32)) * dense_scale
    g, u = y[:, :hid_d], y[:, hid_d:]
    hid_all[me_x] = (g / (1.0 + jnp.exp(-g)) * u * branch).astype(BF16)

    def spread_hidden(d, _):
        over(along_x(d), me_t, HID, hid_all.at[me_x], hid_all.at[me_x], me_x).start()
        return 0

    lax.fori_loop(1, side, spread_hidden, 0)

    far(FAR_DOWN, dd_all, me_y, along_y, 0, hid_d, 0, "wait")

    def hidden_of(d, _):
        x = lax.rem(me_x + side - d, side)
        over(along_x(-d), me_t, HID, hid_all.at[x], hid_all.at[x], x).wait_recv()
        return 0

    lax.fori_loop(1, side, hidden_of, 0)
    x = hid_all[...].reshape(quarter, hid_d)
    for k in range(side):
        y = jnp.dot(x, dd_all[k], preferred_element_type=F32)
        dwn_part[pl.ds(k * side, side)] = y.astype(BF16).reshape(side, rows, block)
    dense_sum = sum_over_tp(DWN_PAIR, DWN, dwn_part, row_place, dwn_pair, dwn_sum, dwn_in)

    y = summed_over_tp(EXP, exp_in, routed_sum)
    spot, col = iota((n * SLOT, cap_rows), 0), iota((n * SLOT, cap_rows), 1)
    within = jnp.bitwise_and(spot, SLOT - 1)
    shift = side.bit_length() - 1
    from_e = jnp.right_shift(spot, SLOT.bit_length() - 1)
    source = few_rows * jnp.bitwise_and(from_e, side - 1) + CAP * jnp.right_shift(from_e, shift) + within
    spread = jnp.where((source == col) & (within < CAP), 1.0, 0.0).astype(BF16)
    ret_out[...] = jnp.dot(spread, y.astype(BF16), preferred_element_type=F32).reshape(n, SLOT, block)

    def give_back(i, _):
        place = lax.rem(i + owned, n)
        column = side * lax.div(i, side) + lax.rem(owned, side)
        own = (column == me_e) & (place == me_t)

        @pl.when(jnp.logical_not(own))
        def _():
            over(column, place, RET, ret_out.at[i], ret_in.at[me_e], me_e).start()

        @pl.when(own)
        def _():
            ret_in[me_e] = ret_out[i]

        return 0

    lax.fori_loop(0, n, give_back, 0)

    def returned(e, _):
        source = lax.rem(e + final_cols, n)

        @pl.when((e != me_e) | (source != me_t))
        def _():
            over(e, source, RET, ret_in.at[e], ret_in.at[e], e).wait_recv()

        return 0

    lax.fori_loop(0, n, returned, 0)

    @pl.when(final_rows != me_e)
    def _():
        shares().wait()

    @pl.when(final_cols != me_e)
    def _():
        to_final().wait()

    routed = jnp.dot(ret_w_in[...], ret_in[...].reshape(n * SLOT, block), precision=HIGHEST,
                     preferred_element_type=F32)
    known = res_fin[...].astype(F32) + routed

    y = summed_over_tp(DWN, dwn_in, dense_sum)
    out_own[...] = (known + y).astype(BF16)

    def columns(j):
        return out.at[:, pl.ds(pl.multiple_of(j * block, block), block)]

    def publish(k, _):
        over(final_rows, 2 * chip(k) + core, OUT, out_own, columns(final_cols), final_cols).start()
        return 0

    lax.fori_loop(1, chips, publish, 0)

    @pl.when(final_rows != me_e)
    def _():
        over(final_rows, me_t, OUT, out_own, columns(final_cols), final_cols).start()

    @pl.when(final_rows == me_e)
    def _():
        out[:, pl.ds(pl.multiple_of(final_cols * block, block), block)] = out_own[...]

    def forward(k, _):
        j = lax.rem(2 * k + lax.rem(me_e + core, 2), n)
        source_e, source_t = side * me_y + lax.rem(j, side), lax.rem(me_e + j, n)

        @pl.when((source_e != me_e) | (source_t != me_t))
        def _():
            over(source_e, source_t, OUT, columns(j), columns(j), j).wait_recv()

        over(me_e, partner, OUT, columns(j), columns(j), j).start()
        return 0

    lax.fori_loop(0, chips, forward, 0)

    def finish(k, _):
        j = lax.rem(2 * k + lax.rem(me_e + core + 1, 2), n)
        over(me_e, partner, OUT, columns(j), columns(j), j).wait_recv()
        return 0

    lax.fori_loop(0, chips, finish, 0)
    rest = pl.ds(0, n - 1)
    sent(ep_copy, TOK, tok_all.at[rest])
    few = pl.ds(0, side - 1)
    sent(ep_copy, KEY, key_all.at[few])
    sent(ep_copy, QKV, qkv_part.at[rest])
    sent(ep_copy, MIX, mix_all.at[rest])
    some = pl.ds(0, chips - 1)
    sent(tp_copy, PRJ_PAIR, prj_pair)
    sent(tp_copy, PRJ, prj_sum.at[some])
    sent(ep_copy, ROW, row_in.at[pl.ds(0, 2 * n - 1)])
    sent(ep_copy, STA, sta_out.at[few])
    sent(ep_copy, DEN, den_part.at[few])
    sent(ep_copy, HID, hid_all.at[few])
    for phase, buffer, rows_of in (
        (NEAR, dgu_all, block), (FAR, dgu_all, block // 2),
        (NEAR_DOWN, dd_all, hid_d), (FAR_DOWN, dd_all, hid_d // 2)):
        sent(ep_copy, phase, buffer.at[pl.ds(0, 2), pl.ds(0, rows_of), :])
    sent(tp_copy, EXP_PAIR, exp_pair)
    sent(tp_copy, EXP, exp_sum.at[some])
    sent(tp_copy, DWN_PAIR, dwn_pair)
    sent(tp_copy, DWN, dwn_sum.at[some])

    @pl.when(final_rows != me_e)
    def _():
        sent(ep_copy, RET, ret_out)
        sent(ep_copy, RES, res_all)
        sent(ep_copy, OUT, res_all)

    @pl.when(final_rows == me_e)
    def _():
        sent(ep_copy, RET, ret_out.at[rest])
        sent(ep_copy, RES, res_all.at[rest])
        sent(ep_copy, OUT, res_all.at[rest])


def on_device(
    n, tokens, state_matrix, state_norm, state_max, mixer_gain, w_query, w_key, w_value, w_outgate,
    w_ingate, w_forget, forget_bias, w_proj, ffn_gain, w_branch, routes, route_weight,
    expert_gate, expert_up, expert_down, dense_gate, dense_up, dense_down,
):
    rows, width = tokens.shape
    head = state_norm.shape[-1]
    block = width // n
    hid_e, hid_d = expert_gate.shape[2], dense_gate.shape[1]
    cap_rows = CAP * n
    args = (
        tokens,
        state_matrix.reshape(rows, head, head),
        state_norm.reshape(rows, head),
        state_max.T,
        mixer_gain.reshape(1, width),
        w_query, w_key, w_value, w_outgate,
        w_ingate.T, w_forget.T,
        forget_bias.reshape(1, n),
        w_proj,
        ffn_gain.reshape(1, width),
        w_branch.reshape(width // 128, 128),
        routes.T, route_weight.T,
        expert_gate.reshape(width, hid_e), expert_up.reshape(width, hid_e),
        expert_down.reshape(hid_e, width),
        dense_gate, dense_up, dense_down,
    )
    vm = pltpu.VMEM
    dma = pltpu.SemaphoreType.DMA
    few_rows, side = CAP * math.isqrt(n), math.isqrt(n)

    def hier(tall):
        return [vm((n, tall, block), BF16)] + [vm((n // 2, tall, block), BF16)] * 3

    scratch = [
        vm((rows, width), BF16), vm((rows, head, head), F32), vm((rows, head), F32), vm((1, rows), F32),
        vm((1, width), F32), vm((block, 4 * head), BF16), vm((2 * n, width), BF16), vm((1, n), F32),
        vm((head, block), BF16), vm((1, width), F32), vm((width // 128, 128), BF16), vm((2, rows), jnp.int32),
        vm((2, rows), F32), vm((width, hid_e), BF16), vm((width, hid_e), BF16), vm((hid_e, width), BF16),
        vm((side, block, 2 * hid_d), BF16), vm((side, hid_d, block), BF16),
        vm((n, rows, block), BF16), vm((side, rows, 128), BF16),
        vm((n, rows, 4 * head), BF16), vm((n, rows, 4 * head), BF16),
        vm((n, rows, head), BF16), *hier(rows),
        vm((rows, block), BF16), vm((n, rows, block), BF16), vm((rows, block), BF16),
        vm((n, few_rows, side * block // 2), BF16), vm((2 * n, few_rows, side * block // 2), BF16),
        vm((side, 8, 128), F32), vm((side, 8, 128), F32),
        vm((side, rows, 2 * hid_d), BF16), vm((side, rows, 2 * hid_d), BF16),
        vm((side, rows, hid_d), BF16), *hier(rows), *hier(cap_rows),
        vm((n, SLOT, block), F32), vm((n, SLOT, block), F32), vm((rows, n * SLOT), F32),
        vm((rows, block), BF16),
        vm((width // 128, 128), F32),
        vm((n * few_rows, side * rows), BF16), vm((side * rows, side * block), BF16), vm((cap_rows, 2 * hid_e), F32), vm((rows, 2 * n), F32),
        vm((head, rows), F32), vm((head, rows), F32), vm((rows, head), F32), vm((rows, head), F32),
        vm((rows, head), F32), vm((rows, n * SLOT), F32),
        dma((len(args),)), dma((PHASES,)), dma((PHASES, 2 * n)), dma((2,)), dma((2,)),
    ]
    any_space = pl.BlockSpec(memory_space=pl.ANY)
    layer_out, new_matrix, new_norm, new_max = pl.pallas_call(
        functools.partial(layer_kernel, n),
        out_shape=(
            vm((rows, width), BF16), vm((rows, head, head), F32), vm((rows, head), F32), vm((1, rows), F32),
        ),
        in_specs=[any_space] * len(args),
        out_specs=[pl.BlockSpec(memory_space=vm)] * 4,
        scratch_shapes=scratch,
        compiler_params=pltpu.CompilerParams(
            collective_id=0, has_side_effects=True, vmem_limit_bytes=56 * 1024 * 1024),
        name="layer",
    )(*args)
    return (layer_out, new_matrix.reshape(rows, 1, head, head), new_norm.reshape(rows, 1, head), new_max.T)


def solution(mesh):
    n = mesh.shape["ep"]
    in_specs = (
        P("ep", None),
        P("ep", "tp", None, None),
        P("ep", "tp", None),
        P("ep", "tp"),
        P(),
        P("ep", "tp"),
        P("ep", "tp"),
        P("ep", "tp"),
        P("ep", "tp"),
        P(),
        P(),
        P(),
        P("tp", "ep"),
        P(),
        P(),
        P("ep", None),
        P("ep", None),
        P("ep", None, "tp"),
        P("ep", None, "tp"),
        P("ep", "tp", None),
        P("ep", "tp"),
        P("ep", "tp"),
        P("tp", "ep"),
    )
    out_specs = (P("ep", None), P("ep", "tp", None, None), P("ep", "tp", None), P("ep", "tp"))
    return jax.shard_map(
        functools.partial(on_device, n), mesh=mesh, in_specs=in_specs, out_specs=out_specs,
        check_vma=False)
```

```python
import functools
import math

import jax
import jax.numpy as jnp
from jax import lax
from jax.experimental import pallas as pl
from jax.experimental.pallas import tpu as pltpu
from jax.sharding import PartitionSpec as P

EPS = 1e-06
MESH = pl.DeviceIdType.MESH
CAP = 6
SLOT = 8
F32 = jnp.float32
BF16 = jnp.bfloat16
HIGHEST = lax.Precision.HIGHEST
NT = (((1,), (1,)), ((), ()))


def landing_spots(n):
    side = math.isqrt(n)
    many = {ROW: 2 * n, NEAR: 6, FAR: 6, NEAR_DOWN: 2, FAR_DOWN: 2, HID: side}
    for phase in (TOK, KEY, QKV, STA, DEN, RET, DWN, EXP):
        many[phase] = 1
    for phase in (DWN_PAIR, EXP_PAIR):
        many[phase] = n // 2
    first, at = [], 0
    for phase in range(PHASES):
        first.append(at)
        at += many.get(phase, n)
    return first, at


def iota(shape, dim):
    return lax.broadcasted_iota(jnp.int32, shape, dim)


def to_column(row, rows):
    diag = iota((rows, row.shape[1]), 0) == iota((rows, row.shape[1]), 1)
    return jnp.sum(jnp.where(diag, row, 0.0), axis=1, keepdims=True)


def to_row(column, lanes):
    rows = column.shape[0]
    diag = iota((rows, lanes), 0) == iota((rows, lanes), 1)
    return jnp.sum(jnp.where(diag, column, 0.0), axis=0, keepdims=True)


(TOK, KEY, QKV, MIX, PROJ, RES, ROW, STA, DEN, HID, DWN_PAIR, DWN, EXP_PAIR, EXP, RET,
 OUT, NEAR, FAR, NEAR_DOWN, FAR_DOWN) = range(20)
PHASES = 20
PARTS = ((0, 64), (64, 64), (128, 128))


def layer_kernel(
    n,
    tok_h, sm_h, sn_h, smax_h, mgain_h, wq_h, wk_h, wv_h, wo_h, win_h, wfo_h, fbias_h,
    wproj_h, fgain_h, wbr_h, routes_h, rw_h, eg_h, eu_h, ed_h, dg_h, du_h, dd_h,
    out, nm, nn, nmax,
    tok, sm, sn, smax, mgain, wqkv, wgates, fbias, proj_all, fgain, wbr, routes, rw,
    eg, eu, ed, dgu_all, dd_all,
    tok_all, key_all, qkv_part, qkv_in, mix_own, mix_in, res_own, res_all, res_fin,
    row_out, row_in, sta_out, sta_in, den_part, den_in, hid_all, dwn_part, dwn_pair, dwn_sum, dwn_in,
    exp_part, exp_pair, exp_sum, exp_in, ret_out, ret_in, ret_w_in, out_own,
    wbr_wide, pick, x_cat, hidden_e, gu_acc, gates, wkt, qt, vrow, keep_rows, numer, ret_w,
    load_sem, send_sem, recv_sem, share_sem, res_sem,
):
    me_e, me_t = lax.axis_index("ep"), lax.axis_index("tp")
    chips = n // 2
    first_spot, _ = landing_spots(n)
    side = math.isqrt(n)
    me_y, me_x = lax.div(me_e, side), lax.rem(me_e, side)
    me_z, core = lax.div(me_t, 2), lax.rem(me_t, 2)
    partner = me_t + 1 - 2 * core
    owned = lax.rem(me_t - me_e + n, n)
    final_rows = side * me_y + lax.rem(owned, side)
    final_cols = side * lax.div(owned, side) + me_x
    rows = tok.shape[0]
    width = tok.shape[1]
    block = width // n
    head = sn.shape[1]
    hid_e = eg.shape[1]
    hid_d = dd_all.shape[1]
    quarter = rows * side
    cap_rows = CAP * n
    few_rows = CAP * side
    dgu, dd = dgu_all.at[me_x], dd_all.at[me_y]

    loads = [
        (tok_h, tok), (mgain_h, mgain), (fgain_h, fgain), (wbr_h, wbr), (routes_h, routes),
        (rw_h, rw), (win_h, wgates.at[pl.ds(0, n), :]), (wfo_h, wgates.at[pl.ds(n, n), :]),
        (fbias_h, fbias), (smax_h, smax), (sn_h, sn),
        (wq_h, wqkv.at[:, pl.ds(0, head)]), (wk_h, wqkv.at[:, pl.ds(head, head)]),
        (wv_h, wqkv.at[:, pl.ds(2 * head, head)]), (wo_h, wqkv.at[:, pl.ds(3 * head, head)]),
        (sm_h, sm), (wproj_h, proj_all.at[me_t]), (dg_h, dgu_all.at[me_x, :, pl.ds(0, hid_d)]),
        (du_h, dgu_all.at[me_x, :, pl.ds(hid_d, hid_d)]), (eg_h, eg), (eu_h, eu), (ed_h, ed), (dd_h, dd),
    ]
    loads = [pltpu.make_async_copy(a, b, load_sem.at[k]) for k, (a, b) in enumerate(loads)]
    for copy in loads:
        copy.start()

    barrier = pltpu.get_barrier_semaphore()

    def greet(d, _):
        pl.semaphore_signal(barrier, 1, device_id=(lax.rem(me_e + d, n), me_t), device_id_type=MESH)
        pl.semaphore_signal(barrier, 1, device_id=(me_e, lax.rem(me_t + d, n)), device_id_type=MESH)
        return 0

    lax.fori_loop(1, n, greet, 0)
    pl.semaphore_wait(barrier, 2 * n - 2)

    def ep_copy(phase, src, dst, peer, landing):
        return pltpu.make_async_remote_copy(
            src_ref=src, dst_ref=dst, send_sem=send_sem.at[phase],
            recv_sem=recv_sem.at[first_spot[phase] + landing], device_id=(peer, me_t), device_id_type=MESH)

    def tp_copy(phase, src, dst, peer, landing):
        return pltpu.make_async_remote_copy(
            src_ref=src, dst_ref=dst, send_sem=send_sem.at[phase],
            recv_sem=recv_sem.at[first_spot[phase] + landing], device_id=(me_e, peer), device_id_type=MESH)

    def over(peer_e, peer_t, phase, src, dst, landing):
        return pltpu.make_async_remote_copy(
            src_ref=src, dst_ref=dst, send_sem=send_sem.at[phase],
            recv_sem=recv_sem.at[first_spot[phase] + landing], device_id=(peer_e, peer_t), device_id_type=MESH)

    def chip(k):
        k = chips - k
        return lax.rem(me_z + chips + lax.div(k + 1, 2) * (2 * lax.rem(k, 2) - 1), chips)

    def sum_over_tp(pair_phase, phase, part, place, pair, summed, arrived, make=None):
        def give(k, _):
            z = lax.rem(me_z + k, chips)
            at = place(2 * z + 1 - core)
            if make is not None:
                part[at] = make(at)
            tp_copy(pair_phase, part.at[at], pair.at[z], partner, z).start()
            return 0

        lax.fori_loop(1, chips + 1, give, 0)

        def add(z):
            at = place(2 * z + core)
            mine = part[at] if make is None else make(at)
            tp_copy(pair_phase, pair.at[z], pair.at[z], partner, z).wait_recv()
            return mine.astype(F32) + pair[z].astype(F32)

        def pass_on(k, _):
            z = chip(k)
            summed[z] = add(z).astype(BF16)
            tp_copy(phase, summed.at[z], arrived.at[me_z], 2 * z + core, 0).start()
            return 0

        lax.fori_loop(1, chips, pass_on, 0)
        return add(me_z)

    def summed_over_tp(phase, arrived, acc):
        await_blocks(phase, arrived.at[pl.ds(0, chips - 1)])
        return others(me_z, chips, arrived, acc)

    def give_projection():
        mine = proj_all.at[me_t]
        tp_copy(PROJ, mine, mine, partner, me_t).start()

        def give(k, _):
            tp_copy(PROJ, mine, mine, 2 * chip(k) + core, me_t).start()
            return 0

        lax.fori_loop(1, chips, give, 0)

    def pass_projection():
        def pass_on(k, _):
            t = 2 * chip(chips - k) + core
            part = proj_all.at[t]
            tp_copy(PROJ, part, part, t, t).wait_recv()
            tp_copy(PROJ, part, part, partner, t).start()
            return 0

        lax.fori_loop(1, chips, pass_on, 0)

    def take_projection():
        def take(z, _):
            t = 2 * z + 1 - core
            tp_copy(PROJ, proj_all.at[t], proj_all.at[t], partner, t).wait_recv()
            return 0

        lax.fori_loop(0, chips, take, 0)

    def along_x(step):
        return side * me_y + lax.rem(me_x + step + side, side)

    def along_y(step):
        return side * lax.rem(me_y + step + side, side) + me_x

    def weight_copy(phase, buffer, block_of, peer, first, many, landing):
        part = buffer.at[block_of, pl.ds(first, many), :]
        return over(peer, me_t, phase, part, part, landing)

    def near(phase, buffer, me, along, first, many, part):
        for way, step in enumerate((1, -1)):
            weight_copy(phase, buffer, me, along(step), first, many, 2 * part + way).start()

    def arrived_near(phase, buffer, me, along, first, many, part):
        for way, step in enumerate((-1, 1)):
            owner = lax.rem(me + step + side, side)
            weight_copy(phase, buffer, owner, along(step), first, many, 2 * part + way).wait_recv()

    def far(phase, buffer, me, along, first, many, part, act):
        half = many // 2
        for way, step in enumerate((1, -1)):
            if act == "start":
                owner = lax.rem(me - step + side, side)
                weight_copy(phase, buffer, owner, along(step), first + way * half, half, 2 * part + way).start()
            else:
                owner = lax.rem(me + 2, side)
                weight_copy(phase, buffer, owner, along(-step), first + way * half, half, 2 * part + way).wait_recv()

    def give_weights(part):
        near(NEAR, dgu_all, me_x, along_x, *PARTS[part], part)

    def pass_weights(part):
        arrived_near(NEAR, dgu_all, me_x, along_x, *PARTS[part], part)
        far(FAR, dgu_all, me_x, along_x, *PARTS[part], part, "start")

    def gather_quarter():
        to_e = side * me_y + lax.rem(owned, side)
        spot = me_x * side + lax.div(owned, side)

        def give(k, _):
            over(to_e, 2 * chip(k) + core, RES, res_own, res_all.at[spot], spot).start()
            return 0

        lax.fori_loop(1, chips, give, 0)

        @pl.when(to_e != me_e)
        def _():
            over(to_e, me_t, RES, res_own, res_all.at[spot], spot).start()

        @pl.when(to_e == me_e)
        def _():
            res_all[spot] = res_own[...]

        pass_weights(2)
        arrived_near(NEAR_DOWN, dd_all, me_y, along_y, 0, hid_d, 0)
        far(FAR_DOWN, dd_all, me_y, along_y, 0, hid_d, 0, "start")

        def source(spot):
            o = side * lax.rem(spot, side) + me_x
            j = side * me_y + lax.div(spot, side)
            return j, lax.rem(o + j, n)

        def spot_of(k, parity):
            return (2 * lax.rem(k, 2) + parity) * side + lax.div(k, 2)

        def pass_on(k, _):
            spot = spot_of(k, lax.rem(core + me_x, 2))
            j, t = source(spot)

            @pl.when((j != me_e) | (t != me_t))
            def _():
                over(j, t, RES, res_all.at[spot], res_all.at[spot], spot).wait_recv()

            over(me_e, partner, RES, res_all.at[spot], res_all.at[spot], spot).start()
            return 0

        lax.fori_loop(0, n // 2, pass_on, 0)

        def take(k, _):
            spot = spot_of(k, lax.rem(core + me_x + 1, 2))
            over(me_e, partner, RES, res_all.at[spot], res_all.at[spot], spot).wait_recv()
            return 0

        lax.fori_loop(0, n // 2, take, 0)

    def row_place(t):
        return lax.rem(t - me_e + n, n)

    def to_peers(copy, me, phase, src_of, dst):
        def one(d, _):
            peer = lax.rem(me + d, n)
            copy(phase, src_of(peer), dst, peer, me).start()
            return 0

        lax.fori_loop(1, n, one, 0)

    def await_peers(copy, me, phase, buffer, use=None, carry=0):
        def one(d, carry):
            peer = lax.rem(me + n - d, n)
            copy(phase, buffer.at[peer], buffer.at[peer], peer, peer).wait_recv()
            return carry if use is None else use(peer, carry)

        return lax.fori_loop(1, n, one, carry)

    def to_y_peers(phase, src_of, dst):
        def one(d, _):
            y = lax.rem(me_y + d, side)
            over(side * y + me_x, me_t, phase, src_of(y), dst, 0).start()
            return 0

        lax.fori_loop(1, side, one, 0)

    def steps(far_first):
        offsets = [(dy, dx) for dy in range(side) for dx in range(side) if dy or dx]
        cross = lambda o: sum(min(d, side - d) for d in o)
        return sorted(offsets, key=cross, reverse=far_first)

    def ep_at(dy, dx):
        return side * lax.rem(me_y + dy, side) + lax.rem(me_x + dx, side)

    def to_ep_peers(phase, src_of, dst):
        for dy, dx in steps(True):
            peer = ep_at(dy, dx)
            ep_copy(phase, src_of(peer), dst, peer, 0).start()

    def await_blocks(phase, blocks):
        over(me_e, partner, phase, blocks, blocks, 0).wait_recv()

    def others(me, many, buffer, acc):
        def one(d, acc):
            return acc + buffer[lax.rem(me + d, many)].astype(F32)

        return lax.fori_loop(1, many, one, acc)

    rest, few = pl.ds(0, n - 1), pl.ds(0, side - 1)
    far_first = (2, 1, 3, 0) if side == 4 else tuple(range(side))

    def sent(copy, phase, many):
        copy(phase, many, many, 0, 0).wait_send()

    loads[0].wait()
    to_ep_peers(TOK,
             lambda peer: tok.at[:, pl.ds(pl.multiple_of(peer * block, block), block)],
             tok_all.at[me_e])
    tok_all[me_e] = tok[:, pl.ds(pl.multiple_of(me_e * block, block), block)]

    loads[16].wait()
    give_projection()
    loads[17].wait()
    loads[18].wait()
    give_weights(0)

    loads[4].wait()
    loads[5].wait()
    route_rows = [routes[pl.ds(k, 1), :] for k in range(2)]
    lanes_e = iota((128, rows), 0)
    named = sum(jnp.where(lanes_e == r, 1.0, 0.0) for r in route_rows)
    earlier = jnp.where(iota((rows, rows), 0) < iota((rows, rows), 1), 1.0, 0.0)
    before = jnp.dot(named.astype(BF16), earlier.astype(BF16), preferred_element_type=F32)
    base = (CAP * me_y).astype(F32)
    key = jnp.where(named > 0.0, before + base, -1.0)
    eye = jnp.where(iota((rows, rows), 0) == iota((rows, rows), 1), 1.0, 0.0)
    key_all[me_y] = lax.dot_general(
        eye.astype(BF16), key.astype(BF16), NT, preferred_element_type=F32).astype(BF16)
    to_y_peers(KEY, lambda y: key_all.at[me_y], key_all.at[me_y])
    weights = [rw[pl.ds(k, 1), :] for k in range(2)]
    total = weights[0] + weights[1]
    spots = iota((n * SLOT, rows), 0)
    share_t = jnp.zeros((n * SLOT, rows), F32)
    for r, w in zip(route_rows, weights):
        slot = jnp.sum(jnp.where(lanes_e == r, before, 0.0), axis=0, keepdims=True)
        hit = (spots.astype(F32) == r.astype(F32) * SLOT + slot)
        share_t = share_t + jnp.where(hit, w / total, 0.0)
    ret_w[...] = lax.dot_general(eye, share_t, NT, precision=HIGHEST, preferred_element_type=F32)

    def shares():
        return pltpu.make_async_remote_copy(
            src_ref=ret_w, dst_ref=ret_w_in, send_sem=share_sem.at[0], recv_sem=share_sem.at[1],
            device_id=(final_rows, me_t), device_id_type=MESH)

    @pl.when(final_rows != me_e)
    def _():
        shares().start()

    @pl.when(final_rows == me_e)
    def _():
        ret_w_in[...] = ret_w[...]

    loads[1].wait()
    squares = jnp.zeros((rows, block), F32)
    for k in range(n):
        part = tok[:, k * block:(k + 1) * block].astype(F32)
        squares = squares + part * part
    scale = lax.rsqrt(jnp.sum(squares, axis=1, keepdims=True) / width + EPS)
    loads[6].wait()
    loads[7].wait()
    gate = jnp.zeros((rows, 2 * n), F32)
    for k in range(n):
        cols = slice(k * block, (k + 1) * block)
        gain = mgain[:, cols]
        normed = (tok[:, cols].astype(F32) * scale * gain).astype(BF16)
        gate = gate + lax.dot_general(normed, wgates[:, cols], NT, preferred_element_type=F32)
    for k in range(8, 11):
        loads[k].wait()
    lane = iota((rows, 2 * n), 1)
    gate_in = jnp.sum(jnp.where(lane == me_t, gate, 0.0), axis=1, keepdims=True)
    gate_forget = jnp.sum(jnp.where(lane == me_t + n, gate, 0.0), axis=1, keepdims=True)
    bias = jnp.sum(jnp.where(iota((1, n), 1) == me_t, fbias[...], 0.0), axis=1, keepdims=True)
    gate_forget = gate_forget + bias
    log_keep = jnp.minimum(gate_forget, 0.0) - jnp.log1p(jnp.exp(-jnp.abs(gate_forget)))
    old_max = to_column(smax[...], rows)
    new_max = jnp.maximum(log_keep + old_max, gate_in)
    keep = jnp.exp(log_keep + old_max - new_max)
    write = jnp.exp(gate_in - new_max)
    nmax[...] = to_row(new_max, rows)

    await_blocks(TOK, tok_all.at[rest])
    for k in range(11, 15):
        loads[k].wait()
    gain_m = mgain[:, pl.ds(pl.multiple_of(me_e * block, block), block)]

    def project(dy):
        at = pl.multiple_of(side * lax.rem(me_y + dy, side), side)
        x = tok_all[pl.ds(at, side)].reshape(quarter, block).astype(F32) * gain_m
        y = jnp.dot(x.astype(BF16), wqkv[...], preferred_element_type=F32)
        qkv_part[pl.ds(at, side)] = y.astype(BF16).reshape(side, rows, 4 * head)
        for dx in far_first:
            if dy or dx:
                peer = ep_at(dy, dx)
                ep_copy(QKV, qkv_part.at[peer], qkv_in.at[me_e], peer, 0).start()

    for dy in far_first:
        project(dy)
    give_weights(1)

    loads[15].wait()
    await_blocks(QKV, qkv_in.at[rest])
    y = others(me_e, n, qkv_in, qkv_part[me_e].astype(F32)) * scale
    query = y[:, :head]
    keys = y[:, head:2 * head] * head ** (-0.5)
    value = y[:, 2 * head:3 * head]
    outgate = y[:, 3 * head:]
    written = write * keys
    new_norm = keep * sn[...] + written
    nn[...] = new_norm
    denom = jnp.sum(query * new_norm, axis=1, keepdims=True)
    qt[...] = query.T
    wkt[...] = written.T
    vrow[...] = value
    keep_rows[...] = jnp.broadcast_to(keep, (rows, head))
    for b in range(rows):
        numer[pl.ds(b, 1), :] = jnp.sum(qt[:, b:b + 1] * sm[b], axis=0, keepdims=True)
    dots = jnp.sum(query * written, axis=1, keepdims=True)
    num = keep * numer[...] + dots * value
    cell = num / jnp.maximum(jnp.abs(denom), 1.0)
    mix_own[...] = (jax.nn.sigmoid(outgate) * cell).astype(BF16)

    def head_place(h):
        return mix_in.at[:, pl.ds(pl.multiple_of(h * head, head), head)]

    for dy, dx in steps(True):
        j = ep_at(dy, dx)
        over(j, lax.rem(me_e + j, n), MIX, mix_own, head_place(me_t), me_t).start()

    @pl.when(owned != me_e)
    def _():
        over(me_e, lax.rem(2 * me_e, n), MIX, mix_own, head_place(me_t), me_t).start()

    @pl.when(owned == me_e)
    def _():
        mix_in[:, pl.ds(pl.multiple_of(me_t * head, head), head)] = mix_own[...]

    give_weights(2)
    loads[22].wait()
    near(NEAR_DOWN, dd_all, me_y, along_y, 0, hid_d, 0)
    pass_projection()
    pass_weights(0)
    pass_weights(1)
    for b in range(rows):
        nm[b] = keep_rows[pl.ds(b, 1), :] * sm[b] + wkt[:, b:b + 1] * vrow[pl.ds(b, 1), :]

    await_blocks(KEY, key_all.at[few])
    key_t = lax.dot_general(
        jnp.where(iota((n, 128), 0) == iota((n, 128), 1), 1.0, 0.0).astype(BF16),
        key_all[...].reshape(quarter, 128), NT, preferred_element_type=F32)
    places = iota((few_rows, quarter), 0).astype(F32)
    for e in range(0, n, 2):
        both = [jnp.where(places == key_t[k:k + 1, :], 1.0, 0.0) for k in (e, e + 1)]
        pick[pl.ds(e * few_rows, 2 * few_rows), :] = jnp.concatenate(both, axis=0).astype(BF16)

    take_projection()

    def head_in(h, _):
        @pl.when((owned != me_e) | (h != me_t))
        def _():
            over(owned, h, MIX, head_place(h), head_place(h), h).wait_recv()

        return 0

    lax.fori_loop(0, n, head_in, 0)
    mixed = jnp.dot(mix_in[...], proj_all[...].reshape(n * head, block), preferred_element_type=F32)
    residual = (tok_all[owned].astype(F32) + mixed).astype(BF16)
    res_own[...] = residual

    def to_final():
        return pltpu.make_async_remote_copy(
            src_ref=res_own, dst_ref=res_fin, send_sem=res_sem.at[0], recv_sem=res_sem.at[1],
            device_id=(final_cols, me_t), device_id_type=MESH)

    gather_quarter()

    @pl.when(final_cols != me_e)
    def _():
        to_final().start()

    @pl.when(final_cols == me_e)
    def _():
        res_fin[...] = res_own[...]

    loads[2].wait()
    loads[3].wait()

    def pass_rows(peer):
        spot = core * n + peer
        tp_copy(ROW, row_in.at[spot], row_in.at[spot], partner, spot).start()

    half_side = side // 2
    res_half = jnp.concatenate(
        [res_all[pl.ds((core * half_side + k) * side, side)].reshape(quarter, block)
         for k in range(half_side)], axis=1)

    def dispatch(dy):
        at = pl.multiple_of(side * lax.rem(me_y + dy, side), side)
        y = jnp.dot(pick[pl.ds(pl.multiple_of(at * few_rows, side * few_rows), side * few_rows), :],
                    res_half, preferred_element_type=F32)
        row_out[pl.ds(at, side)] = y.reshape(side, few_rows, half_side * block).astype(BF16)
        for dx in far_first:
            if dy or dx:
                peer, spot = ep_at(dy, dx), core * n + me_e
                ep_copy(ROW, row_out.at[peer], row_in.at[spot], peer, spot).start()

    for dy in far_first:
        dispatch(dy)
    row_in[core * n + me_e] = row_out[me_e]
    pass_rows(me_e)

    wbr_wide[...] = wbr[...].astype(F32)
    lines = block // 128
    squares = [jnp.zeros((rows, 1), F32)] * side
    branches = [jnp.zeros((rows, 1), F32)] * side
    for k in range(side):
        j = side * me_y + k
        gain_f = fgain[:, pl.ds(pl.multiple_of(j * block, block), block)]
        gain_b = gain_f * jnp.concatenate(
            [wbr_wide[pl.ds(j * lines + i, 1), :] for i in range(lines)], axis=1)
        for g in range(side):
            r = res_all[k * side + g].astype(F32)
            squares[g] = squares[g] + jnp.sum(r * r, axis=1, keepdims=True)
            branches[g] = branches[g] + jnp.sum(r * gain_b, axis=1, keepdims=True)
            x_cat[pl.ds(g * rows, rows), k * block:(k + 1) * block] = (r * gain_f).astype(BF16)
    for g in range(side):
        sta_out[g] = jnp.where(iota((8, 128), 0) == 0, to_row(squares[g], 128), to_row(branches[g], 128))
    to_y_peers(STA, lambda y: sta_out.at[y], sta_in.at[me_y])

    for part, (first, many) in enumerate(PARTS):
        far(FAR, dgu_all, me_x, along_x, first, many, part, "wait")
    weights = dgu_all[...].reshape(side * block, 2 * hid_d)
    x = x_cat[...]
    for k in range(2 * hid_d // block):
        y = jnp.dot(x, weights[:, k * block:(k + 1) * block], preferred_element_type=F32)
        den_part[:, :, k * block:(k + 1) * block] = y.astype(BF16).reshape(side, rows, block)
    to_y_peers(DEN, lambda y: den_part.at[y], den_in.at[me_y])

    loads[19].wait()
    loads[20].wait()

    deep = half_side * block

    def expert_in(y, half, ss):
        x = row_in[pl.ds(half * n + y * side, side)].astype(F32).reshape(cap_rows, deep)
        at = pl.multiple_of(y * side * block + half * deep, deep)
        xg = (x * fgain[:, pl.ds(at, deep)]).astype(BF16)
        gu_acc[:, pl.ds(0, hid_e)] += jnp.dot(xg, eg[pl.ds(at, deep), :], preferred_element_type=F32)
        gu_acc[:, pl.ds(hid_e, hid_e)] += jnp.dot(xg, eu[pl.ds(at, deep), :], preferred_element_type=F32)
        return ss + jnp.sum(x * x, axis=1, keepdims=True)

    def expert_first(d, ss):
        y = lax.rem(me_y + side - d, side)

        def one(k, _):
            peer = side * y + lax.rem(me_x + k, side)
            spot = core * n + peer

            @pl.when(peer != me_e)
            def _():
                ep_copy(ROW, row_in.at[spot], row_in.at[spot], peer, spot).wait_recv()
                pass_rows(peer)

            return 0

        lax.fori_loop(0, side, one, 0)
        return expert_in(y, core, ss)

    def expert_second(d, ss):
        y = lax.rem(me_y + side - d, side)

        def one(k, _):
            other = (1 - core) * n + side * y + k
            tp_copy(ROW, row_in.at[other], row_in.at[other], partner, other).wait_recv()
            return 0

        lax.fori_loop(0, side, one, 0)
        return expert_in(y, 1 - core, ss)

    gu_acc[...] = jnp.zeros_like(gu_acc)
    ss = expert_first(0, jnp.zeros((cap_rows, 1), F32))
    ss = lax.fori_loop(1, side, lambda d, ss: expert_second(d - 1, expert_first(d, ss)), ss)
    ss = expert_second(side - 1, ss)
    row_scale = lax.rsqrt(ss / width + EPS)
    g = gu_acc[:, :hid_e] * row_scale
    u = gu_acc[:, hid_e:] * row_scale
    hidden_e[...] = (g / (1.0 + jnp.exp(-g)) * u).astype(BF16)
    loads[21].wait()

    def expert_out(at):
        return jnp.dot(hidden_e[...], ed[:, pl.ds(pl.multiple_of(at * block, block), block)],
                       preferred_element_type=F32).astype(BF16)

    routed_sum = sum_over_tp(
        EXP_PAIR, EXP, exp_part, row_place, exp_pair, exp_sum, exp_in, expert_out)

    await_blocks(STA, sta_in.at[few])
    sums = others(me_y, side, sta_in, sta_out[me_y])
    dense_scale = lax.rsqrt(to_column(sums[0:1, :], rows) / width + EPS)
    branch = jax.nn.sigmoid(to_column(sums[1:2, :], rows) * dense_scale)
    await_blocks(DEN, den_in.at[few])
    y = others(me_y, side, den_in, den_part[me_y].astype(F32)) * dense_scale
    g, u = y[:, :hid_d], y[:, hid_d:]
    hid_all[me_x] = (g / (1.0 + jnp.exp(-g)) * u * branch).astype(BF16)

    def spread_hidden(d, _):
        over(along_x(d), me_t, HID, hid_all.at[me_x], hid_all.at[me_x], me_x).start()
        return 0

    lax.fori_loop(1, side, spread_hidden, 0)

    far(FAR_DOWN, dd_all, me_y, along_y, 0, hid_d, 0, "wait")

    def hidden_of(d, _):
        x = lax.rem(me_x + side - d, side)
        over(along_x(-d), me_t, HID, hid_all.at[x], hid_all.at[x], x).wait_recv()
        return 0

    lax.fori_loop(1, side, hidden_of, 0)
    x = hid_all[...].reshape(quarter, hid_d)
    for k in range(side):
        y = jnp.dot(x, dd_all[k], preferred_element_type=F32)
        dwn_part[pl.ds(k * side, side)] = y.astype(BF16).reshape(side, rows, block)
    dense_sum = sum_over_tp(DWN_PAIR, DWN, dwn_part, row_place, dwn_pair, dwn_sum, dwn_in)

    y = summed_over_tp(EXP, exp_in, routed_sum)
    spot, col = iota((n * SLOT, cap_rows), 0), iota((n * SLOT, cap_rows), 1)
    within = jnp.bitwise_and(spot, SLOT - 1)
    shift = side.bit_length() - 1
    from_e = jnp.right_shift(spot, SLOT.bit_length() - 1)
    source = few_rows * jnp.bitwise_and(from_e, side - 1) + CAP * jnp.right_shift(from_e, shift) + within
    spread = jnp.where((source == col) & (within < CAP), 1.0, 0.0).astype(BF16)
    ret_out[...] = jnp.dot(
        spread, y.astype(BF16), preferred_element_type=F32).reshape(n, SLOT, block).astype(BF16)

    def give_back(i, _):
        place = lax.rem(i + owned, n)
        column = side * lax.div(i, side) + lax.rem(owned, side)
        own = (column == me_e) & (place == me_t)

        @pl.when(jnp.logical_not(own))
        def _():
            over(column, place, RET, ret_out.at[i], ret_in.at[me_e], 0).start()

        @pl.when(own)
        def _():
            ret_in[me_e] = ret_out[i]

        return 0

    lax.fori_loop(0, n, give_back, 0)

    @pl.when(final_rows != me_e)
    def _():
        await_blocks(RET, ret_in)

    @pl.when(final_rows == me_e)
    def _():
        await_blocks(RET, ret_in.at[rest])

    @pl.when(final_rows != me_e)
    def _():
        shares().wait()

    @pl.when(final_cols != me_e)
    def _():
        to_final().wait()

    routed = jnp.dot(ret_w_in[...], ret_in[...].astype(F32).reshape(n * SLOT, block), precision=HIGHEST,
                     preferred_element_type=F32)
    known = res_fin[...].astype(F32) + routed

    y = summed_over_tp(DWN, dwn_in, dense_sum)
    out_own[...] = (known + y).astype(BF16)

    def columns(j):
        return out.at[:, pl.ds(pl.multiple_of(j * block, block), block)]

    def publish(k, _):
        over(final_rows, 2 * chip(k) + core, OUT, out_own, columns(final_cols), final_cols).start()
        return 0

    lax.fori_loop(1, chips, publish, 0)

    @pl.when(final_rows != me_e)
    def _():
        over(final_rows, me_t, OUT, out_own, columns(final_cols), final_cols).start()

    @pl.when(final_rows == me_e)
    def _():
        out[:, pl.ds(pl.multiple_of(final_cols * block, block), block)] = out_own[...]

    def forward(k, _):
        j = lax.rem(2 * k + lax.rem(me_e + core, 2), n)
        source_e, source_t = side * me_y + lax.rem(j, side), lax.rem(me_e + j, n)

        @pl.when((source_e != me_e) | (source_t != me_t))
        def _():
            over(source_e, source_t, OUT, columns(j), columns(j), j).wait_recv()

        over(me_e, partner, OUT, columns(j), columns(j), j).start()
        return 0

    lax.fori_loop(0, chips, forward, 0)

    def finish(k, _):
        j = lax.rem(2 * k + lax.rem(me_e + core + 1, 2), n)
        over(me_e, partner, OUT, columns(j), columns(j), j).wait_recv()
        return 0

    lax.fori_loop(0, chips, finish, 0)
    sent(ep_copy, TOK, tok_all.at[rest])
    sent(ep_copy, KEY, key_all.at[few])
    sent(ep_copy, QKV, qkv_part.at[rest])
    some = pl.ds(0, chips - 1)

    @pl.when(owned != me_e)
    def _():
        sent(ep_copy, MIX, mix_in)

    @pl.when(owned == me_e)
    def _():
        sent(ep_copy, MIX, mix_in.at[:, pl.ds(0, (n - 1) * head)])

    sent(tp_copy, PROJ, proj_all.at[rest])
    sent(ep_copy, ROW, row_in.at[pl.ds(0, 2 * n - 1)])
    sent(ep_copy, STA, sta_out.at[few])
    sent(ep_copy, DEN, den_part.at[few])
    sent(ep_copy, HID, hid_all.at[few])
    for phase, buffer, rows_of in (
        (NEAR, dgu_all, block), (FAR, dgu_all, block // 2),
        (NEAR_DOWN, dd_all, hid_d), (FAR_DOWN, dd_all, hid_d // 2)):
        sent(ep_copy, phase, buffer.at[pl.ds(0, 2), pl.ds(0, rows_of), :])
    sent(tp_copy, EXP_PAIR, exp_pair)
    sent(tp_copy, EXP, exp_sum.at[some])
    sent(tp_copy, DWN_PAIR, dwn_pair)
    sent(tp_copy, DWN, dwn_sum.at[some])

    @pl.when(final_rows != me_e)
    def _():
        sent(ep_copy, RET, ret_out)
        sent(ep_copy, RES, res_all)
        sent(ep_copy, OUT, res_all)

    @pl.when(final_rows == me_e)
    def _():
        sent(ep_copy, RET, ret_out.at[rest])
        sent(ep_copy, RES, res_all.at[rest])
        sent(ep_copy, OUT, res_all.at[rest])


def on_device(
    n, tokens, state_matrix, state_norm, state_max, mixer_gain, w_query, w_key, w_value, w_outgate,
    w_ingate, w_forget, forget_bias, w_proj, ffn_gain, w_branch, routes, route_weight,
    expert_gate, expert_up, expert_down, dense_gate, dense_up, dense_down,
):
    rows, width = tokens.shape
    head = state_norm.shape[-1]
    block = width // n
    hid_e, hid_d = expert_gate.shape[2], dense_gate.shape[1]
    cap_rows = CAP * n
    args = (
        tokens,
        state_matrix.reshape(rows, head, head),
        state_norm.reshape(rows, head),
        state_max.T,
        mixer_gain.reshape(1, width),
        w_query, w_key, w_value, w_outgate,
        w_ingate.T, w_forget.T,
        forget_bias.reshape(1, n),
        w_proj,
        ffn_gain.reshape(1, width),
        w_branch.reshape(width // 128, 128),
        routes.T, route_weight.T,
        expert_gate.reshape(width, hid_e), expert_up.reshape(width, hid_e),
        expert_down.reshape(hid_e, width),
        dense_gate, dense_up, dense_down,
    )
    vm = pltpu.VMEM
    dma = pltpu.SemaphoreType.DMA
    few_rows, side = CAP * math.isqrt(n), math.isqrt(n)

    def hier(tall):
        return [vm((n, tall, block), BF16)] + [vm((n // 2, tall, block), BF16)] * 3

    scratch = [
        vm((rows, width), BF16), vm((rows, head, head), F32), vm((rows, head), F32), vm((1, rows), F32),
        vm((1, width), F32), vm((block, 4 * head), BF16), vm((2 * n, width), BF16), vm((1, n), F32),
        vm((n, head, block), BF16), vm((1, width), F32), vm((width // 128, 128), BF16), vm((2, rows), jnp.int32),
        vm((2, rows), F32), vm((width, hid_e), BF16), vm((width, hid_e), BF16), vm((hid_e, width), BF16),
        vm((side, block, 2 * hid_d), BF16), vm((side, hid_d, block), BF16),
        vm((n, rows, block), BF16), vm((side, rows, 128), BF16),
        vm((n, rows, 4 * head), BF16), vm((n, rows, 4 * head), BF16),
        vm((rows, head), BF16), vm((rows, n * head), BF16),
        vm((rows, block), BF16), vm((n, rows, block), BF16), vm((rows, block), BF16),
        vm((n, few_rows, side * block // 2), BF16), vm((2 * n, few_rows, side * block // 2), BF16),
        vm((side, 8, 128), F32), vm((side, 8, 128), F32),
        vm((side, rows, 2 * hid_d), BF16), vm((side, rows, 2 * hid_d), BF16),
        vm((side, rows, hid_d), BF16), *hier(rows), *hier(cap_rows),
        vm((n, SLOT, block), BF16), vm((n, SLOT, block), BF16), vm((rows, n * SLOT), F32),
        vm((rows, block), BF16),
        vm((width // 128, 128), F32),
        vm((n * few_rows, side * rows), BF16), vm((side * rows, side * block), BF16), vm((cap_rows, hid_e), BF16), vm((cap_rows, 2 * hid_e), F32), vm((rows, 2 * n), F32),
        vm((head, rows), F32), vm((head, rows), F32), vm((rows, head), F32), vm((rows, head), F32),
        vm((rows, head), F32), vm((rows, n * SLOT), F32),
        dma((len(args),)), dma((PHASES,)), dma((landing_spots(n)[1],)), dma((2,)), dma((2,)),
    ]
    any_space = pl.BlockSpec(memory_space=pl.ANY)
    layer_out, new_matrix, new_norm, new_max = pl.pallas_call(
        functools.partial(layer_kernel, n),
        out_shape=(
            vm((rows, width), BF16), vm((rows, head, head), F32), vm((rows, head), F32), vm((1, rows), F32),
        ),
        in_specs=[any_space] * len(args),
        out_specs=[pl.BlockSpec(memory_space=vm)] * 4,
        scratch_shapes=scratch,
        compiler_params=pltpu.CompilerParams(
            collective_id=0, has_side_effects=True, vmem_limit_bytes=56 * 1024 * 1024),
        name="layer",
    )(*args)
    return (layer_out, new_matrix.reshape(rows, 1, head, head), new_norm.reshape(rows, 1, head), new_max.T)


def solution(mesh):
    n = mesh.shape["ep"]
    in_specs = (
        P("ep", None),
        P("ep", "tp", None, None),
        P("ep", "tp", None),
        P("ep", "tp"),
        P(),
        P("ep", "tp"),
        P("ep", "tp"),
        P("ep", "tp"),
        P("ep", "tp"),
        P(),
        P(),
        P(),
        P("tp", "ep"),
        P(),
        P(),
        P("ep", None),
        P("ep", None),
        P("ep", None, "tp"),
        P("ep", None, "tp"),
        P("ep", "tp", None),
        P("ep", "tp"),
        P("ep", "tp"),
        P("tp", "ep"),
    )
    out_specs = (P("ep", None), P("ep", "tp", None, None), P("ep", "tp", None), P("ep", "tp"))
    return jax.shard_map(
        functools.partial(on_device, n), mesh=mesh, in_specs=in_specs, out_specs=out_specs,
        check_vma=False)
```

```python
import functools
import math

import jax
import jax.numpy as jnp
from jax import lax
from jax.experimental import pallas as pl
from jax.experimental.pallas import tpu as pltpu
from jax.sharding import PartitionSpec as P

EPS = 1e-06
MESH = pl.DeviceIdType.MESH
CAP = 6
SLOT = 8
F32 = jnp.float32
BF16 = jnp.bfloat16
HIGHEST = lax.Precision.HIGHEST
NT = (((1,), (1,)), ((), ()))


def landing_spots(n):
    side = math.isqrt(n)
    many = {ROW: n + side, RES: n + 1, NEAR: 6, FAR: 6, NEAR_DOWN: 2, FAR_DOWN: 2, HID: side}
    for phase in (TOK, KEY, QKV, STA, DEN, RET, MIX, DWN, DWN_PAIR, EXP):
        many[phase] = 1
    many[EXP_PAIR] = n // 2
    many[PROJ] = many[OUT] = n // 2 + 1
    first, at = [], 0
    for phase in range(PHASES):
        first.append(at)
        at += many.get(phase, n)
    return first, at


def iota(shape, dim):
    return lax.broadcasted_iota(jnp.int32, shape, dim)


def to_column(row, rows):
    diag = iota((rows, row.shape[1]), 0) == iota((rows, row.shape[1]), 1)
    return jnp.sum(jnp.where(diag, row, 0.0), axis=1, keepdims=True)


def to_row(column, lanes):
    rows = column.shape[0]
    diag = iota((rows, lanes), 0) == iota((rows, lanes), 1)
    return jnp.sum(jnp.where(diag, column, 0.0), axis=0, keepdims=True)


(TOK, KEY, QKV, MIX, PROJ, RES, ROW, STA, DEN, HID, DWN_PAIR, DWN, EXP_PAIR, EXP, RET,
 OUT, NEAR, FAR, NEAR_DOWN, FAR_DOWN) = range(20)
PHASES = 20
PARTS = ((0, 64), (64, 64), (128, 128))


def layer_kernel(
    n,
    tok_h, sm_h, sn_h, smax_h, mgain_h, wq_h, wk_h, wv_h, wo_h, win_h, wfo_h, fbias_h,
    wproj_h, fgain_h, wbr_h, routes_h, rw_h, eg_h, eu_h, ed_h, dg_h, du_h, dd_h,
    out, nm, nn, nmax,
    tok, sm, sn, smax, mgain, wqkv, wgates, fbias, proj_all, fgain, wbr, routes, rw,
    eg, eu, ed, dgu_all, dd_all,
    tok_all, key_all, qkv_part, qkv_in, mix_own, mix_in, res_own, res_all, res_fin,
    row_out, row_in, sta_out, sta_in, den_part, den_in, hid_all, dwn_part, dwn_pair, dwn_sum, dwn_in,
    exp_part, exp_pair, exp_sum, exp_in, ret_out, ret_in, out_own,
    wbr_wide, pick, x_cat, hidden_e, gu_acc, gates, wkt, qt, vrow, keep_rows, numer, ret_w,
    load_sem, send_sem, recv_sem, res_sem,
):
    me_e, me_t = lax.axis_index("ep"), lax.axis_index("tp")
    chips = n // 2
    first_spot, _ = landing_spots(n)
    side = math.isqrt(n)
    me_y, me_x = lax.div(me_e, side), lax.rem(me_e, side)
    me_z, core = lax.div(me_t, 2), lax.rem(me_t, 2)
    partner = me_t + 1 - 2 * core
    owned = lax.rem(me_t - me_e + n, n)
    rows = tok.shape[0]
    width = tok.shape[1]
    block = width // n
    head = sn.shape[1]
    hid_e = eg.shape[1]
    hid_d = dd_all.shape[1]
    quarter = rows * side
    cap_rows = CAP * n
    few_rows = CAP * side
    dgu, dd = dgu_all.at[me_x], dd_all.at[me_y]

    loads = [
        (tok_h, tok), (mgain_h, mgain), (fgain_h, fgain), (wbr_h, wbr), (routes_h, routes),
        (rw_h, rw), (win_h, wgates.at[pl.ds(0, n), :]), (wfo_h, wgates.at[pl.ds(n, n), :]),
        (fbias_h, fbias), (smax_h, smax), (sn_h, sn),
        (wq_h, wqkv.at[:, pl.ds(0, head)]), (wk_h, wqkv.at[:, pl.ds(head, head)]),
        (wv_h, wqkv.at[:, pl.ds(2 * head, head)]), (wo_h, wqkv.at[:, pl.ds(3 * head, head)]),
        (sm_h, sm), (wproj_h, proj_all.at[me_t]), (dg_h, dgu_all.at[me_x, :, pl.ds(0, hid_d)]),
        (du_h, dgu_all.at[me_x, :, pl.ds(hid_d, hid_d)]), (eg_h, eg), (eu_h, eu), (ed_h, ed), (dd_h, dd),
    ]
    loads = [pltpu.make_async_copy(a, b, load_sem.at[k]) for k, (a, b) in enumerate(loads)]
    for copy in loads:
        copy.start()

    barrier = pltpu.get_barrier_semaphore()

    def greet(d, _):
        pl.semaphore_signal(barrier, 1, device_id=(lax.rem(me_e + d, n), me_t), device_id_type=MESH)
        pl.semaphore_signal(barrier, 1, device_id=(me_e, lax.rem(me_t + d, n)), device_id_type=MESH)
        return 0

    lax.fori_loop(1, n, greet, 0)
    pl.semaphore_wait(barrier, 2 * n - 2)

    def ep_copy(phase, src, dst, peer, landing):
        return pltpu.make_async_remote_copy(
            src_ref=src, dst_ref=dst, send_sem=send_sem.at[phase],
            recv_sem=recv_sem.at[first_spot[phase] + landing], device_id=(peer, me_t), device_id_type=MESH)

    def tp_copy(phase, src, dst, peer, landing):
        return pltpu.make_async_remote_copy(
            src_ref=src, dst_ref=dst, send_sem=send_sem.at[phase],
            recv_sem=recv_sem.at[first_spot[phase] + landing], device_id=(me_e, peer), device_id_type=MESH)

    def over(peer_e, peer_t, phase, src, dst, landing):
        return pltpu.make_async_remote_copy(
            src_ref=src, dst_ref=dst, send_sem=send_sem.at[phase],
            recv_sem=recv_sem.at[first_spot[phase] + landing], device_id=(peer_e, peer_t), device_id_type=MESH)

    def chip(k):
        k = chips - k
        return lax.rem(me_z + chips + lax.div(k + 1, 2) * (2 * lax.rem(k, 2) - 1), chips)

    def sum_over_tp(pair_phase, phase, part, pair, summed, arrived, make):
        def give(k, _):
            z = lax.rem(me_z + k, chips)
            at = 2 * z + 1 - core
            part[at] = make(at)
            tp_copy(pair_phase, part.at[at], pair.at[z], partner, z).start()
            return 0

        lax.fori_loop(1, chips + 1, give, 0)

        def add(z):
            mine = make(2 * z + core)
            tp_copy(pair_phase, pair.at[z], pair.at[z], partner, z).wait_recv()
            return mine.astype(F32) + pair[z].astype(F32)

        def pass_on(k, _):
            z = chip(k)
            summed[z] = add(z).astype(BF16)
            tp_copy(phase, summed.at[z], arrived.at[me_z], 2 * z + core, 0).start()
            return 0

        lax.fori_loop(1, chips, pass_on, 0)
        return add(me_z)

    def summed_over_tp(phase, arrived, acc):
        await_blocks(phase, arrived.at[pl.ds(0, chips - 1)])
        return others(me_z, chips, arrived, acc)

    def give_over_tp(phase, mine, spot):
        tp_copy(phase, mine, spot(me_t), partner, chips).start()

        def give(k, _):
            tp_copy(phase, mine, spot(me_t), 2 * chip(k) + core, me_z).start()
            return 0

        lax.fori_loop(1, chips, give, 0)

    def pass_over_tp(phase, spot):
        def pass_on(k, _):
            z = chip(chips - k)
            part = spot(2 * z + core)
            tp_copy(phase, part, part, 2 * z + core, z).wait_recv()
            tp_copy(phase, part, part, partner, chips).start()
            return 0

        lax.fori_loop(1, chips, pass_on, 0)

    def take_over_tp(phase, half):
        tp_copy(phase, half, half, partner, chips).wait_recv()

    def projection(t):
        return proj_all.at[t]

    def along_x(step):
        return side * me_y + lax.rem(me_x + step + side, side)

    def along_y(step):
        return side * lax.rem(me_y + step + side, side) + me_x

    def weight_copy(phase, buffer, block_of, peer, first, many, landing):
        part = buffer.at[block_of, pl.ds(first, many), :]
        return over(peer, me_t, phase, part, part, landing)

    def near(phase, buffer, me, along, first, many, part):
        for way, step in enumerate((1, -1)):
            weight_copy(phase, buffer, me, along(step), first, many, 2 * part + way).start()

    def arrived_near(phase, buffer, me, along, first, many, part):
        for way, step in enumerate((-1, 1)):
            owner = lax.rem(me + step + side, side)
            weight_copy(phase, buffer, owner, along(step), first, many, 2 * part + way).wait_recv()

    def far(phase, buffer, me, along, first, many, part, act):
        half = many // 2
        for way, step in enumerate((1, -1)):
            if act == "start":
                owner = lax.rem(me - step + side, side)
                weight_copy(phase, buffer, owner, along(step), first + way * half, half, 2 * part + way).start()
            else:
                owner = lax.rem(me + 2, side)
                weight_copy(phase, buffer, owner, along(-step), first + way * half, half, 2 * part + way).wait_recv()

    def give_weights(part):
        near(NEAR, dgu_all, me_x, along_x, *PARTS[part], part)

    def pass_weights(part):
        arrived_near(NEAR, dgu_all, me_x, along_x, *PARTS[part], part)
        far(FAR, dgu_all, me_x, along_x, *PARTS[part], part, "start")

    def gather_quarter():
        to_e = side * me_y + lax.rem(owned, side)
        spot = me_x * side + lax.div(owned, side)

        def give(k, _):
            over(to_e, 2 * chip(k) + core, RES, res_own, res_all.at[spot], spot).start()
            return 0

        lax.fori_loop(1, chips, give, 0)

        @pl.when(to_e != me_e)
        def _():
            over(to_e, me_t, RES, res_own, res_all.at[spot], spot).start()

        @pl.when(to_e == me_e)
        def _():
            res_all[spot] = res_own[...]

        pass_weights(2)
        arrived_near(NEAR_DOWN, dd_all, me_y, along_y, 0, hid_d, 0)
        far(FAR_DOWN, dd_all, me_y, along_y, 0, hid_d, 0, "start")

        def source(spot):
            o = side * lax.rem(spot, side) + me_x
            j = side * me_y + lax.div(spot, side)
            return j, lax.rem(o + j, n)

        def spot_of(k, parity):
            return (2 * lax.rem(k, 2) + parity) * side + lax.div(k, 2)

        def pass_on(k, _):
            spot = spot_of(k, lax.rem(core + me_x, 2))
            j, t = source(spot)

            @pl.when((j != me_e) | (t != me_t))
            def _():
                over(j, t, RES, res_all.at[spot], res_all.at[spot], spot).wait_recv()

            over(me_e, partner, RES, res_all.at[spot], res_all.at[spot], n).start()
            return 0

        lax.fori_loop(0, n // 2, pass_on, 0)

        half = res_all.at[pl.ds(0, chips)]
        over(me_e, partner, RES, half, half, n).wait_recv()

    def to_y_peers(phase, src_of, dst):
        def one(d, _):
            y = lax.rem(me_y + d, side)
            over(side * y + me_x, me_t, phase, src_of(y), dst, 0).start()
            return 0

        lax.fori_loop(1, side, one, 0)

    def steps(far_first):
        offsets = [(dy, dx) for dy in range(side) for dx in range(side) if dy or dx]
        cross = lambda o: sum(min(d, side - d) for d in o)
        return sorted(offsets, key=cross, reverse=far_first)

    def ep_at(dy, dx):
        return side * lax.rem(me_y + dy, side) + lax.rem(me_x + dx, side)

    def to_ep_peers(phase, src_of, dst):
        for dy, dx in steps(True):
            peer = ep_at(dy, dx)
            ep_copy(phase, src_of(peer), dst, peer, 0).start()

    def await_blocks(phase, blocks):
        over(me_e, partner, phase, blocks, blocks, 0).wait_recv()

    def others(me, many, buffer, acc):
        def one(d, acc):
            return acc + buffer[lax.rem(me + d, many)].astype(F32)

        return lax.fori_loop(1, many, one, acc)

    rest, few = pl.ds(0, n - 1), pl.ds(0, side - 1)
    far_first = (2, 1, 3, 0) if side == 4 else tuple(range(side))

    def sent(copy, phase, many):
        copy(phase, many, many, 0, 0).wait_send()

    loads[0].wait()
    to_ep_peers(TOK,
             lambda peer: tok.at[:, pl.ds(pl.multiple_of(peer * block, block), block)],
             tok_all.at[me_e])
    tok_all[me_e] = tok[:, pl.ds(pl.multiple_of(me_e * block, block), block)]

    loads[16].wait()
    give_over_tp(PROJ, projection(me_t), projection)
    loads[17].wait()
    loads[18].wait()
    give_weights(0)

    loads[4].wait()
    loads[5].wait()
    route_rows = [routes[pl.ds(k, 1), :] for k in range(2)]
    lanes_e = iota((128, rows), 0)
    named = sum(jnp.where(lanes_e == r, 1.0, 0.0) for r in route_rows)
    earlier = jnp.where(iota((rows, rows), 0) < iota((rows, rows), 1), 1.0, 0.0)
    before = jnp.dot(named.astype(BF16), earlier.astype(BF16), preferred_element_type=F32)
    base = (CAP * me_y).astype(F32)
    key = jnp.where(named > 0.0, before + base, -1.0)
    eye = jnp.where(iota((rows, rows), 0) == iota((rows, rows), 1), 1.0, 0.0)
    key_all[me_y] = lax.dot_general(
        eye.astype(BF16), key.astype(BF16), NT, preferred_element_type=F32).astype(BF16)
    to_y_peers(KEY, lambda y: key_all.at[me_y], key_all.at[me_y])
    weights = [rw[pl.ds(k, 1), :] for k in range(2)]
    total = weights[0] + weights[1]
    spots = iota((n * SLOT, rows), 0)
    share_t = jnp.zeros((n * SLOT, rows), F32)
    for r, w in zip(route_rows, weights):
        slot = jnp.sum(jnp.where(lanes_e == r, before, 0.0), axis=0, keepdims=True)
        hit = (spots.astype(F32) == r.astype(F32) * SLOT + slot)
        share_t = share_t + jnp.where(hit, w / total, 0.0)
    ret_w[...] = lax.dot_general(eye, share_t, NT, precision=HIGHEST, preferred_element_type=F32)

    loads[1].wait()
    squares = jnp.zeros((rows, block), F32)
    for k in range(n):
        part = tok[:, k * block:(k + 1) * block].astype(F32)
        squares = squares + part * part
    scale = lax.rsqrt(jnp.sum(squares, axis=1, keepdims=True) / width + EPS)
    loads[6].wait()
    loads[7].wait()
    gate = jnp.zeros((rows, 2 * n), F32)
    for k in range(n):
        cols = slice(k * block, (k + 1) * block)
        gain = mgain[:, cols]
        normed = (tok[:, cols].astype(F32) * scale * gain).astype(BF16)
        gate = gate + lax.dot_general(normed, wgates[:, cols], NT, preferred_element_type=F32)
    for k in range(8, 11):
        loads[k].wait()
    lane = iota((rows, 2 * n), 1)
    gate_in = jnp.sum(jnp.where(lane == me_t, gate, 0.0), axis=1, keepdims=True)
    gate_forget = jnp.sum(jnp.where(lane == me_t + n, gate, 0.0), axis=1, keepdims=True)
    bias = jnp.sum(jnp.where(iota((1, n), 1) == me_t, fbias[...], 0.0), axis=1, keepdims=True)
    gate_forget = gate_forget + bias
    log_keep = jnp.minimum(gate_forget, 0.0) - jnp.log1p(jnp.exp(-jnp.abs(gate_forget)))
    old_max = to_column(smax[...], rows)
    new_max = jnp.maximum(log_keep + old_max, gate_in)
    keep = jnp.exp(log_keep + old_max - new_max)
    write = jnp.exp(gate_in - new_max)
    nmax[...] = to_row(new_max, rows)

    await_blocks(TOK, tok_all.at[rest])
    for k in range(11, 15):
        loads[k].wait()
    gain_m = mgain[:, pl.ds(pl.multiple_of(me_e * block, block), block)]

    def project(dy):
        at = pl.multiple_of(side * lax.rem(me_y + dy, side), side)
        x = tok_all[pl.ds(at, side)].reshape(quarter, block).astype(F32) * gain_m
        y = jnp.dot(x.astype(BF16), wqkv[...], preferred_element_type=F32)
        qkv_part[pl.ds(at, side)] = y.astype(BF16).reshape(side, rows, 4 * head)
        for dx in far_first:
            if dy or dx:
                peer = ep_at(dy, dx)
                ep_copy(QKV, qkv_part.at[peer], qkv_in.at[me_e], peer, 0).start()

    for dy in far_first:
        project(dy)
    give_weights(1)

    loads[15].wait()
    await_blocks(QKV, qkv_in.at[rest])
    y = others(me_e, n, qkv_in, qkv_part[me_e].astype(F32)) * scale
    query = y[:, :head]
    keys = y[:, head:2 * head] * head ** (-0.5)
    value = y[:, 2 * head:3 * head]
    outgate = y[:, 3 * head:]
    written = write * keys
    new_norm = keep * sn[...] + written
    nn[...] = new_norm
    denom = jnp.sum(query * new_norm, axis=1, keepdims=True)
    qt[...] = query.T
    wkt[...] = written.T
    vrow[...] = value
    keep_rows[...] = jnp.broadcast_to(keep, (rows, head))
    for b in range(rows):
        numer[pl.ds(b, 1), :] = jnp.sum(qt[:, b:b + 1] * sm[b], axis=0, keepdims=True)
    dots = jnp.sum(query * written, axis=1, keepdims=True)
    num = keep * numer[...] + dots * value
    cell = num / jnp.maximum(jnp.abs(denom), 1.0)
    mix_own[...] = (jax.nn.sigmoid(outgate) * cell).astype(BF16)

    def head_place(h):
        return mix_in.at[:, pl.ds(pl.multiple_of(h * head, head), head)]

    for dy, dx in steps(True):
        j = ep_at(dy, dx)
        over(j, lax.rem(me_e + j, n), MIX, mix_own, head_place(me_t), 0).start()

    @pl.when(owned != me_e)
    def _():
        over(me_e, lax.rem(2 * me_e, n), MIX, mix_own, head_place(me_t), 0).start()

    @pl.when(owned == me_e)
    def _():
        mix_in[:, pl.ds(pl.multiple_of(me_t * head, head), head)] = mix_own[...]

    give_weights(2)
    loads[22].wait()
    near(NEAR_DOWN, dd_all, me_y, along_y, 0, hid_d, 0)
    pass_over_tp(PROJ, projection)
    pass_weights(0)
    pass_weights(1)
    for b in range(rows):
        nm[b] = keep_rows[pl.ds(b, 1), :] * sm[b] + wkt[:, b:b + 1] * vrow[pl.ds(b, 1), :]

    await_blocks(KEY, key_all.at[few])
    key_t = lax.dot_general(
        jnp.where(iota((n, 128), 0) == iota((n, 128), 1), 1.0, 0.0).astype(BF16),
        key_all[...].reshape(quarter, 128), NT, preferred_element_type=F32)
    places = iota((few_rows, quarter), 0).astype(F32)
    for e in range(0, n, 2):
        both = [jnp.where(places == key_t[k:k + 1, :], 1.0, 0.0) for k in (e, e + 1)]
        pick[pl.ds(e * few_rows, 2 * few_rows), :] = jnp.concatenate(both, axis=0).astype(BF16)

    take_over_tp(PROJ, proj_all.at[pl.ds(0, chips)])

    @pl.when(owned != me_e)
    def _():
        await_blocks(MIX, mix_in)

    @pl.when(owned == me_e)
    def _():
        await_blocks(MIX, mix_in.at[:, pl.ds(0, (n - 1) * head)])

    mixed = jnp.dot(mix_in[...], proj_all[...].reshape(n * head, block), preferred_element_type=F32)
    residual = (tok_all[owned].astype(F32) + mixed).astype(BF16)
    res_own[...] = residual

    def to_final():
        return pltpu.make_async_remote_copy(
            src_ref=res_own, dst_ref=res_fin, send_sem=res_sem.at[0], recv_sem=res_sem.at[1],
            device_id=(owned, me_e), device_id_type=MESH)

    corner = (owned == me_e) & (me_e == me_t)

    gather_quarter()

    @pl.when(jnp.logical_not(corner))
    def _():
        to_final().start()

    @pl.when(corner)
    def _():
        res_fin[...] = res_own[...]

    loads[2].wait()
    loads[3].wait()

    def pass_rows(peer):
        part = row_in.at[core * n + peer]
        tp_copy(ROW, part, part, partner, n + lax.div(peer, side)).start()

    half_side = side // 2
    res_half = jnp.concatenate(
        [res_all[pl.ds((core * half_side + k) * side, side)].reshape(quarter, block)
         for k in range(half_side)], axis=1)

    def dispatch(dy):
        at = pl.multiple_of(side * lax.rem(me_y + dy, side), side)
        y = jnp.dot(pick[pl.ds(pl.multiple_of(at * few_rows, side * few_rows), side * few_rows), :],
                    res_half, preferred_element_type=F32)
        row_out[pl.ds(at, side)] = y.reshape(side, few_rows, half_side * block).astype(BF16)
        for dx in far_first:
            if dy or dx:
                peer, spot = ep_at(dy, dx), core * n + me_e
                ep_copy(ROW, row_out.at[peer], row_in.at[spot], peer, me_e).start()

    for dy in far_first:
        dispatch(dy)
    row_in[core * n + me_e] = row_out[me_e]
    pass_rows(me_e)

    wbr_wide[...] = wbr[...].astype(F32)
    lines = block // 128
    squares = [jnp.zeros((rows, 1), F32)] * side
    branches = [jnp.zeros((rows, 1), F32)] * side
    for k in range(side):
        j = side * me_y + k
        gain_f = fgain[:, pl.ds(pl.multiple_of(j * block, block), block)]
        gain_b = gain_f * jnp.concatenate(
            [wbr_wide[pl.ds(j * lines + i, 1), :] for i in range(lines)], axis=1)
        for g in range(side):
            r = res_all[k * side + g].astype(F32)
            squares[g] = squares[g] + jnp.sum(r * r, axis=1, keepdims=True)
            branches[g] = branches[g] + jnp.sum(r * gain_b, axis=1, keepdims=True)
            x_cat[pl.ds(g * rows, rows), k * block:(k + 1) * block] = (r * gain_f).astype(BF16)
    for g in range(side):
        sta_out[g] = jnp.where(iota((8, 128), 0) == 0, to_row(squares[g], 128), to_row(branches[g], 128))
    to_y_peers(STA, lambda y: sta_out.at[y], sta_in.at[me_y])

    for part, (first, many) in enumerate(PARTS):
        far(FAR, dgu_all, me_x, along_x, first, many, part, "wait")
    weights = dgu_all[...].reshape(side * block, 2 * hid_d)
    x = x_cat[...]
    for k in range(2 * hid_d // block):
        y = jnp.dot(x, weights[:, k * block:(k + 1) * block], preferred_element_type=F32)
        den_part[:, :, k * block:(k + 1) * block] = y.astype(BF16).reshape(side, rows, block)
    to_y_peers(DEN, lambda y: den_part.at[y], den_in.at[me_y])

    loads[19].wait()
    loads[20].wait()

    deep = half_side * block

    def expert_in(y, half, ss):
        x = row_in[pl.ds(half * n + y * side, side)].astype(F32).reshape(cap_rows, deep)
        at = pl.multiple_of(y * side * block + half * deep, deep)
        xg = (x * fgain[:, pl.ds(at, deep)]).astype(BF16)
        gu_acc[:, pl.ds(0, hid_e)] += jnp.dot(xg, eg[pl.ds(at, deep), :], preferred_element_type=F32)
        gu_acc[:, pl.ds(hid_e, hid_e)] += jnp.dot(xg, eu[pl.ds(at, deep), :], preferred_element_type=F32)
        return ss + jnp.sum(x * x, axis=1, keepdims=True)

    def expert_first(d, ss):
        y = lax.rem(me_y + side - d, side)

        def one(k, _):
            peer = side * y + lax.rem(me_x + k, side)
            spot = core * n + peer

            @pl.when(peer != me_e)
            def _():
                ep_copy(ROW, row_in.at[spot], row_in.at[spot], peer, peer).wait_recv()
                pass_rows(peer)

            return 0

        lax.fori_loop(0, side, one, 0)
        return expert_in(y, core, ss)

    def expert_second(d, ss):
        y = lax.rem(me_y + side - d, side)

        part = row_in.at[pl.ds((1 - core) * n + side * y, side)]
        tp_copy(ROW, part, part, partner, n + y).wait_recv()
        return expert_in(y, 1 - core, ss)

    gu_acc[...] = jnp.zeros_like(gu_acc)
    ss = expert_first(0, jnp.zeros((cap_rows, 1), F32))
    ss = lax.fori_loop(1, side, lambda d, ss: expert_second(d - 1, expert_first(d, ss)), ss)
    ss = expert_second(side - 1, ss)
    row_scale = lax.rsqrt(ss / width + EPS)
    g = gu_acc[:, :hid_e] * row_scale
    u = gu_acc[:, hid_e:] * row_scale
    hidden_e[...] = (g / (1.0 + jnp.exp(-g)) * u).astype(BF16)
    loads[21].wait()

    def expert_out(at):
        return jnp.dot(hidden_e[...], ed[:, pl.ds(pl.multiple_of(at * block, block), block)],
                       preferred_element_type=F32).astype(BF16)

    routed_sum = sum_over_tp(
        EXP_PAIR, EXP, exp_part, exp_pair, exp_sum, exp_in, expert_out)

    await_blocks(STA, sta_in.at[few])
    sums = others(me_y, side, sta_in, sta_out[me_y])
    dense_scale = lax.rsqrt(to_column(sums[0:1, :], rows) / width + EPS)
    branch = jax.nn.sigmoid(to_column(sums[1:2, :], rows) * dense_scale)
    await_blocks(DEN, den_in.at[few])
    y = others(me_y, side, den_in, den_part[me_y].astype(F32)) * dense_scale
    g, u = y[:, :hid_d], y[:, hid_d:]
    hid_all[me_x] = (g / (1.0 + jnp.exp(-g)) * u * branch).astype(BF16)

    def spread_hidden(d, _):
        over(along_x(d), me_t, HID, hid_all.at[me_x], hid_all.at[me_x], me_x).start()
        return 0

    lax.fori_loop(1, side, spread_hidden, 0)

    far(FAR_DOWN, dd_all, me_y, along_y, 0, hid_d, 0, "wait")

    def hidden_of(d, _):
        x = lax.rem(me_x + side - d, side)
        over(along_x(-d), me_t, HID, hid_all.at[x], hid_all.at[x], x).wait_recv()
        return 0

    lax.fori_loop(1, side, hidden_of, 0)
    x = hid_all[...].reshape(quarter, hid_d)
    for k in range(side):
        y = jnp.dot(x, dd_all[k], preferred_element_type=F32)
        dwn_part[pl.ds(k * side, side)] = y.astype(BF16).reshape(side, rows, block)
    end_core = lax.rem(me_x, 2)
    home = lax.rem(me_t, side) == me_x

    @pl.when(core != end_core)
    def _():
        tp_copy(DWN_PAIR, dwn_part, dwn_pair, partner, 0).start()

    @pl.when(core == end_core)
    def _():
        tp_copy(DWN_PAIR, dwn_pair, dwn_pair, partner, 0).wait_recv()
        for dx in far_first:
            def to_end(c, _):
                x = lax.rem(me_x + dx, side)
                k = side * c + x
                dwn_sum[k] = (dwn_part[k].astype(F32) + dwn_pair[k].astype(F32)).astype(BF16)
                z = 2 * c + lax.div(me_x, 2)
                here = (x == me_x) & (z == me_z)

                @pl.when(jnp.logical_not(here))
                def _():
                    over(side * me_y + x, 2 * z + core, DWN, dwn_sum.at[k], dwn_in.at[me_z], 0).start()

                @pl.when(here)
                def _():
                    dwn_in[me_z] = dwn_sum[k]

                return 0

            lax.fori_loop(0, side, to_end, 0)

    y = summed_over_tp(EXP, exp_in, routed_sum)
    spot, col = iota((n * SLOT, cap_rows), 0), iota((n * SLOT, cap_rows), 1)
    within = jnp.bitwise_and(spot, SLOT - 1)
    shift = side.bit_length() - 1
    from_e = jnp.right_shift(spot, SLOT.bit_length() - 1)
    source = few_rows * jnp.bitwise_and(from_e, side - 1) + CAP * jnp.right_shift(from_e, shift) + within
    spread = jnp.where((source == col) & (within < CAP), 1.0, 0.0).astype(BF16)
    ret_out[...] = jnp.dot(
        spread, y.astype(BF16), preferred_element_type=F32).reshape(n, SLOT, block).astype(BF16)

    to_ep_peers(RET, lambda peer: ret_out.at[peer], ret_in.at[me_e])
    ret_in[me_e] = ret_out[me_e]

    await_blocks(RET, ret_in.at[rest])

    @pl.when(jnp.logical_not(corner))
    def _():
        to_final().wait()

    routed = jnp.dot(ret_w[...], ret_in[...].astype(F32).reshape(n * SLOT, block), precision=HIGHEST,
                     preferred_element_type=F32)
    known = res_fin[...].astype(F32) + routed

    @pl.when(home)
    def _():
        await_blocks(DWN, dwn_in.at[pl.ds(0, chips - 1)])

    @pl.when(jnp.logical_not(home))
    def _():
        await_blocks(DWN, dwn_in)

    y = others(me_z, chips, dwn_in, dwn_in[me_z].astype(F32))
    out_own[...] = (known + y).astype(BF16)

    def columns(j):
        return out.at[:, pl.ds(pl.multiple_of(j * block, block), block)]

    give_over_tp(OUT, out_own, columns)
    out[:, pl.ds(pl.multiple_of(me_t * block, block), block)] = out_own[...]
    pass_over_tp(OUT, columns)
    take_over_tp(OUT, out.at[:, pl.ds(0, chips * block)])
    sent(ep_copy, TOK, tok_all.at[rest])
    sent(ep_copy, KEY, key_all.at[few])
    sent(ep_copy, QKV, qkv_part.at[rest])
    some = pl.ds(0, chips - 1)

    @pl.when(owned != me_e)
    def _():
        sent(ep_copy, MIX, mix_in)

    @pl.when(owned == me_e)
    def _():
        sent(ep_copy, MIX, mix_in.at[:, pl.ds(0, (n - 1) * head)])

    sent(tp_copy, PROJ, proj_all.at[rest])
    sent(ep_copy, ROW, row_in.at[pl.ds(0, 2 * n - 1)])
    sent(ep_copy, STA, sta_out.at[few])
    sent(ep_copy, DEN, den_part.at[few])
    sent(ep_copy, HID, hid_all.at[few])
    for phase, buffer, rows_of in (
        (NEAR, dgu_all, block), (FAR, dgu_all, block // 2),
        (NEAR_DOWN, dd_all, hid_d), (FAR_DOWN, dd_all, hid_d // 2)):
        sent(ep_copy, phase, buffer.at[pl.ds(0, 2), pl.ds(0, rows_of), :])
    sent(tp_copy, EXP_PAIR, exp_pair)
    sent(tp_copy, EXP, exp_sum.at[some])
    sent(ep_copy, RET, ret_out.at[rest])
    sent(tp_copy, OUT, tok_all.at[rest])

    @pl.when(core != end_core)
    def _():
        sent(tp_copy, DWN_PAIR, dwn_part)

    @pl.when(home)
    def _():
        sent(ep_copy, DWN, dwn_sum.at[rest])

    @pl.when((core == end_core) & jnp.logical_not(home))
    def _():
        sent(ep_copy, DWN, dwn_sum)

    own_column = lax.rem(owned, side) == me_x

    @pl.when(jnp.logical_not(own_column))
    def _():
        sent(ep_copy, RES, res_all)

    @pl.when(own_column)
    def _():
        sent(ep_copy, RES, res_all.at[rest])


def on_device(
    n, tokens, state_matrix, state_norm, state_max, mixer_gain, w_query, w_key, w_value, w_outgate,
    w_ingate, w_forget, forget_bias, w_proj, ffn_gain, w_branch, routes, route_weight,
    expert_gate, expert_up, expert_down, dense_gate, dense_up, dense_down,
):
    rows, width = tokens.shape
    head = state_norm.shape[-1]
    block = width // n
    hid_e, hid_d = expert_gate.shape[2], dense_gate.shape[1]
    cap_rows = CAP * n
    args = (
        tokens,
        state_matrix.reshape(rows, head, head),
        state_norm.reshape(rows, head),
        state_max.T,
        mixer_gain.reshape(1, width),
        w_query, w_key, w_value, w_outgate,
        w_ingate.T, w_forget.T,
        forget_bias.reshape(1, n),
        w_proj,
        ffn_gain.reshape(1, width),
        w_branch.reshape(width // 128, 128),
        routes.T, route_weight.T,
        expert_gate.reshape(width, hid_e), expert_up.reshape(width, hid_e),
        expert_down.reshape(hid_e, width),
        dense_gate, dense_up, dense_down,
    )
    vm = pltpu.VMEM
    dma = pltpu.SemaphoreType.DMA
    few_rows, side = CAP * math.isqrt(n), math.isqrt(n)

    def hier(tall):
        return [vm((n, tall, block), BF16)] + [vm((n // 2, tall, block), BF16)] * 3

    scratch = [
        vm((rows, width), BF16), vm((rows, head, head), F32), vm((rows, head), F32), vm((1, rows), F32),
        vm((1, width), F32), vm((block, 4 * head), BF16), vm((2 * n, width), BF16), vm((1, n), F32),
        vm((n, head, block), BF16), vm((1, width), F32), vm((width // 128, 128), BF16), vm((2, rows), jnp.int32),
        vm((2, rows), F32), vm((width, hid_e), BF16), vm((width, hid_e), BF16), vm((hid_e, width), BF16),
        vm((side, block, 2 * hid_d), BF16), vm((side, hid_d, block), BF16),
        vm((n, rows, block), BF16), vm((side, rows, 128), BF16),
        vm((n, rows, 4 * head), BF16), vm((n, rows, 4 * head), BF16),
        vm((rows, head), BF16), vm((rows, n * head), BF16),
        vm((rows, block), BF16), vm((n, rows, block), BF16), vm((rows, block), BF16),
        vm((n, few_rows, side * block // 2), BF16), vm((2 * n, few_rows, side * block // 2), BF16),
        vm((side, 8, 128), F32), vm((side, 8, 128), F32),
        vm((side, rows, 2 * hid_d), BF16), vm((side, rows, 2 * hid_d), BF16),
        vm((side, rows, hid_d), BF16), *[vm((n, rows, block), BF16)] * 3, vm((n // 2, rows, block), BF16),
        *hier(cap_rows),
        vm((n, SLOT, block), BF16), vm((n, SLOT, block), BF16),
        vm((rows, block), BF16),
        vm((width // 128, 128), F32),
        vm((n * few_rows, side * rows), BF16), vm((side * rows, side * block), BF16), vm((cap_rows, hid_e), BF16), vm((cap_rows, 2 * hid_e), F32), vm((rows, 2 * n), F32),
        vm((head, rows), F32), vm((head, rows), F32), vm((rows, head), F32), vm((rows, head), F32),
        vm((rows, head), F32), vm((rows, n * SLOT), F32),
        dma((len(args),)), dma((PHASES,)), dma((landing_spots(n)[1],)), dma((2,)),
    ]
    any_space = pl.BlockSpec(memory_space=pl.ANY)
    layer_out, new_matrix, new_norm, new_max = pl.pallas_call(
        functools.partial(layer_kernel, n),
        out_shape=(
            vm((rows, width), BF16), vm((rows, head, head), F32), vm((rows, head), F32), vm((1, rows), F32),
        ),
        in_specs=[any_space] * len(args),
        out_specs=[pl.BlockSpec(memory_space=vm)] * 4,
        scratch_shapes=scratch,
        compiler_params=pltpu.CompilerParams(
            collective_id=0, has_side_effects=True, vmem_limit_bytes=56 * 1024 * 1024),
        name="layer",
    )(*args)
    return (layer_out, new_matrix.reshape(rows, 1, head, head), new_norm.reshape(rows, 1, head), new_max.T)


def solution(mesh):
    n = mesh.shape["ep"]
    in_specs = (
        P("ep", None),
        P("ep", "tp", None, None),
        P("ep", "tp", None),
        P("ep", "tp"),
        P(),
        P("ep", "tp"),
        P("ep", "tp"),
        P("ep", "tp"),
        P("ep", "tp"),
        P(),
        P(),
        P(),
        P("tp", "ep"),
        P(),
        P(),
        P("ep", None),
        P("ep", None),
        P("ep", None, "tp"),
        P("ep", None, "tp"),
        P("ep", "tp", None),
        P("ep", "tp"),
        P("ep", "tp"),
        P("tp", "ep"),
    )
    out_specs = (P("ep", None), P("ep", "tp", None, None), P("ep", "tp", None), P("ep", "tp"))
    return jax.shard_map(
        functools.partial(on_device, n), mesh=mesh, in_specs=in_specs, out_specs=out_specs,
        check_vma=False)
```

```python
import functools
import math

import jax
import jax.numpy as jnp
from jax import lax
from jax.experimental import pallas as pl
from jax.experimental.pallas import tpu as pltpu
from jax.sharding import PartitionSpec as P

EPS = 1e-06
MESH = pl.DeviceIdType.MESH
CAP = 6
SLOT = 8
F32 = jnp.float32
BF16 = jnp.bfloat16
HIGHEST = lax.Precision.HIGHEST
NT = (((1,), (1,)), ((), ()))


def landing_spots(n):
    side = math.isqrt(n)
    many = {ROW: n + side, RES: n + 1, NEAR: 6, FAR: 6, NEAR_DOWN: 2, FAR_DOWN: 2, HID: side}
    for phase in (TOK, KEY, QKV, STA, DEN, RET, MIX, DWN, DWN_PAIR, EXP):
        many[phase] = 1
    many[EXP_PAIR] = n // 2
    many[PROJ] = many[OUT] = n // 2 + 1
    first, at = [], 0
    for phase in range(PHASES):
        first.append(at)
        at += many.get(phase, n)
    return first, at


def iota(shape, dim):
    return lax.broadcasted_iota(jnp.int32, shape, dim)


def to_column(row, rows):
    diag = iota((rows, row.shape[1]), 0) == iota((rows, row.shape[1]), 1)
    return jnp.sum(jnp.where(diag, row, 0.0), axis=1, keepdims=True)


def to_row(column, lanes):
    rows = column.shape[0]
    diag = iota((rows, lanes), 0) == iota((rows, lanes), 1)
    return jnp.sum(jnp.where(diag, column, 0.0), axis=0, keepdims=True)


(TOK, KEY, QKV, MIX, PROJ, RES, ROW, STA, DEN, HID, DWN_PAIR, DWN, EXP_PAIR, EXP, RET,
 OUT, NEAR, FAR, NEAR_DOWN, FAR_DOWN) = range(20)
PHASES = 20
AHEAD = 3
PARTS = ((0, 64), (64, 64), (128, 128))


def layer_kernel(
    n,
    tok_h, sm_h, sn_h, smax_h, mgain_h, wq_h, wk_h, wv_h, wo_h, win_h, wfo_h, fbias_h,
    wproj_h, fgain_h, wbr_h, routes_h, rw_h, eg_h, eu_h, ed_h, dg_h, du_h, dd_h,
    out, nm, nn, nmax,
    tok, sm, sn, smax, mgain, wqkv, wgates, fbias, proj_all, fgain, wbr, routes, rw,
    eg, eu, ed, dgu_all, dd_all,
    tok_all, key_all, qkv_part, qkv_in, mix_own, mix_in, res_own, res_all, res_fin,
    row_out, row_in, sta_out, sta_in, den_part, den_in, hid_all, dwn_part, dwn_pair, dwn_sum, dwn_in,
    exp_part, exp_pair, exp_sum, exp_in, ret_out, ret_in, out_own,
    wbr_wide, pick, x_cat, hidden_e, gu_acc, gates, wkt, qt, vrow, keep_rows, numer, ret_w,
    load_sem, send_sem, recv_sem, res_sem,
):
    me_e, me_t = lax.axis_index("ep"), lax.axis_index("tp")
    chips = n // 2
    first_spot, _ = landing_spots(n)
    side = math.isqrt(n)
    me_y, me_x = lax.div(me_e, side), lax.rem(me_e, side)
    me_z, core = lax.div(me_t, 2), lax.rem(me_t, 2)
    partner = me_t + 1 - 2 * core
    owned = lax.rem(me_t - me_e + n, n)
    rows = tok.shape[0]
    width = tok.shape[1]
    block = width // n
    head = sn.shape[1]
    hid_e = eg.shape[1]
    hid_d = dd_all.shape[1]
    quarter = rows * side
    cap_rows = CAP * n
    few_rows = CAP * side
    dgu, dd = dgu_all.at[me_x], dd_all.at[me_y]

    loads = [
        (tok_h, tok), (mgain_h, mgain), (fgain_h, fgain), (wbr_h, wbr), (routes_h, routes),
        (rw_h, rw), (win_h, wgates.at[pl.ds(0, n), :]), (wfo_h, wgates.at[pl.ds(n, n), :]),
        (fbias_h, fbias), (smax_h, smax), (sn_h, sn),
        (wq_h, wqkv.at[:, pl.ds(0, head)]), (wk_h, wqkv.at[:, pl.ds(head, head)]),
        (wv_h, wqkv.at[:, pl.ds(2 * head, head)]), (wo_h, wqkv.at[:, pl.ds(3 * head, head)]),
        (sm_h, sm), (wproj_h, proj_all.at[me_t]), (dg_h, dgu_all.at[me_x, :, pl.ds(0, hid_d)]),
        (du_h, dgu_all.at[me_x, :, pl.ds(hid_d, hid_d)]), (eg_h, eg), (eu_h, eu), (ed_h, ed), (dd_h, dd),
    ]
    loads = [pltpu.make_async_copy(a, b, load_sem.at[k]) for k, (a, b) in enumerate(loads)]
    for copy in loads:
        copy.start()

    barrier = pltpu.get_barrier_semaphore()

    def greet(d, _):
        pl.semaphore_signal(barrier, 1, device_id=(lax.rem(me_e + d, n), me_t), device_id_type=MESH)
        pl.semaphore_signal(barrier, 1, device_id=(me_e, lax.rem(me_t + d, n)), device_id_type=MESH)
        return 0

    lax.fori_loop(1, n, greet, 0)
    pl.semaphore_wait(barrier, 2 * n - 2)

    def ep_copy(phase, src, dst, peer, landing):
        return pltpu.make_async_remote_copy(
            src_ref=src, dst_ref=dst, send_sem=send_sem.at[phase],
            recv_sem=recv_sem.at[first_spot[phase] + landing], device_id=(peer, me_t), device_id_type=MESH)

    def tp_copy(phase, src, dst, peer, landing):
        return pltpu.make_async_remote_copy(
            src_ref=src, dst_ref=dst, send_sem=send_sem.at[phase],
            recv_sem=recv_sem.at[first_spot[phase] + landing], device_id=(me_e, peer), device_id_type=MESH)

    def over(peer_e, peer_t, phase, src, dst, landing):
        return pltpu.make_async_remote_copy(
            src_ref=src, dst_ref=dst, send_sem=send_sem.at[phase],
            recv_sem=recv_sem.at[first_spot[phase] + landing], device_id=(peer_e, peer_t), device_id_type=MESH)

    def chip(k):
        k = chips - k
        return lax.rem(me_z + chips + lax.div(k + 1, 2) * (2 * lax.rem(k, 2) - 1), chips)

    def sum_over_tp(pair_phase, phase, part, pair, summed, arrived, make):
        def give(k):
            z = chip(k)
            at = 2 * z + 1 - core
            part[at] = make(at)
            tp_copy(pair_phase, part.at[at], pair.at[z], partner, z).start()

        def add(z):
            mine = make(2 * z + core)
            tp_copy(pair_phase, pair.at[z], pair.at[z], partner, z).wait_recv()
            return mine.astype(F32) + pair[z].astype(F32)

        def pass_on(k):
            z = chip(k)
            summed[z] = add(z).astype(BF16)
            tp_copy(phase, summed.at[z], arrived.at[me_z], 2 * z + core, 0).start()

        def both(k, _):
            give(k)
            pass_on(k - AHEAD)
            return 0

        def first(k, _):
            give(k)
            return 0

        def last(k, _):
            pass_on(k)
            return 0

        lax.fori_loop(1, AHEAD + 1, first, 0)
        lax.fori_loop(AHEAD + 1, chips + 1, both, 0)
        lax.fori_loop(chips + 1 - AHEAD, chips, last, 0)
        return add(me_z)

    def summed_over_tp(phase, arrived, acc):
        await_blocks(phase, arrived.at[pl.ds(0, chips - 1)])
        return others(me_z, chips, arrived, acc)

    def give_over_tp(phase, mine, spot):
        tp_copy(phase, mine, spot(me_t), partner, chips).start()

        def give(k, _):
            tp_copy(phase, mine, spot(me_t), 2 * chip(k) + core, me_z).start()
            return 0

        lax.fori_loop(1, chips, give, 0)

    def pass_over_tp(phase, spot):
        def pass_on(k, _):
            z = chip(chips - k)
            part = spot(2 * z + core)
            tp_copy(phase, part, part, 2 * z + core, z).wait_recv()
            tp_copy(phase, part, part, partner, chips).start()
            return 0

        lax.fori_loop(1, chips, pass_on, 0)

    def take_over_tp(phase, half):
        tp_copy(phase, half, half, partner, chips).wait_recv()

    def projection(t):
        return proj_all.at[t]

    def along_x(step):
        return side * me_y + lax.rem(me_x + step + side, side)

    def along_y(step):
        return side * lax.rem(me_y + step + side, side) + me_x

    def weight_copy(phase, buffer, block_of, peer, first, many, landing):
        part = buffer.at[block_of, pl.ds(first, many), :]
        return over(peer, me_t, phase, part, part, landing)

    def near(phase, buffer, me, along, first, many, part):
        for way, step in enumerate((1, -1)):
            weight_copy(phase, buffer, me, along(step), first, many, 2 * part + way).start()

    def arrived_near(phase, buffer, me, along, first, many, part):
        for way, step in enumerate((-1, 1)):
            owner = lax.rem(me + step + side, side)
            weight_copy(phase, buffer, owner, along(step), first, many, 2 * part + way).wait_recv()

    def far(phase, buffer, me, along, first, many, part, act):
        half = many // 2
        for way, step in enumerate((1, -1)):
            if act == "start":
                owner = lax.rem(me - step + side, side)
                weight_copy(phase, buffer, owner, along(step), first + way * half, half, 2 * part + way).start()
            else:
                owner = lax.rem(me + 2, side)
                weight_copy(phase, buffer, owner, along(-step), first + way * half, half, 2 * part + way).wait_recv()

    def give_weights(part):
        near(NEAR, dgu_all, me_x, along_x, *PARTS[part], part)

    def pass_weights(part):
        arrived_near(NEAR, dgu_all, me_x, along_x, *PARTS[part], part)
        far(FAR, dgu_all, me_x, along_x, *PARTS[part], part, "start")

    def gather_quarter():
        to_e = side * me_y + lax.rem(owned, side)
        spot = me_x * side + lax.div(owned, side)

        def give(k, _):
            over(to_e, 2 * chip(k) + core, RES, res_own, res_all.at[spot], spot).start()
            return 0

        lax.fori_loop(1, chips, give, 0)

        @pl.when(to_e != me_e)
        def _():
            over(to_e, me_t, RES, res_own, res_all.at[spot], spot).start()

        @pl.when(to_e == me_e)
        def _():
            res_all[spot] = res_own[...]

        pass_weights(2)
        arrived_near(NEAR_DOWN, dd_all, me_y, along_y, 0, hid_d, 0)
        far(FAR_DOWN, dd_all, me_y, along_y, 0, hid_d, 0, "start")

        def source(spot):
            o = side * lax.rem(spot, side) + me_x
            j = side * me_y + lax.div(spot, side)
            return j, lax.rem(o + j, n)

        def spot_of(k, parity):
            return (2 * lax.rem(k, 2) + parity) * side + lax.div(k, 2)

        def pass_on(k, _):
            spot = spot_of(k, lax.rem(core + me_x, 2))
            j, t = source(spot)

            @pl.when((j != me_e) | (t != me_t))
            def _():
                over(j, t, RES, res_all.at[spot], res_all.at[spot], spot).wait_recv()

            over(me_e, partner, RES, res_all.at[spot], res_all.at[spot], n).start()
            return 0

        lax.fori_loop(0, n // 2, pass_on, 0)

        half = res_all.at[pl.ds(0, chips)]
        over(me_e, partner, RES, half, half, n).wait_recv()

    def to_y_peers(phase, src_of, dst):
        def one(d, _):
            y = lax.rem(me_y + d, side)
            over(side * y + me_x, me_t, phase, src_of(y), dst, 0).start()
            return 0

        lax.fori_loop(1, side, one, 0)

    def steps(far_first):
        offsets = [(dy, dx) for dy in range(side) for dx in range(side) if dy or dx]
        cross = lambda o: sum(min(d, side - d) for d in o)
        return sorted(offsets, key=cross, reverse=far_first)

    def ep_at(dy, dx):
        return side * lax.rem(me_y + dy, side) + lax.rem(me_x + dx, side)

    def to_ep_peers(phase, src_of, dst):
        for dy, dx in steps(True):
            peer = ep_at(dy, dx)
            ep_copy(phase, src_of(peer), dst, peer, 0).start()

    def await_blocks(phase, blocks):
        over(me_e, partner, phase, blocks, blocks, 0).wait_recv()

    def others(me, many, buffer, acc):
        def one(d, acc):
            return acc + buffer[lax.rem(me + d, many)].astype(F32)

        return lax.fori_loop(1, many, one, acc)

    rest, few = pl.ds(0, n - 1), pl.ds(0, side - 1)
    far_first = (2, 1, 3, 0) if side == 4 else tuple(range(side))

    def sent(copy, phase, many):
        copy(phase, many, many, 0, 0).wait_send()

    loads[0].wait()
    to_ep_peers(TOK,
             lambda peer: tok.at[:, pl.ds(pl.multiple_of(peer * block, block), block)],
             tok_all.at[me_e])
    tok_all[me_e] = tok[:, pl.ds(pl.multiple_of(me_e * block, block), block)]

    loads[16].wait()
    give_over_tp(PROJ, projection(me_t), projection)
    loads[17].wait()
    loads[18].wait()
    give_weights(0)

    loads[4].wait()
    loads[5].wait()
    route_rows = [routes[pl.ds(k, 1), :] for k in range(2)]
    lanes_e = iota((128, rows), 0)
    named = sum(jnp.where(lanes_e == r, 1.0, 0.0) for r in route_rows)
    earlier = jnp.where(iota((rows, rows), 0) < iota((rows, rows), 1), 1.0, 0.0)
    before = jnp.dot(named.astype(BF16), earlier.astype(BF16), preferred_element_type=F32)
    base = (CAP * me_y).astype(F32)
    key = jnp.where(named > 0.0, before + base, -1.0)
    eye = jnp.where(iota((rows, rows), 0) == iota((rows, rows), 1), 1.0, 0.0)
    key_all[me_y] = lax.dot_general(
        eye.astype(BF16), key.astype(BF16), NT, preferred_element_type=F32).astype(BF16)
    to_y_peers(KEY, lambda y: key_all.at[me_y], key_all.at[me_y])
    weights = [rw[pl.ds(k, 1), :] for k in range(2)]
    total = weights[0] + weights[1]
    spots = iota((n * SLOT, rows), 0)
    share_t = jnp.zeros((n * SLOT, rows), F32)
    for r, w in zip(route_rows, weights):
        slot = jnp.sum(jnp.where(lanes_e == r, before, 0.0), axis=0, keepdims=True)
        hit = (spots.astype(F32) == r.astype(F32) * SLOT + slot)
        share_t = share_t + jnp.where(hit, w / total, 0.0)
    ret_w[...] = lax.dot_general(eye, share_t, NT, precision=HIGHEST, preferred_element_type=F32)

    loads[1].wait()
    squares = jnp.zeros((rows, block), F32)
    for k in range(n):
        part = tok[:, k * block:(k + 1) * block].astype(F32)
        squares = squares + part * part
    scale = lax.rsqrt(jnp.sum(squares, axis=1, keepdims=True) / width + EPS)
    loads[6].wait()
    loads[7].wait()
    gate = jnp.zeros((rows, 2 * n), F32)
    for k in range(n):
        cols = slice(k * block, (k + 1) * block)
        gain = mgain[:, cols]
        normed = (tok[:, cols].astype(F32) * scale * gain).astype(BF16)
        gate = gate + lax.dot_general(normed, wgates[:, cols], NT, preferred_element_type=F32)
    for k in range(8, 11):
        loads[k].wait()
    lane = iota((rows, 2 * n), 1)
    gate_in = jnp.sum(jnp.where(lane == me_t, gate, 0.0), axis=1, keepdims=True)
    gate_forget = jnp.sum(jnp.where(lane == me_t + n, gate, 0.0), axis=1, keepdims=True)
    bias = jnp.sum(jnp.where(iota((1, n), 1) == me_t, fbias[...], 0.0), axis=1, keepdims=True)
    gate_forget = gate_forget + bias
    log_keep = jnp.minimum(gate_forget, 0.0) - jnp.log1p(jnp.exp(-jnp.abs(gate_forget)))
    old_max = to_column(smax[...], rows)
    new_max = jnp.maximum(log_keep + old_max, gate_in)
    keep = jnp.exp(log_keep + old_max - new_max)
    write = jnp.exp(gate_in - new_max)
    nmax[...] = to_row(new_max, rows)

    await_blocks(TOK, tok_all.at[rest])
    for k in range(11, 15):
        loads[k].wait()
    gain_m = mgain[:, pl.ds(pl.multiple_of(me_e * block, block), block)]

    def project(dy):
        at = pl.multiple_of(side * lax.rem(me_y + dy, side), side)
        x = tok_all[pl.ds(at, side)].reshape(quarter, block).astype(F32) * gain_m
        y = jnp.dot(x.astype(BF16), wqkv[...], preferred_element_type=F32)
        qkv_part[pl.ds(at, side)] = y.astype(BF16).reshape(side, rows, 4 * head)
        for dx in far_first:
            if dy or dx:
                peer = ep_at(dy, dx)
                ep_copy(QKV, qkv_part.at[peer], qkv_in.at[me_e], peer, 0).start()

    for dy in far_first:
        project(dy)
    give_weights(1)

    loads[15].wait()
    await_blocks(QKV, qkv_in.at[rest])
    y = others(me_e, n, qkv_in, qkv_part[me_e].astype(F32)) * scale
    query = y[:, :head]
    keys = y[:, head:2 * head] * head ** (-0.5)
    value = y[:, 2 * head:3 * head]
    outgate = y[:, 3 * head:]
    written = write * keys
    new_norm = keep * sn[...] + written
    nn[...] = new_norm
    denom = jnp.sum(query * new_norm, axis=1, keepdims=True)
    qt[...] = query.T
    wkt[...] = written.T
    vrow[...] = value
    keep_rows[...] = jnp.broadcast_to(keep, (rows, head))
    for b in range(rows):
        numer[pl.ds(b, 1), :] = jnp.sum(qt[:, b:b + 1] * sm[b], axis=0, keepdims=True)
    dots = jnp.sum(query * written, axis=1, keepdims=True)
    num = keep * numer[...] + dots * value
    cell = num / jnp.maximum(jnp.abs(denom), 1.0)
    mix_own[...] = (jax.nn.sigmoid(outgate) * cell).astype(BF16)

    def head_place(h):
        return mix_in.at[:, pl.ds(pl.multiple_of(h * head, head), head)]

    for dy, dx in steps(True):
        j = ep_at(dy, dx)
        over(j, lax.rem(me_e + j, n), MIX, mix_own, head_place(me_t), 0).start()

    @pl.when(owned != me_e)
    def _():
        over(me_e, lax.rem(2 * me_e, n), MIX, mix_own, head_place(me_t), 0).start()

    @pl.when(owned == me_e)
    def _():
        mix_in[:, pl.ds(pl.multiple_of(me_t * head, head), head)] = mix_own[...]

    give_weights(2)
    loads[22].wait()
    near(NEAR_DOWN, dd_all, me_y, along_y, 0, hid_d, 0)
    pass_over_tp(PROJ, projection)
    pass_weights(0)
    pass_weights(1)
    for b in range(rows):
        nm[b] = keep_rows[pl.ds(b, 1), :] * sm[b] + wkt[:, b:b + 1] * vrow[pl.ds(b, 1), :]

    await_blocks(KEY, key_all.at[few])
    key_t = lax.dot_general(
        jnp.where(iota((n, 128), 0) == iota((n, 128), 1), 1.0, 0.0).astype(BF16),
        key_all[...].reshape(quarter, 128), NT, preferred_element_type=F32)
    places = iota((few_rows, quarter), 0).astype(F32)
    for e in range(0, n, 2):
        both = [jnp.where(places == key_t[k:k + 1, :], 1.0, 0.0) for k in (e, e + 1)]
        pick[pl.ds(e * few_rows, 2 * few_rows), :] = jnp.concatenate(both, axis=0).astype(BF16)

    take_over_tp(PROJ, proj_all.at[pl.ds(0, chips)])

    @pl.when(owned != me_e)
    def _():
        await_blocks(MIX, mix_in)

    @pl.when(owned == me_e)
    def _():
        await_blocks(MIX, mix_in.at[:, pl.ds(0, (n - 1) * head)])

    mixed = jnp.dot(mix_in[...], proj_all[...].reshape(n * head, block), preferred_element_type=F32)
    residual = (tok_all[owned].astype(F32) + mixed).astype(BF16)
    res_own[...] = residual

    def to_final():
        return pltpu.make_async_remote_copy(
            src_ref=res_own, dst_ref=res_fin, send_sem=res_sem.at[0], recv_sem=res_sem.at[1],
            device_id=(owned, me_e), device_id_type=MESH)

    corner = (owned == me_e) & (me_e == me_t)

    gather_quarter()

    @pl.when(jnp.logical_not(corner))
    def _():
        to_final().start()

    @pl.when(corner)
    def _():
        res_fin[...] = res_own[...]

    loads[2].wait()
    loads[3].wait()

    def pass_rows(peer):
        part = row_in.at[core * n + peer]
        tp_copy(ROW, part, part, partner, n + lax.div(peer, side)).start()

    half_side = side // 2
    res_half = jnp.concatenate(
        [res_all[pl.ds((core * half_side + k) * side, side)].reshape(quarter, block)
         for k in range(half_side)], axis=1)

    def dispatch(dy):
        at = pl.multiple_of(side * lax.rem(me_y + dy, side), side)
        y = jnp.dot(pick[pl.ds(pl.multiple_of(at * few_rows, side * few_rows), side * few_rows), :],
                    res_half, preferred_element_type=F32)
        y = y.reshape(side, few_rows, half_side * block)
        row_out[pl.ds(at, side)] = jnp.concatenate(
            [y[:, :, k * block:(k + 1) * block] for k in range(half_side)], axis=1).astype(BF16)
        for dx in far_first:
            if dy or dx:
                peer, spot = ep_at(dy, dx), core * n + me_e
                ep_copy(ROW, row_out.at[peer], row_in.at[spot], peer, me_e).start()

    for dy in far_first:
        dispatch(dy)
    row_in[core * n + me_e] = row_out[me_e]
    pass_rows(me_e)

    wbr_wide[...] = wbr[...].astype(F32)
    lines = block // 128
    squares = [jnp.zeros((rows, 1), F32)] * side
    branches = [jnp.zeros((rows, 1), F32)] * side
    for k in range(side):
        j = side * me_y + k
        gain_f = fgain[:, pl.ds(pl.multiple_of(j * block, block), block)]
        gain_b = gain_f * jnp.concatenate(
            [wbr_wide[pl.ds(j * lines + i, 1), :] for i in range(lines)], axis=1)
        for g in range(side):
            r = res_all[k * side + g].astype(F32)
            squares[g] = squares[g] + jnp.sum(r * r, axis=1, keepdims=True)
            branches[g] = branches[g] + jnp.sum(r * gain_b, axis=1, keepdims=True)
            x_cat[pl.ds(g * rows, rows), k * block:(k + 1) * block] = (r * gain_f).astype(BF16)
    for g in range(side):
        sta_out[g] = jnp.where(iota((8, 128), 0) == 0, to_row(squares[g], 128), to_row(branches[g], 128))
    to_y_peers(STA, lambda y: sta_out.at[y], sta_in.at[me_y])

    for part, (first, many) in enumerate(PARTS):
        far(FAR, dgu_all, me_x, along_x, first, many, part, "wait")
    weights = dgu_all[...].reshape(side * block, 2 * hid_d)
    x = x_cat[...]
    for k in range(2 * hid_d // block):
        y = jnp.dot(x, weights[:, k * block:(k + 1) * block], preferred_element_type=F32)
        den_part[:, :, k * block:(k + 1) * block] = y.astype(BF16).reshape(side, rows, block)
    to_y_peers(DEN, lambda y: den_part.at[y], den_in.at[me_y])

    loads[19].wait()
    loads[20].wait()

    deep = half_side * block

    def expert_in(y, half, ss):
        x = row_in[pl.ds(half * n + y * side, side)].astype(F32)
        x = jnp.concatenate(
            [x[:, k * few_rows:(k + 1) * few_rows].reshape(cap_rows, block) for k in range(half_side)], axis=1)
        at = pl.multiple_of(y * side * block + half * deep, deep)
        xg = (x * fgain[:, pl.ds(at, deep)]).astype(BF16)
        gu_acc[:, pl.ds(0, hid_e)] += jnp.dot(xg, eg[pl.ds(at, deep), :], preferred_element_type=F32)
        gu_acc[:, pl.ds(hid_e, hid_e)] += jnp.dot(xg, eu[pl.ds(at, deep), :], preferred_element_type=F32)
        return ss + jnp.sum(x * x, axis=1, keepdims=True)

    def expert_first(d, ss):
        y = lax.rem(me_y + side - d, side)

        def one(k, _):
            peer = side * y + lax.rem(me_x + k, side)
            spot = core * n + peer

            @pl.when(peer != me_e)
            def _():
                ep_copy(ROW, row_in.at[spot], row_in.at[spot], peer, peer).wait_recv()
                pass_rows(peer)

            return 0

        lax.fori_loop(0, side, one, 0)
        return expert_in(y, core, ss)

    def expert_second(d, ss):
        y = lax.rem(me_y + side - d, side)

        part = row_in.at[pl.ds((1 - core) * n + side * y, side)]
        tp_copy(ROW, part, part, partner, n + y).wait_recv()
        return expert_in(y, 1 - core, ss)

    gu_acc[...] = jnp.zeros_like(gu_acc)
    ss = expert_first(0, jnp.zeros((cap_rows, 1), F32))
    ss = lax.fori_loop(1, side, lambda d, ss: expert_second(d - 1, expert_first(d, ss)), ss)
    ss = expert_second(side - 1, ss)
    row_scale = lax.rsqrt(ss / width + EPS)
    g = gu_acc[:, :hid_e] * row_scale
    u = gu_acc[:, hid_e:] * row_scale
    hidden_e[...] = (g / (1.0 + jnp.exp(-g)) * u).astype(BF16)
    loads[21].wait()

    def expert_out(at):
        return jnp.dot(hidden_e[...], ed[:, pl.ds(pl.multiple_of(at * block, block), block)],
                       preferred_element_type=F32).astype(BF16)

    routed_sum = sum_over_tp(
        EXP_PAIR, EXP, exp_part, exp_pair, exp_sum, exp_in, expert_out)

    await_blocks(STA, sta_in.at[few])
    sums = others(me_y, side, sta_in, sta_out[me_y])
    dense_scale = lax.rsqrt(to_column(sums[0:1, :], rows) / width + EPS)
    branch = jax.nn.sigmoid(to_column(sums[1:2, :], rows) * dense_scale)
    await_blocks(DEN, den_in.at[few])
    y = others(me_y, side, den_in, den_part[me_y].astype(F32)) * dense_scale
    g, u = y[:, :hid_d], y[:, hid_d:]
    hid_all[me_x] = (g / (1.0 + jnp.exp(-g)) * u * branch).astype(BF16)

    def spread_hidden(d, _):
        over(along_x(d), me_t, HID, hid_all.at[me_x], hid_all.at[me_x], me_x).start()
        return 0

    lax.fori_loop(1, side, spread_hidden, 0)

    far(FAR_DOWN, dd_all, me_y, along_y, 0, hid_d, 0, "wait")

    def hidden_of(d, _):
        x = lax.rem(me_x + side - d, side)
        over(along_x(-d), me_t, HID, hid_all.at[x], hid_all.at[x], x).wait_recv()
        return 0

    lax.fori_loop(1, side, hidden_of, 0)
    x = hid_all[...].reshape(quarter, hid_d)
    for k in range(side):
        y = jnp.dot(x, dd_all[k], preferred_element_type=F32)
        dwn_part[pl.ds(k * side, side)] = y.astype(BF16).reshape(side, rows, block)
    end_core = lax.rem(me_x, 2)
    home = lax.rem(me_t, side) == me_x

    @pl.when(core != end_core)
    def _():
        tp_copy(DWN_PAIR, dwn_part, dwn_pair, partner, 0).start()

    @pl.when(core == end_core)
    def _():
        tp_copy(DWN_PAIR, dwn_pair, dwn_pair, partner, 0).wait_recv()
        for dx in far_first:
            def to_end(c, _):
                x = lax.rem(me_x + dx, side)
                k = side * c + x
                dwn_sum[k] = (dwn_part[k].astype(F32) + dwn_pair[k].astype(F32)).astype(BF16)
                z = 2 * c + lax.div(me_x, 2)
                here = (x == me_x) & (z == me_z)

                @pl.when(jnp.logical_not(here))
                def _():
                    over(side * me_y + x, 2 * z + core, DWN, dwn_sum.at[k], dwn_in.at[me_z], 0).start()

                @pl.when(here)
                def _():
                    dwn_in[me_z] = dwn_sum[k]

                return 0

            lax.fori_loop(0, side, to_end, 0)

    y = summed_over_tp(EXP, exp_in, routed_sum)
    spot, col = iota((n * SLOT, cap_rows), 0), iota((n * SLOT, cap_rows), 1)
    within = jnp.bitwise_and(spot, SLOT - 1)
    shift = side.bit_length() - 1
    from_e = jnp.right_shift(spot, SLOT.bit_length() - 1)
    source = few_rows * jnp.bitwise_and(from_e, side - 1) + CAP * jnp.right_shift(from_e, shift) + within
    spread = jnp.where((source == col) & (within < CAP), 1.0, 0.0).astype(BF16)
    ret_out[...] = jnp.dot(
        spread, y.astype(BF16), preferred_element_type=F32).reshape(n, SLOT, block).astype(BF16)

    to_ep_peers(RET, lambda peer: ret_out.at[peer], ret_in.at[me_e])
    ret_in[me_e] = ret_out[me_e]

    await_blocks(RET, ret_in.at[rest])

    @pl.when(jnp.logical_not(corner))
    def _():
        to_final().wait()

    routed = jnp.dot(ret_w[...], ret_in[...].astype(F32).reshape(n * SLOT, block), precision=HIGHEST,
                     preferred_element_type=F32)
    known = res_fin[...].astype(F32) + routed

    @pl.when(home)
    def _():
        await_blocks(DWN, dwn_in.at[pl.ds(0, chips - 1)])

    @pl.when(jnp.logical_not(home))
    def _():
        await_blocks(DWN, dwn_in)

    y = others(me_z, chips, dwn_in, dwn_in[me_z].astype(F32))
    out_own[...] = (known + y).astype(BF16)

    def columns(j):
        return out.at[:, pl.ds(pl.multiple_of(j * block, block), block)]

    give_over_tp(OUT, out_own, columns)
    out[:, pl.ds(pl.multiple_of(me_t * block, block), block)] = out_own[...]
    pass_over_tp(OUT, columns)
    take_over_tp(OUT, out.at[:, pl.ds(0, chips * block)])
    sent(ep_copy, TOK, tok_all.at[rest])
    sent(ep_copy, KEY, key_all.at[few])
    sent(ep_copy, QKV, qkv_part.at[rest])
    some = pl.ds(0, chips - 1)

    @pl.when(owned != me_e)
    def _():
        sent(ep_copy, MIX, mix_in)

    @pl.when(owned == me_e)
    def _():
        sent(ep_copy, MIX, mix_in.at[:, pl.ds(0, (n - 1) * head)])

    sent(tp_copy, PROJ, proj_all.at[rest])
    sent(ep_copy, ROW, row_in.at[pl.ds(0, 2 * n - 1)])
    sent(ep_copy, STA, sta_out.at[few])
    sent(ep_copy, DEN, den_part.at[few])
    sent(ep_copy, HID, hid_all.at[few])
    for phase, buffer, rows_of in (
        (NEAR, dgu_all, block), (FAR, dgu_all, block // 2),
        (NEAR_DOWN, dd_all, hid_d), (FAR_DOWN, dd_all, hid_d // 2)):
        sent(ep_copy, phase, buffer.at[pl.ds(0, 2), pl.ds(0, rows_of), :])
    sent(tp_copy, EXP_PAIR, exp_pair)
    sent(tp_copy, EXP, exp_sum.at[some])
    sent(ep_copy, RET, ret_out.at[rest])
    sent(tp_copy, OUT, tok_all.at[rest])

    @pl.when(core != end_core)
    def _():
        sent(tp_copy, DWN_PAIR, dwn_part)

    @pl.when(home)
    def _():
        sent(ep_copy, DWN, dwn_sum.at[rest])

    @pl.when((core == end_core) & jnp.logical_not(home))
    def _():
        sent(ep_copy, DWN, dwn_sum)

    own_column = lax.rem(owned, side) == me_x

    @pl.when(jnp.logical_not(own_column))
    def _():
        sent(ep_copy, RES, res_all)

    @pl.when(own_column)
    def _():
        sent(ep_copy, RES, res_all.at[rest])


def put_out(*refs):
    *arrays, sem = refs
    copies = [pltpu.make_async_copy(arrays[k], arrays[4 + k], sem.at[k]) for k in range(4)]
    for copy in copies:
        copy.start()
    for copy in copies:
        copy.wait()


def on_device(
    n, tokens, state_matrix, state_norm, state_max, mixer_gain, w_query, w_key, w_value, w_outgate,
    w_ingate, w_forget, forget_bias, w_proj, ffn_gain, w_branch, routes, route_weight,
    expert_gate, expert_up, expert_down, dense_gate, dense_up, dense_down,
):
    rows, width = tokens.shape
    head = state_norm.shape[-1]
    block = width // n
    hid_e, hid_d = expert_gate.shape[2], dense_gate.shape[1]
    cap_rows = CAP * n
    args = (
        tokens,
        state_matrix.reshape(rows, head, head),
        state_norm.reshape(rows, head),
        state_max.T,
        mixer_gain.reshape(1, width),
        w_query, w_key, w_value, w_outgate,
        w_ingate.T, w_forget.T,
        forget_bias.reshape(1, n),
        w_proj,
        ffn_gain.reshape(1, width),
        w_branch.reshape(width // 128, 128),
        routes.T, route_weight.T,
        expert_gate.reshape(width, hid_e), expert_up.reshape(width, hid_e),
        expert_down.reshape(hid_e, width),
        dense_gate, dense_up, dense_down,
    )
    vm = pltpu.VMEM
    dma = pltpu.SemaphoreType.DMA
    few_rows, side = CAP * math.isqrt(n), math.isqrt(n)

    def hier(tall):
        return [vm((n, tall, block), BF16)] + [vm((n // 2, tall, block), BF16)] * 3

    scratch = [
        vm((rows, width), BF16), vm((rows, head, head), F32), vm((rows, head), F32), vm((1, rows), F32),
        vm((1, width), F32), vm((block, 4 * head), BF16), vm((2 * n, width), BF16), vm((1, n), F32),
        vm((n, head, block), BF16), vm((1, width), F32), vm((width // 128, 128), BF16), vm((2, rows), jnp.int32),
        vm((2, rows), F32), vm((width, hid_e), BF16), vm((width, hid_e), BF16), vm((hid_e, width), BF16),
        vm((side, block, 2 * hid_d), BF16), vm((side, hid_d, block), BF16),
        vm((n, rows, block), BF16), vm((side, rows, 128), BF16),
        vm((n, rows, 4 * head), BF16), vm((n, rows, 4 * head), BF16),
        vm((rows, head), BF16), vm((rows, n * head), BF16),
        vm((rows, block), BF16), vm((n, rows, block), BF16), vm((rows, block), BF16),
        vm((n, few_rows * side // 2, block), BF16), vm((2 * n, few_rows * side // 2, block), BF16),
        vm((side, 8, 128), F32), vm((side, 8, 128), F32),
        vm((side, rows, 2 * hid_d), BF16), vm((side, rows, 2 * hid_d), BF16),
        vm((side, rows, hid_d), BF16), *[vm((n, rows, block), BF16)] * 3, vm((n // 2, rows, block), BF16),
        *hier(cap_rows),
        vm((n, SLOT, block), BF16), vm((n, SLOT, block), BF16),
        vm((rows, block), BF16),
        vm((width // 128, 128), F32),
        vm((n * few_rows, side * rows), BF16), vm((side * rows, side * block), BF16), vm((cap_rows, hid_e), BF16), vm((cap_rows, 2 * hid_e), F32), vm((rows, 2 * n), F32),
        vm((head, rows), F32), vm((head, rows), F32), vm((rows, head), F32), vm((rows, head), F32),
        vm((rows, head), F32), vm((rows, n * SLOT), F32),
        dma((len(args),)), dma((PHASES,)), dma((landing_spots(n)[1],)), dma((2,)),
    ]
    any_space = pl.BlockSpec(memory_space=pl.ANY)
    layer_out, new_matrix, new_norm, new_max = pl.pallas_call(
        functools.partial(layer_kernel, n),
        out_shape=(
            vm((rows, width), BF16), vm((rows, head, head), F32), vm((rows, head), F32), vm((1, rows), F32),
        ),
        in_specs=[any_space] * len(args),
        out_specs=[pl.BlockSpec(memory_space=vm)] * 4,
        scratch_shapes=scratch,
        compiler_params=pltpu.CompilerParams(
            collective_id=0, has_side_effects=True, vmem_limit_bytes=56 * 1024 * 1024),
        name="layer",
    )(*args)
    results = (layer_out, new_matrix, new_norm, new_max)
    results = tuple(pltpu.with_memory_space_constraint(r, vm) for r in results)
    layer_out, new_matrix, new_norm, new_max = pl.pallas_call(
        put_out,
        out_shape=tuple(jax.ShapeDtypeStruct(r.shape, r.dtype) for r in results),
        in_specs=[pl.BlockSpec(memory_space=vm)] * 4,
        out_specs=[any_space] * 4,
        scratch_shapes=[dma((4,))],
        name="put_out",
    )(*results)
    return (layer_out, new_matrix.reshape(rows, 1, head, head), new_norm.reshape(rows, 1, head), new_max.T)


def solution(mesh):
    n = mesh.shape["ep"]
    in_specs = (
        P("ep", None),
        P("ep", "tp", None, None),
        P("ep", "tp", None),
        P("ep", "tp"),
        P(),
        P("ep", "tp"),
        P("ep", "tp"),
        P("ep", "tp"),
        P("ep", "tp"),
        P(),
        P(),
        P(),
        P("tp", "ep"),
        P(),
        P(),
        P("ep", None),
        P("ep", None),
        P("ep", None, "tp"),
        P("ep", None, "tp"),
        P("ep", "tp", None),
        P("ep", "tp"),
        P("ep", "tp"),
        P("tp", "ep"),
    )
    out_specs = (P("ep", None), P("ep", "tp", None, None), P("ep", "tp", None), P("ep", "tp"))
    return jax.shard_map(
        functools.partial(on_device, n), mesh=mesh, in_specs=in_specs, out_specs=out_specs,
        check_vma=False)
```

```python
import functools
import math

import jax
import jax.numpy as jnp
from jax import lax
from jax.experimental import pallas as pl
from jax.experimental.pallas import tpu as pltpu
from jax.sharding import PartitionSpec as P

EPS = 1e-06
MESH = pl.DeviceIdType.MESH
CAP = 6
SLOT = 8
F32 = jnp.float32
BF16 = jnp.bfloat16
HIGHEST = lax.Precision.HIGHEST
NT = (((1,), (1,)), ((), ()))


def landing_spots(n):
    side = math.isqrt(n)
    many = {ROW: n + side, RES: n + 1, NEAR: 6, FAR: 6, NEAR_DOWN: 2, FAR_DOWN: 2, HID: side}
    for phase in (TOK, KEY, QKV, STA, DEN, RET, MIX, DWN, DWN_PAIR, EXP):
        many[phase] = 1
    many[EXP_PAIR] = n // 2
    many[PROJ] = many[OUT] = n // 2 + 1
    first, at = [], 0
    for phase in range(PHASES):
        first.append(at)
        at += many.get(phase, n)
    return first, at


def iota(shape, dim):
    return lax.broadcasted_iota(jnp.int32, shape, dim)


def loop(first, end, body, carry):
    for k in range(first, end):
        carry = body(k, carry)
    return carry


def to_column(row, rows):
    diag = iota((rows, row.shape[1]), 0) == iota((rows, row.shape[1]), 1)
    return jnp.sum(jnp.where(diag, row, 0.0), axis=1, keepdims=True)


def to_row(column, lanes):
    rows = column.shape[0]
    diag = iota((rows, lanes), 0) == iota((rows, lanes), 1)
    return jnp.sum(jnp.where(diag, column, 0.0), axis=0, keepdims=True)


(TOK, KEY, QKV, MIX, PROJ, RES, ROW, STA, DEN, HID, DWN_PAIR, DWN, EXP_PAIR, EXP, RET,
 OUT, NEAR, FAR, NEAR_DOWN, FAR_DOWN) = range(20)
PHASES = 20
AHEAD = 3
PARTS = ((0, 64), (64, 64), (128, 128))


def layer_kernel(
    n,
    tok_h, sm_h, sn_h, smax_h, mgain_h, wq_h, wk_h, wv_h, wo_h, win_h, wfo_h, fbias_h,
    wproj_h, fgain_h, wbr_h, routes_h, rw_h, eg_h, eu_h, ed_h, dg_h, du_h, dd_h,
    out, nm, nn, nmax,
    tok, sm, sn, smax, mgain, wqkv, wgates, fbias, proj_all, fgain, wbr, routes, rw,
    eg, eu, ed, dgu_all, dd_all,
    tok_all, key_all, qkv_part, qkv_in, mix_own, mix_in, res_own, res_all, res_fin,
    row_out, row_in, sta_out, sta_in, den_part, den_in, hid_all, dwn_part, dwn_pair, dwn_sum, dwn_in,
    exp_part, exp_pair, exp_sum, exp_in, ret_out, ret_in, out_own,
    wbr_wide, pick, x_cat, hidden_e, gu_acc, gates, wkt, qt, vrow, keep_rows, numer, ret_w,
    load_sem, send_sem, recv_sem, res_sem,
):
    me_e, me_t = lax.axis_index("ep"), lax.axis_index("tp")
    chips = n // 2
    first_spot, _ = landing_spots(n)
    side = math.isqrt(n)
    me_y, me_x = lax.div(me_e, side), lax.rem(me_e, side)
    me_z, core = lax.div(me_t, 2), lax.rem(me_t, 2)
    partner = me_t + 1 - 2 * core
    owned = lax.rem(me_t - me_e + n, n)
    rows = tok.shape[0]
    width = tok.shape[1]
    block = width // n
    head = sn.shape[1]
    hid_e = eg.shape[1]
    hid_d = dd_all.shape[1]
    quarter = rows * side
    cap_rows = CAP * n
    few_rows = CAP * side
    dgu, dd = dgu_all.at[me_x], dd_all.at[me_y]

    loads = [
        (tok_h, tok), (mgain_h, mgain), (fgain_h, fgain), (wbr_h, wbr), (routes_h, routes),
        (rw_h, rw), (win_h, wgates.at[pl.ds(0, n), :]), (wfo_h, wgates.at[pl.ds(n, n), :]),
        (fbias_h, fbias), (smax_h, smax), (sn_h, sn),
        (wq_h, wqkv.at[:, pl.ds(0, head)]), (wk_h, wqkv.at[:, pl.ds(head, head)]),
        (wv_h, wqkv.at[:, pl.ds(2 * head, head)]), (wo_h, wqkv.at[:, pl.ds(3 * head, head)]),
        (sm_h, sm), (wproj_h, proj_all.at[me_t]), (dg_h, dgu_all.at[me_x, :, pl.ds(0, hid_d)]),
        (du_h, dgu_all.at[me_x, :, pl.ds(hid_d, hid_d)]), (eg_h, eg), (eu_h, eu), (ed_h, ed), (dd_h, dd),
    ]
    loads = [pltpu.make_async_copy(a, b, load_sem.at[k]) for k, (a, b) in enumerate(loads)]
    for copy in loads:
        copy.start()

    barrier = pltpu.get_barrier_semaphore()

    def greet(d, _):
        pl.semaphore_signal(barrier, 1, device_id=(lax.rem(me_e + d, n), me_t), device_id_type=MESH)
        pl.semaphore_signal(barrier, 1, device_id=(me_e, lax.rem(me_t + d, n)), device_id_type=MESH)
        return 0

    lax.fori_loop(1, n, greet, 0)
    pl.semaphore_wait(barrier, 2 * n - 2)

    def ep_copy(phase, src, dst, peer, landing):
        return pltpu.make_async_remote_copy(
            src_ref=src, dst_ref=dst, send_sem=send_sem.at[phase],
            recv_sem=recv_sem.at[first_spot[phase] + landing], device_id=(peer, me_t), device_id_type=MESH)

    def tp_copy(phase, src, dst, peer, landing):
        return pltpu.make_async_remote_copy(
            src_ref=src, dst_ref=dst, send_sem=send_sem.at[phase],
            recv_sem=recv_sem.at[first_spot[phase] + landing], device_id=(me_e, peer), device_id_type=MESH)

    def over(peer_e, peer_t, phase, src, dst, landing):
        return pltpu.make_async_remote_copy(
            src_ref=src, dst_ref=dst, send_sem=send_sem.at[phase],
            recv_sem=recv_sem.at[first_spot[phase] + landing], device_id=(peer_e, peer_t), device_id_type=MESH)

    def chip(k):
        k = chips - k
        return lax.rem(me_z + chips + lax.div(k + 1, 2) * (2 * lax.rem(k, 2) - 1), chips)

    def sum_over_tp(pair_phase, phase, part, pair, summed, arrived, make):
        def give(k):
            z = chip(k)
            at = 2 * z + 1 - core
            part[at] = make(at)
            tp_copy(pair_phase, part.at[at], pair.at[z], partner, z).start()

        def add(z):
            mine = make(2 * z + core)
            tp_copy(pair_phase, pair.at[z], pair.at[z], partner, z).wait_recv()
            return mine.astype(F32) + pair[z].astype(F32)

        def pass_on(k):
            z = chip(k)
            summed[z] = add(z).astype(BF16)
            tp_copy(phase, summed.at[z], arrived.at[me_z], 2 * z + core, 0).start()

        def both(k, _):
            give(k)
            pass_on(k - AHEAD)
            return 0

        def first(k, _):
            give(k)
            return 0

        def last(k, _):
            pass_on(k)
            return 0

        loop(1, AHEAD + 1, first, 0)
        loop(AHEAD + 1, chips + 1, both, 0)
        loop(chips + 1 - AHEAD, chips, last, 0)
        return add(me_z)

    def summed_over_tp(phase, arrived, acc):
        await_blocks(phase, arrived.at[pl.ds(0, chips - 1)])
        return others(me_z, chips, arrived, acc)

    def give_over_tp(phase, mine, spot):
        tp_copy(phase, mine, spot(me_t), partner, chips).start()

        def give(k, _):
            tp_copy(phase, mine, spot(me_t), 2 * chip(k) + core, me_z).start()
            return 0

        lax.fori_loop(1, chips, give, 0)

    def pass_over_tp(phase, spot):
        def pass_on(k, _):
            z = chip(chips - k)
            part = spot(2 * z + core)
            tp_copy(phase, part, part, 2 * z + core, z).wait_recv()
            tp_copy(phase, part, part, partner, chips).start()
            return 0

        lax.fori_loop(1, chips, pass_on, 0)

    def take_over_tp(phase, half):
        tp_copy(phase, half, half, partner, chips).wait_recv()

    def projection(t):
        return proj_all.at[t]

    def along_x(step):
        return side * me_y + lax.rem(me_x + step + side, side)

    def along_y(step):
        return side * lax.rem(me_y + step + side, side) + me_x

    def weight_copy(phase, buffer, block_of, peer, first, many, landing):
        part = buffer.at[block_of, pl.ds(first, many), :]
        return over(peer, me_t, phase, part, part, landing)

    def near(phase, buffer, me, along, first, many, part):
        for way, step in enumerate((1, -1)):
            weight_copy(phase, buffer, me, along(step), first, many, 2 * part + way).start()

    def arrived_near(phase, buffer, me, along, first, many, part):
        for way, step in enumerate((-1, 1)):
            owner = lax.rem(me + step + side, side)
            weight_copy(phase, buffer, owner, along(step), first, many, 2 * part + way).wait_recv()

    def far(phase, buffer, me, along, first, many, part, act):
        half = many // 2
        for way, step in enumerate((1, -1)):
            if act == "start":
                owner = lax.rem(me - step + side, side)
                weight_copy(phase, buffer, owner, along(step), first + way * half, half, 2 * part + way).start()
            else:
                owner = lax.rem(me + 2, side)
                weight_copy(phase, buffer, owner, along(-step), first + way * half, half, 2 * part + way).wait_recv()

    def give_weights(part):
        near(NEAR, dgu_all, me_x, along_x, *PARTS[part], part)

    def pass_weights(part):
        arrived_near(NEAR, dgu_all, me_x, along_x, *PARTS[part], part)
        far(FAR, dgu_all, me_x, along_x, *PARTS[part], part, "start")

    def gather_quarter():
        to_e = side * me_y + lax.rem(owned, side)
        spot = me_x * side + lax.div(owned, side)

        def give(k, _):
            over(to_e, 2 * chip(k) + core, RES, res_own, res_all.at[spot], spot).start()
            return 0

        lax.fori_loop(1, chips, give, 0)

        @pl.when(to_e != me_e)
        def _():
            over(to_e, me_t, RES, res_own, res_all.at[spot], spot).start()

        @pl.when(to_e == me_e)
        def _():
            res_all[spot] = res_own[...]

        pass_weights(2)
        arrived_near(NEAR_DOWN, dd_all, me_y, along_y, 0, hid_d, 0)
        far(FAR_DOWN, dd_all, me_y, along_y, 0, hid_d, 0, "start")

        def source(spot):
            o = side * lax.rem(spot, side) + me_x
            j = side * me_y + lax.div(spot, side)
            return j, lax.rem(o + j, n)

        def spot_of(k, parity):
            return (2 * lax.rem(k, 2) + parity) * side + lax.div(k, 2)

        def pass_on(k, _):
            spot = spot_of(k, lax.rem(core + me_x, 2))
            j, t = source(spot)

            @pl.when((j != me_e) | (t != me_t))
            def _():
                over(j, t, RES, res_all.at[spot], res_all.at[spot], spot).wait_recv()

            over(me_e, partner, RES, res_all.at[spot], res_all.at[spot], n).start()
            return 0

        lax.fori_loop(0, n // 2, pass_on, 0)

        half = res_all.at[pl.ds(0, chips)]
        over(me_e, partner, RES, half, half, n).wait_recv()

    def to_y_peers(phase, src_of, dst):
        def one(d, _):
            y = lax.rem(me_y + d, side)
            over(side * y + me_x, me_t, phase, src_of(y), dst, 0).start()
            return 0

        lax.fori_loop(1, side, one, 0)

    def steps(far_first):
        offsets = [(dy, dx) for dy in range(side) for dx in range(side) if dy or dx]
        cross = lambda o: sum(min(d, side - d) for d in o)
        return sorted(offsets, key=cross, reverse=far_first)

    def ep_at(dy, dx):
        return side * lax.rem(me_y + dy, side) + lax.rem(me_x + dx, side)

    def to_ep_peers(phase, src_of, dst):
        for dy, dx in steps(True):
            peer = ep_at(dy, dx)
            ep_copy(phase, src_of(peer), dst, peer, 0).start()

    def await_blocks(phase, blocks):
        over(me_e, partner, phase, blocks, blocks, 0).wait_recv()

    def others(me, many, buffer, acc):
        def one(d, acc):
            return acc + buffer[lax.rem(me + d, many)].astype(F32)

        return loop(1, many, one, acc)

    rest, few = pl.ds(0, n - 1), pl.ds(0, side - 1)
    far_first = (2, 1, 3, 0) if side == 4 else tuple(range(side))

    def sent(copy, phase, many):
        copy(phase, many, many, 0, 0).wait_send()

    loads[0].wait()
    to_ep_peers(TOK,
             lambda peer: tok.at[:, pl.ds(pl.multiple_of(peer * block, block), block)],
             tok_all.at[me_e])
    tok_all[me_e] = tok[:, pl.ds(pl.multiple_of(me_e * block, block), block)]

    loads[16].wait()
    give_over_tp(PROJ, projection(me_t), projection)
    loads[17].wait()
    loads[18].wait()
    give_weights(0)

    loads[4].wait()
    loads[5].wait()
    route_rows = [routes[pl.ds(k, 1), :] for k in range(2)]
    lanes_e = iota((128, rows), 0)
    named = sum(jnp.where(lanes_e == r, 1.0, 0.0) for r in route_rows)
    earlier = jnp.where(iota((rows, rows), 0) < iota((rows, rows), 1), 1.0, 0.0)
    before = jnp.dot(named.astype(BF16), earlier.astype(BF16), preferred_element_type=F32)
    base = (CAP * me_y).astype(F32)
    key = jnp.where(named > 0.0, before + base, -1.0)
    eye = jnp.where(iota((rows, rows), 0) == iota((rows, rows), 1), 1.0, 0.0)
    key_all[me_y] = lax.dot_general(
        eye.astype(BF16), key.astype(BF16), NT, preferred_element_type=F32).astype(BF16)
    to_y_peers(KEY, lambda y: key_all.at[me_y], key_all.at[me_y])
    weights = [rw[pl.ds(k, 1), :] for k in range(2)]
    total = weights[0] + weights[1]
    spots = iota((n * SLOT, rows), 0)
    share_t = jnp.zeros((n * SLOT, rows), F32)
    for r, w in zip(route_rows, weights):
        slot = jnp.sum(jnp.where(lanes_e == r, before, 0.0), axis=0, keepdims=True)
        hit = (spots.astype(F32) == r.astype(F32) * SLOT + slot)
        share_t = share_t + jnp.where(hit, w / total, 0.0)
    ret_w[...] = lax.dot_general(eye, share_t, NT, precision=HIGHEST, preferred_element_type=F32)

    loads[1].wait()
    squares = jnp.zeros((rows, block), F32)
    for k in range(n):
        part = tok[:, k * block:(k + 1) * block].astype(F32)
        squares = squares + part * part
    scale = lax.rsqrt(jnp.sum(squares, axis=1, keepdims=True) / width + EPS)
    loads[6].wait()
    loads[7].wait()
    gate = jnp.zeros((rows, 2 * n), F32)
    for k in range(n):
        cols = slice(k * block, (k + 1) * block)
        gain = mgain[:, cols]
        normed = (tok[:, cols].astype(F32) * scale * gain).astype(BF16)
        gate = gate + lax.dot_general(normed, wgates[:, cols], NT, preferred_element_type=F32)
    for k in range(8, 11):
        loads[k].wait()
    lane = iota((rows, 2 * n), 1)
    gate_in = jnp.sum(jnp.where(lane == me_t, gate, 0.0), axis=1, keepdims=True)
    gate_forget = jnp.sum(jnp.where(lane == me_t + n, gate, 0.0), axis=1, keepdims=True)
    bias = jnp.sum(jnp.where(iota((1, n), 1) == me_t, fbias[...], 0.0), axis=1, keepdims=True)
    gate_forget = gate_forget + bias
    log_keep = jnp.minimum(gate_forget, 0.0) - jnp.log1p(jnp.exp(-jnp.abs(gate_forget)))
    old_max = to_column(smax[...], rows)
    new_max = jnp.maximum(log_keep + old_max, gate_in)
    keep = jnp.exp(log_keep + old_max - new_max)
    write = jnp.exp(gate_in - new_max)
    nmax[...] = to_row(new_max, rows)

    await_blocks(TOK, tok_all.at[rest])
    for k in range(11, 15):
        loads[k].wait()
    gain_m = mgain[:, pl.ds(pl.multiple_of(me_e * block, block), block)]

    def project(dy):
        at = pl.multiple_of(side * lax.rem(me_y + dy, side), side)
        x = tok_all[pl.ds(at, side)].reshape(quarter, block).astype(F32) * gain_m
        y = jnp.dot(x.astype(BF16), wqkv[...], preferred_element_type=F32)
        qkv_part[pl.ds(at, side)] = y.astype(BF16).reshape(side, rows, 4 * head)
        for dx in far_first:
            if dy or dx:
                peer = ep_at(dy, dx)
                ep_copy(QKV, qkv_part.at[peer], qkv_in.at[me_e], peer, 0).start()

    for dy in far_first:
        project(dy)
    give_weights(1)

    loads[15].wait()
    await_blocks(QKV, qkv_in.at[rest])
    y = others(me_e, n, qkv_in, qkv_part[me_e].astype(F32)) * scale
    query = y[:, :head]
    keys = y[:, head:2 * head] * head ** (-0.5)
    value = y[:, 2 * head:3 * head]
    outgate = y[:, 3 * head:]
    written = write * keys
    new_norm = keep * sn[...] + written
    nn[...] = new_norm
    denom = jnp.sum(query * new_norm, axis=1, keepdims=True)
    qt[...] = query.T
    wkt[...] = written.T
    vrow[...] = value
    keep_rows[...] = jnp.broadcast_to(keep, (rows, head))
    for b in range(rows):
        numer[pl.ds(b, 1), :] = jnp.sum(qt[:, b:b + 1] * sm[b], axis=0, keepdims=True)
    dots = jnp.sum(query * written, axis=1, keepdims=True)
    num = keep * numer[...] + dots * value
    cell = num / jnp.maximum(jnp.abs(denom), 1.0)
    mix_own[...] = (jax.nn.sigmoid(outgate) * cell).astype(BF16)

    def head_place(h):
        return mix_in.at[:, pl.ds(pl.multiple_of(h * head, head), head)]

    for dy, dx in steps(True):
        j = ep_at(dy, dx)
        over(j, lax.rem(me_e + j, n), MIX, mix_own, head_place(me_t), 0).start()

    @pl.when(owned != me_e)
    def _():
        over(me_e, lax.rem(2 * me_e, n), MIX, mix_own, head_place(me_t), 0).start()

    @pl.when(owned == me_e)
    def _():
        mix_in[:, pl.ds(pl.multiple_of(me_t * head, head), head)] = mix_own[...]

    give_weights(2)
    loads[22].wait()
    near(NEAR_DOWN, dd_all, me_y, along_y, 0, hid_d, 0)
    pass_over_tp(PROJ, projection)
    pass_weights(0)
    pass_weights(1)
    for b in range(rows):
        nm[b] = keep_rows[pl.ds(b, 1), :] * sm[b] + wkt[:, b:b + 1] * vrow[pl.ds(b, 1), :]

    await_blocks(KEY, key_all.at[few])
    key_t = lax.dot_general(
        jnp.where(iota((n, 128), 0) == iota((n, 128), 1), 1.0, 0.0).astype(BF16),
        key_all[...].reshape(quarter, 128), NT, preferred_element_type=F32)
    places = iota((few_rows, quarter), 0).astype(F32)
    for e in range(0, n, 2):
        both = [jnp.where(places == key_t[k:k + 1, :], 1.0, 0.0) for k in (e, e + 1)]
        pick[pl.ds(e * few_rows, 2 * few_rows), :] = jnp.concatenate(both, axis=0).astype(BF16)

    take_over_tp(PROJ, proj_all.at[pl.ds(0, chips)])

    @pl.when(owned != me_e)
    def _():
        await_blocks(MIX, mix_in)

    @pl.when(owned == me_e)
    def _():
        await_blocks(MIX, mix_in.at[:, pl.ds(0, (n - 1) * head)])

    mixed = jnp.dot(mix_in[...], proj_all[...].reshape(n * head, block), preferred_element_type=F32)
    residual = (tok_all[owned].astype(F32) + mixed).astype(BF16)
    res_own[...] = residual

    def to_final():
        return pltpu.make_async_remote_copy(
            src_ref=res_own, dst_ref=res_fin, send_sem=res_sem.at[0], recv_sem=res_sem.at[1],
            device_id=(owned, me_e), device_id_type=MESH)

    corner = (owned == me_e) & (me_e == me_t)

    gather_quarter()

    @pl.when(jnp.logical_not(corner))
    def _():
        to_final().start()

    @pl.when(corner)
    def _():
        res_fin[...] = res_own[...]

    loads[2].wait()
    loads[3].wait()

    def pass_rows(peer):
        part = row_in.at[core * n + peer]
        tp_copy(ROW, part, part, partner, n + lax.div(peer, side)).start()

    half_side = side // 2
    res_half = jnp.concatenate(
        [res_all[pl.ds((core * half_side + k) * side, side)].reshape(quarter, block)
         for k in range(half_side)], axis=1)

    def dispatch(dy):
        at = pl.multiple_of(side * lax.rem(me_y + dy, side), side)
        y = jnp.dot(pick[pl.ds(pl.multiple_of(at * few_rows, side * few_rows), side * few_rows), :],
                    res_half, preferred_element_type=F32)
        y = y.reshape(side, few_rows, half_side * block)
        row_out[pl.ds(at, side)] = jnp.concatenate(
            [y[:, :, k * block:(k + 1) * block] for k in range(half_side)], axis=1).astype(BF16)
        for dx in far_first:
            if dy or dx:
                peer, spot = ep_at(dy, dx), core * n + me_e
                ep_copy(ROW, row_out.at[peer], row_in.at[spot], peer, me_e).start()

    for dy in far_first:
        dispatch(dy)
    row_in[core * n + me_e] = row_out[me_e]
    pass_rows(me_e)

    wbr_wide[...] = wbr[...].astype(F32)
    lines = block // 128
    squares = [jnp.zeros((rows, 1), F32)] * side
    branches = [jnp.zeros((rows, 1), F32)] * side
    for k in range(side):
        j = side * me_y + k
        gain_f = fgain[:, pl.ds(pl.multiple_of(j * block, block), block)]
        gain_b = gain_f * jnp.concatenate(
            [wbr_wide[pl.ds(j * lines + i, 1), :] for i in range(lines)], axis=1)
        for g in range(side):
            r = res_all[k * side + g].astype(F32)
            squares[g] = squares[g] + jnp.sum(r * r, axis=1, keepdims=True)
            branches[g] = branches[g] + jnp.sum(r * gain_b, axis=1, keepdims=True)
            x_cat[pl.ds(g * rows, rows), k * block:(k + 1) * block] = (r * gain_f).astype(BF16)
    for g in range(side):
        sta_out[g] = jnp.where(iota((8, 128), 0) == 0, to_row(squares[g], 128), to_row(branches[g], 128))
    to_y_peers(STA, lambda y: sta_out.at[y], sta_in.at[me_y])

    for part, (first, many) in enumerate(PARTS):
        far(FAR, dgu_all, me_x, along_x, first, many, part, "wait")
    weights = dgu_all[...].reshape(side * block, 2 * hid_d)
    x = x_cat[...]
    for k in range(2 * hid_d // block):
        y = jnp.dot(x, weights[:, k * block:(k + 1) * block], preferred_element_type=F32)
        den_part[:, :, k * block:(k + 1) * block] = y.astype(BF16).reshape(side, rows, block)
    to_y_peers(DEN, lambda y: den_part.at[y], den_in.at[me_y])

    loads[19].wait()
    loads[20].wait()

    deep = half_side * block

    def expert_in(y, half, ss):
        x = row_in[pl.ds(half * n + y * side, side)].astype(F32)
        x = jnp.concatenate(
            [x[:, k * few_rows:(k + 1) * few_rows].reshape(cap_rows, block) for k in range(half_side)], axis=1)
        at = pl.multiple_of(y * side * block + half * deep, deep)
        xg = (x * fgain[:, pl.ds(at, deep)]).astype(BF16)
        gu_acc[:, pl.ds(0, hid_e)] += jnp.dot(xg, eg[pl.ds(at, deep), :], preferred_element_type=F32)
        gu_acc[:, pl.ds(hid_e, hid_e)] += jnp.dot(xg, eu[pl.ds(at, deep), :], preferred_element_type=F32)
        return ss + jnp.sum(x * x, axis=1, keepdims=True)

    def expert_first(d, ss):
        y = lax.rem(me_y + side - d, side)

        def one(k, _):
            peer = side * y + lax.rem(me_x + k, side)
            spot = core * n + peer

            @pl.when(peer != me_e)
            def _():
                ep_copy(ROW, row_in.at[spot], row_in.at[spot], peer, peer).wait_recv()
                pass_rows(peer)

            return 0

        lax.fori_loop(0, side, one, 0)
        return expert_in(y, core, ss)

    def expert_second(d, ss):
        y = lax.rem(me_y + side - d, side)

        part = row_in.at[pl.ds((1 - core) * n + side * y, side)]
        tp_copy(ROW, part, part, partner, n + y).wait_recv()
        return expert_in(y, 1 - core, ss)

    gu_acc[...] = jnp.zeros_like(gu_acc)
    ss = expert_first(0, jnp.zeros((cap_rows, 1), F32))
    ss = loop(1, side, lambda d, ss: expert_second(d - 1, expert_first(d, ss)), ss)
    ss = expert_second(side - 1, ss)
    row_scale = lax.rsqrt(ss / width + EPS)
    g = gu_acc[:, :hid_e] * row_scale
    u = gu_acc[:, hid_e:] * row_scale
    hidden_e[...] = (g / (1.0 + jnp.exp(-g)) * u).astype(BF16)
    loads[21].wait()

    def expert_out(at):
        return jnp.dot(hidden_e[...], ed[:, pl.ds(pl.multiple_of(at * block, block), block)],
                       preferred_element_type=F32).astype(BF16)

    routed_sum = sum_over_tp(
        EXP_PAIR, EXP, exp_part, exp_pair, exp_sum, exp_in, expert_out)

    await_blocks(STA, sta_in.at[few])
    sums = others(me_y, side, sta_in, sta_out[me_y])
    dense_scale = lax.rsqrt(to_column(sums[0:1, :], rows) / width + EPS)
    branch = jax.nn.sigmoid(to_column(sums[1:2, :], rows) * dense_scale)
    await_blocks(DEN, den_in.at[few])
    y = others(me_y, side, den_in, den_part[me_y].astype(F32)) * dense_scale
    g, u = y[:, :hid_d], y[:, hid_d:]
    hid_all[me_x] = (g / (1.0 + jnp.exp(-g)) * u * branch).astype(BF16)

    def spread_hidden(d, _):
        over(along_x(d), me_t, HID, hid_all.at[me_x], hid_all.at[me_x], me_x).start()
        return 0

    lax.fori_loop(1, side, spread_hidden, 0)

    far(FAR_DOWN, dd_all, me_y, along_y, 0, hid_d, 0, "wait")

    def hidden_of(d, _):
        x = lax.rem(me_x + side - d, side)
        over(along_x(-d), me_t, HID, hid_all.at[x], hid_all.at[x], x).wait_recv()
        return 0

    lax.fori_loop(1, side, hidden_of, 0)
    x = hid_all[...].reshape(quarter, hid_d)
    for k in range(side):
        y = jnp.dot(x, dd_all[k], preferred_element_type=F32)
        dwn_part[pl.ds(k * side, side)] = y.astype(BF16).reshape(side, rows, block)
    end_core = lax.rem(me_x, 2)
    home = lax.rem(me_t, side) == me_x

    @pl.when(core != end_core)
    def _():
        tp_copy(DWN_PAIR, dwn_part, dwn_pair, partner, 0).start()

    @pl.when(core == end_core)
    def _():
        tp_copy(DWN_PAIR, dwn_pair, dwn_pair, partner, 0).wait_recv()
        for dx in far_first:
            def to_end(c, _):
                x = lax.rem(me_x + dx, side)
                k = side * c + x
                dwn_sum[k] = (dwn_part[k].astype(F32) + dwn_pair[k].astype(F32)).astype(BF16)
                z = 2 * c + lax.div(me_x, 2)
                here = (x == me_x) & (z == me_z)

                @pl.when(jnp.logical_not(here))
                def _():
                    over(side * me_y + x, 2 * z + core, DWN, dwn_sum.at[k], dwn_in.at[me_z], 0).start()

                @pl.when(here)
                def _():
                    dwn_in[me_z] = dwn_sum[k]

                return 0

            lax.fori_loop(0, side, to_end, 0)

    y = summed_over_tp(EXP, exp_in, routed_sum)
    spot, col = iota((n * SLOT, cap_rows), 0), iota((n * SLOT, cap_rows), 1)
    within = jnp.bitwise_and(spot, SLOT - 1)
    shift = side.bit_length() - 1
    from_e = jnp.right_shift(spot, SLOT.bit_length() - 1)
    source = few_rows * jnp.bitwise_and(from_e, side - 1) + CAP * jnp.right_shift(from_e, shift) + within
    spread = jnp.where((source == col) & (within < CAP), 1.0, 0.0).astype(BF16)
    ret_out[...] = jnp.dot(
        spread, y.astype(BF16), preferred_element_type=F32).reshape(n, SLOT, block).astype(BF16)

    to_ep_peers(RET, lambda peer: ret_out.at[peer], ret_in.at[me_e])
    ret_in[me_e] = ret_out[me_e]

    await_blocks(RET, ret_in.at[rest])

    @pl.when(jnp.logical_not(corner))
    def _():
        to_final().wait()

    routed = jnp.dot(ret_w[...], ret_in[...].astype(F32).reshape(n * SLOT, block), precision=HIGHEST,
                     preferred_element_type=F32)
    known = res_fin[...].astype(F32) + routed

    @pl.when(home)
    def _():
        await_blocks(DWN, dwn_in.at[pl.ds(0, chips - 1)])

    @pl.when(jnp.logical_not(home))
    def _():
        await_blocks(DWN, dwn_in)

    y = others(me_z, chips, dwn_in, dwn_in[me_z].astype(F32))
    out_own[...] = (known + y).astype(BF16)

    def columns(j):
        return out.at[:, pl.ds(pl.multiple_of(j * block, block), block)]

    give_over_tp(OUT, out_own, columns)
    out[:, pl.ds(pl.multiple_of(me_t * block, block), block)] = out_own[...]
    pass_over_tp(OUT, columns)
    take_over_tp(OUT, out.at[:, pl.ds(0, chips * block)])
    sent(ep_copy, TOK, tok_all.at[rest])
    sent(ep_copy, KEY, key_all.at[few])
    sent(ep_copy, QKV, qkv_part.at[rest])
    some = pl.ds(0, chips - 1)

    @pl.when(owned != me_e)
    def _():
        sent(ep_copy, MIX, mix_in)

    @pl.when(owned == me_e)
    def _():
        sent(ep_copy, MIX, mix_in.at[:, pl.ds(0, (n - 1) * head)])

    sent(tp_copy, PROJ, proj_all.at[rest])
    sent(ep_copy, ROW, row_in.at[pl.ds(0, 2 * n - 1)])
    sent(ep_copy, STA, sta_out.at[few])
    sent(ep_copy, DEN, den_part.at[few])
    sent(ep_copy, HID, hid_all.at[few])
    for phase, buffer, rows_of in (
        (NEAR, dgu_all, block), (FAR, dgu_all, block // 2),
        (NEAR_DOWN, dd_all, hid_d), (FAR_DOWN, dd_all, hid_d // 2)):
        sent(ep_copy, phase, buffer.at[pl.ds(0, 2), pl.ds(0, rows_of), :])
    sent(tp_copy, EXP_PAIR, exp_pair)
    sent(tp_copy, EXP, exp_sum.at[some])
    sent(ep_copy, RET, ret_out.at[rest])
    sent(tp_copy, OUT, tok_all.at[rest])

    @pl.when(core != end_core)
    def _():
        sent(tp_copy, DWN_PAIR, dwn_part)

    @pl.when(home)
    def _():
        sent(ep_copy, DWN, dwn_sum.at[rest])

    @pl.when((core == end_core) & jnp.logical_not(home))
    def _():
        sent(ep_copy, DWN, dwn_sum)

    own_column = lax.rem(owned, side) == me_x

    @pl.when(jnp.logical_not(own_column))
    def _():
        sent(ep_copy, RES, res_all)

    @pl.when(own_column)
    def _():
        sent(ep_copy, RES, res_all.at[rest])


def put_out(*refs):
    *arrays, sem = refs
    copies = [pltpu.make_async_copy(arrays[k], arrays[4 + k], sem.at[k]) for k in range(4)]
    for copy in copies:
        copy.start()
    for copy in copies:
        copy.wait()


def on_device(
    n, tokens, state_matrix, state_norm, state_max, mixer_gain, w_query, w_key, w_value, w_outgate,
    w_ingate, w_forget, forget_bias, w_proj, ffn_gain, w_branch, routes, route_weight,
    expert_gate, expert_up, expert_down, dense_gate, dense_up, dense_down,
):
    rows, width = tokens.shape
    head = state_norm.shape[-1]
    block = width // n
    hid_e, hid_d = expert_gate.shape[2], dense_gate.shape[1]
    cap_rows = CAP * n
    args = (
        tokens,
        state_matrix.reshape(rows, head, head),
        state_norm.reshape(rows, head),
        state_max.T,
        mixer_gain.reshape(1, width),
        w_query, w_key, w_value, w_outgate,
        w_ingate.T, w_forget.T,
        forget_bias.reshape(1, n),
        w_proj,
        ffn_gain.reshape(1, width),
        w_branch.reshape(width // 128, 128),
        routes.T, route_weight.T,
        expert_gate.reshape(width, hid_e), expert_up.reshape(width, hid_e),
        expert_down.reshape(hid_e, width),
        dense_gate, dense_up, dense_down,
    )
    vm = pltpu.VMEM
    dma = pltpu.SemaphoreType.DMA
    few_rows, side = CAP * math.isqrt(n), math.isqrt(n)

    def hier(tall):
        return [vm((n, tall, block), BF16)] + [vm((n // 2, tall, block), BF16)] * 3

    scratch = [
        vm((rows, width), BF16), vm((rows, head, head), F32), vm((rows, head), F32), vm((1, rows), F32),
        vm((1, width), F32), vm((block, 4 * head), BF16), vm((2 * n, width), BF16), vm((1, n), F32),
        vm((n, head, block), BF16), vm((1, width), F32), vm((width // 128, 128), BF16), vm((2, rows), jnp.int32),
        vm((2, rows), F32), vm((width, hid_e), BF16), vm((width, hid_e), BF16), vm((hid_e, width), BF16),
        vm((side, block, 2 * hid_d), BF16), vm((side, hid_d, block), BF16),
        vm((n, rows, block), BF16), vm((side, rows, 128), BF16),
        vm((n, rows, 4 * head), BF16), vm((n, rows, 4 * head), BF16),
        vm((rows, head), BF16), vm((rows, n * head), BF16),
        vm((rows, block), BF16), vm((n, rows, block), BF16), vm((rows, block), BF16),
        vm((n, few_rows * side // 2, block), BF16), vm((2 * n, few_rows * side // 2, block), BF16),
        vm((side, 8, 128), F32), vm((side, 8, 128), F32),
        vm((side, rows, 2 * hid_d), BF16), vm((side, rows, 2 * hid_d), BF16),
        vm((side, rows, hid_d), BF16), *[vm((n, rows, block), BF16)] * 3, vm((n // 2, rows, block), BF16),
        *hier(cap_rows),
        vm((n, SLOT, block), BF16), vm((n, SLOT, block), BF16),
        vm((rows, block), BF16),
        vm((width // 128, 128), F32),
        vm((n * few_rows, side * rows), BF16), vm((side * rows, side * block), BF16), vm((cap_rows, hid_e), BF16), vm((cap_rows, 2 * hid_e), F32), vm((rows, 2 * n), F32),
        vm((head, rows), F32), vm((head, rows), F32), vm((rows, head), F32), vm((rows, head), F32),
        vm((rows, head), F32), vm((rows, n * SLOT), F32),
        dma((len(args),)), dma((PHASES,)), dma((landing_spots(n)[1],)), dma((2,)),
    ]
    any_space = pl.BlockSpec(memory_space=pl.ANY)
    layer_out, new_matrix, new_norm, new_max = pl.pallas_call(
        functools.partial(layer_kernel, n),
        out_shape=(
            vm((rows, width), BF16), vm((rows, head, head), F32), vm((rows, head), F32), vm((1, rows), F32),
        ),
        in_specs=[any_space] * len(args),
        out_specs=[pl.BlockSpec(memory_space=vm)] * 4,
        scratch_shapes=scratch,
        compiler_params=pltpu.CompilerParams(
            collective_id=0, has_side_effects=True, vmem_limit_bytes=56 * 1024 * 1024),
        name="layer",
    )(*args)
    results = (layer_out, new_matrix, new_norm, new_max)
    results = tuple(pltpu.with_memory_space_constraint(r, vm) for r in results)
    layer_out, new_matrix, new_norm, new_max = pl.pallas_call(
        put_out,
        out_shape=tuple(jax.ShapeDtypeStruct(r.shape, r.dtype) for r in results),
        in_specs=[pl.BlockSpec(memory_space=vm)] * 4,
        out_specs=[any_space] * 4,
        scratch_shapes=[dma((4,))],
        name="put_out",
    )(*results)
    return (layer_out, new_matrix.reshape(rows, 1, head, head), new_norm.reshape(rows, 1, head), new_max.T)


def solution(mesh):
    n = mesh.shape["ep"]
    in_specs = (
        P("ep", None),
        P("ep", "tp", None, None),
        P("ep", "tp", None),
        P("ep", "tp"),
        P(),
        P("ep", "tp"),
        P("ep", "tp"),
        P("ep", "tp"),
        P("ep", "tp"),
        P(),
        P(),
        P(),
        P("tp", "ep"),
        P(),
        P(),
        P("ep", None),
        P("ep", None),
        P("ep", None, "tp"),
        P("ep", None, "tp"),
        P("ep", "tp", None),
        P("ep", "tp"),
        P("ep", "tp"),
        P("tp", "ep"),
    )
    out_specs = (P("ep", None), P("ep", "tp", None, None), P("ep", "tp", None), P("ep", "tp"))
    return jax.shard_map(
        functools.partial(on_device, n), mesh=mesh, in_specs=in_specs, out_specs=out_specs,
        check_vma=False)
```

```python
import functools
import math

import jax
import jax.numpy as jnp
from jax import lax
from jax.experimental import pallas as pl
from jax.experimental.pallas import tpu as pltpu
from jax.sharding import PartitionSpec as P

EPS = 1e-06
MESH = pl.DeviceIdType.MESH
CAP = 6
SLOT = 8
F32 = jnp.float32
BF16 = jnp.bfloat16
HIGHEST = lax.Precision.HIGHEST
NT = (((1,), (1,)), ((), ()))


def landing_spots(n):
    side = math.isqrt(n)
    many = {ROW: n + side, RES: n + 1, NEAR: 6, FAR: 6, NEAR_DOWN: 2, FAR_DOWN: 2, HID: side}
    for phase in (TOK, KEY, QKV, STA, DEN, RET, MIX, DWN, DWN_PAIR, EXP):
        many[phase] = 1
    many[EXP_PAIR] = n // 2
    many[PROJ] = many[OUT] = n // 2 + 1
    first, at = [], 0
    for phase in range(PHASES):
        first.append(at)
        at += many.get(phase, n)
    return first, at


def iota(shape, dim):
    return lax.broadcasted_iota(jnp.int32, shape, dim)


def loop(first, end, body, carry):
    for k in range(first, end):
        carry = body(k, carry)
    return carry


def to_column(row, rows):
    diag = iota((rows, row.shape[1]), 0) == iota((rows, row.shape[1]), 1)
    return jnp.sum(jnp.where(diag, row, 0.0), axis=1, keepdims=True)


def to_row(column, lanes):
    rows = column.shape[0]
    diag = iota((rows, lanes), 0) == iota((rows, lanes), 1)
    return jnp.sum(jnp.where(diag, column, 0.0), axis=0, keepdims=True)


(TOK, KEY, QKV, MIX, PROJ, RES, ROW, STA, DEN, HID, DWN_PAIR, DWN, EXP_PAIR, EXP, RET,
 OUT, NEAR, FAR, NEAR_DOWN, FAR_DOWN) = range(20)
PHASES = 20
AHEAD = 2
PARTS = ((0, 64), (64, 64), (128, 128))


def layer_kernel(
    n,
    tok_h, sm_h, sn_h, smax_h, mgain_h, wq_h, wk_h, wv_h, wo_h, win_h, wfo_h, fbias_h,
    wproj_h, fgain_h, wbr_h, routes_h, rw_h, eg_h, eu_h, ed_h, dg_h, du_h, dd_h,
    out, nm, nn, nmax,
    tok, sm, sn, smax, mgain, wqkv, wgates, fbias, proj_all, fgain, wbr, routes, rw,
    eg, eu, ed, dgu_all, dd_all,
    tok_all, key_all, qkv_part, qkv_in, mix_own, mix_in, res_own, res_all, res_fin,
    row_out, row_in, sta_out, sta_in, den_part, den_in, hid_all, dwn_part, dwn_pair, dwn_sum, dwn_in,
    exp_part, exp_pair, exp_sum, exp_in, ret_out, ret_in, out_own,
    wbr_wide, pick, x_cat, hidden_e, gu_acc, gates, wkt, qt, vrow, keep_rows, numer, ret_w,
    load_sem, send_sem, recv_sem, res_sem,
):
    me_e, me_t = lax.axis_index("ep"), lax.axis_index("tp")
    chips = n // 2
    first_spot, _ = landing_spots(n)
    side = math.isqrt(n)
    me_y, me_x = lax.div(me_e, side), lax.rem(me_e, side)
    me_z, core = lax.div(me_t, 2), lax.rem(me_t, 2)
    partner = me_t + 1 - 2 * core
    owned = lax.rem(me_t - me_e + n, n)
    rows = tok.shape[0]
    width = tok.shape[1]
    block = width // n
    head = sn.shape[1]
    hid_e = eg.shape[1]
    hid_d = dd_all.shape[1]
    quarter = rows * side
    cap_rows = CAP * n
    few_rows = CAP * side
    dgu, dd = dgu_all.at[me_x], dd_all.at[me_y]

    loads = [
        (tok_h, tok), (mgain_h, mgain), (fgain_h, fgain), (wbr_h, wbr), (routes_h, routes),
        (rw_h, rw), (win_h, wgates.at[pl.ds(0, n), :]), (wfo_h, wgates.at[pl.ds(n, n), :]),
        (fbias_h, fbias), (smax_h, smax), (sn_h, sn),
        (wq_h, wqkv.at[:, pl.ds(0, head)]), (wk_h, wqkv.at[:, pl.ds(head, head)]),
        (wv_h, wqkv.at[:, pl.ds(2 * head, head)]), (wo_h, wqkv.at[:, pl.ds(3 * head, head)]),
        (sm_h, sm), (wproj_h, proj_all.at[me_t]), (dg_h, dgu_all.at[me_x, :, pl.ds(0, hid_d)]),
        (du_h, dgu_all.at[me_x, :, pl.ds(hid_d, hid_d)]), (eg_h, eg), (eu_h, eu), (ed_h, ed), (dd_h, dd),
    ]
    loads = [pltpu.make_async_copy(a, b, load_sem.at[k]) for k, (a, b) in enumerate(loads)]
    for copy in loads:
        copy.start()

    barrier = pltpu.get_barrier_semaphore()

    def greet(d, _):
        pl.semaphore_signal(barrier, 1, device_id=(lax.rem(me_e + d, n), me_t), device_id_type=MESH)
        pl.semaphore_signal(barrier, 1, device_id=(me_e, lax.rem(me_t + d, n)), device_id_type=MESH)
        return 0

    lax.fori_loop(1, n, greet, 0)
    pl.semaphore_wait(barrier, 2 * n - 2)

    def ep_copy(phase, src, dst, peer, landing):
        return pltpu.make_async_remote_copy(
            src_ref=src, dst_ref=dst, send_sem=send_sem.at[phase],
            recv_sem=recv_sem.at[first_spot[phase] + landing], device_id=(peer, me_t), device_id_type=MESH)

    def tp_copy(phase, src, dst, peer, landing):
        return pltpu.make_async_remote_copy(
            src_ref=src, dst_ref=dst, send_sem=send_sem.at[phase],
            recv_sem=recv_sem.at[first_spot[phase] + landing], device_id=(me_e, peer), device_id_type=MESH)

    def over(peer_e, peer_t, phase, src, dst, landing):
        return pltpu.make_async_remote_copy(
            src_ref=src, dst_ref=dst, send_sem=send_sem.at[phase],
            recv_sem=recv_sem.at[first_spot[phase] + landing], device_id=(peer_e, peer_t), device_id_type=MESH)

    def chip(k):
        k = chips - k
        return lax.rem(me_z + chips + lax.div(k + 1, 2) * (2 * lax.rem(k, 2) - 1), chips)

    def sum_over_tp(pair_phase, phase, part, pair, summed, arrived, make):
        def give(k):
            z = chip(k)
            at = 2 * z + 1 - core
            part[at] = make(at)
            tp_copy(pair_phase, part.at[at], pair.at[z], partner, z).start()

        def add(z):
            mine = make(2 * z + core)
            tp_copy(pair_phase, pair.at[z], pair.at[z], partner, z).wait_recv()
            return mine.astype(F32) + pair[z].astype(F32)

        def pass_on(k):
            z = chip(k)
            summed[z] = add(z).astype(BF16)
            tp_copy(phase, summed.at[z], arrived.at[me_z], 2 * z + core, 0).start()

        def both(k, _):
            give(k)
            pass_on(k - AHEAD)
            return 0

        def first(k, _):
            give(k)
            return 0

        def last(k, _):
            pass_on(k)
            return 0

        loop(1, AHEAD + 1, first, 0)
        loop(AHEAD + 1, chips + 1, both, 0)
        loop(chips + 1 - AHEAD, chips, last, 0)
        return add(me_z)

    def summed_over_tp(phase, arrived, acc):
        await_blocks(phase, arrived.at[pl.ds(0, chips - 1)])
        return others(me_z, chips, arrived, acc)

    def give_over_tp(phase, mine, spot):
        tp_copy(phase, mine, spot(me_t), partner, chips).start()

        def give(k, _):
            tp_copy(phase, mine, spot(me_t), 2 * chip(k) + core, me_z).start()
            return 0

        lax.fori_loop(1, chips, give, 0)

    def pass_over_tp(phase, spot):
        def pass_on(k, _):
            z = chip(chips - k)
            part = spot(2 * z + core)
            tp_copy(phase, part, part, 2 * z + core, z).wait_recv()
            tp_copy(phase, part, part, partner, chips).start()
            return 0

        lax.fori_loop(1, chips, pass_on, 0)

    def take_over_tp(phase, half):
        tp_copy(phase, half, half, partner, chips).wait_recv()

    def projection(t):
        return proj_all.at[t]

    def along_x(step):
        return side * me_y + lax.rem(me_x + step + side, side)

    def along_y(step):
        return side * lax.rem(me_y + step + side, side) + me_x

    def weight_copy(phase, buffer, block_of, peer, first, many, landing):
        part = buffer.at[block_of, pl.ds(first, many), :]
        return over(peer, me_t, phase, part, part, landing)

    def near(phase, buffer, me, along, first, many, part):
        for way, step in enumerate((1, -1)):
            weight_copy(phase, buffer, me, along(step), first, many, 2 * part + way).start()

    def arrived_near(phase, buffer, me, along, first, many, part):
        for way, step in enumerate((-1, 1)):
            owner = lax.rem(me + step + side, side)
            weight_copy(phase, buffer, owner, along(step), first, many, 2 * part + way).wait_recv()

    def far(phase, buffer, me, along, first, many, part, act):
        half = many // 2
        for way, step in enumerate((1, -1)):
            if act == "start":
                owner = lax.rem(me - step + side, side)
                weight_copy(phase, buffer, owner, along(step), first + way * half, half, 2 * part + way).start()
            else:
                owner = lax.rem(me + 2, side)
                weight_copy(phase, buffer, owner, along(-step), first + way * half, half, 2 * part + way).wait_recv()

    def give_weights(part):
        near(NEAR, dgu_all, me_x, along_x, *PARTS[part], part)

    def pass_weights(part):
        arrived_near(NEAR, dgu_all, me_x, along_x, *PARTS[part], part)
        far(FAR, dgu_all, me_x, along_x, *PARTS[part], part, "start")

    def gather_quarter():
        to_e = side * me_y + lax.rem(owned, side)
        spot = me_x * side + lax.div(owned, side)

        def give(k, _):
            over(to_e, 2 * chip(k) + core, RES, res_own, res_all.at[spot], spot).start()
            return 0

        lax.fori_loop(1, chips, give, 0)

        @pl.when(to_e != me_e)
        def _():
            over(to_e, me_t, RES, res_own, res_all.at[spot], spot).start()

        @pl.when(to_e == me_e)
        def _():
            res_all[spot] = res_own[...]

        pass_weights(2)
        arrived_near(NEAR_DOWN, dd_all, me_y, along_y, 0, hid_d, 0)
        far(FAR_DOWN, dd_all, me_y, along_y, 0, hid_d, 0, "start")

        def source(spot):
            o = side * lax.rem(spot, side) + me_x
            j = side * me_y + lax.div(spot, side)
            return j, lax.rem(o + j, n)

        def spot_of(k, parity):
            return (2 * lax.rem(k, 2) + parity) * side + lax.div(k, 2)

        def pass_on(k, _):
            spot = spot_of(k, lax.rem(core + me_x, 2))
            j, t = source(spot)

            @pl.when((j != me_e) | (t != me_t))
            def _():
                over(j, t, RES, res_all.at[spot], res_all.at[spot], spot).wait_recv()

            over(me_e, partner, RES, res_all.at[spot], res_all.at[spot], n).start()
            return 0

        lax.fori_loop(0, n // 2, pass_on, 0)

        half = res_all.at[pl.ds(0, chips)]
        over(me_e, partner, RES, half, half, n).wait_recv()

    def to_y_peers(phase, src_of, dst):
        def one(d, _):
            y = lax.rem(me_y + d, side)
            over(side * y + me_x, me_t, phase, src_of(y), dst, 0).start()
            return 0

        lax.fori_loop(1, side, one, 0)

    def steps(far_first):
        offsets = [(dy, dx) for dy in range(side) for dx in range(side) if dy or dx]
        cross = lambda o: sum(min(d, side - d) for d in o)
        return sorted(offsets, key=cross, reverse=far_first)

    def ep_at(dy, dx):
        return side * lax.rem(me_y + dy, side) + lax.rem(me_x + dx, side)

    def to_ep_peers(phase, src_of, dst):
        for dy, dx in steps(True):
            peer = ep_at(dy, dx)
            ep_copy(phase, src_of(peer), dst, peer, 0).start()

    def await_blocks(phase, blocks):
        over(me_e, partner, phase, blocks, blocks, 0).wait_recv()

    def others(me, many, buffer, acc):
        def one(d, acc):
            return acc + buffer[lax.rem(me + d, many)].astype(F32)

        return loop(1, many, one, acc)

    rest, few = pl.ds(0, n - 1), pl.ds(0, side - 1)
    far_first = (2, 1, 3, 0) if side == 4 else tuple(range(side))

    def sent(copy, phase, many):
        copy(phase, many, many, 0, 0).wait_send()

    loads[0].wait()
    to_ep_peers(TOK,
             lambda peer: tok.at[:, pl.ds(pl.multiple_of(peer * block, block), block)],
             tok_all.at[me_e])
    tok_all[me_e] = tok[:, pl.ds(pl.multiple_of(me_e * block, block), block)]

    loads[16].wait()
    give_over_tp(PROJ, projection(me_t), projection)
    loads[17].wait()
    loads[18].wait()
    give_weights(0)

    loads[4].wait()
    loads[5].wait()
    route_rows = [routes[pl.ds(k, 1), :] for k in range(2)]
    lanes_e = iota((128, rows), 0)
    named = sum(jnp.where(lanes_e == r, 1.0, 0.0) for r in route_rows)
    earlier = jnp.where(iota((rows, rows), 0) < iota((rows, rows), 1), 1.0, 0.0)
    before = jnp.dot(named.astype(BF16), earlier.astype(BF16), preferred_element_type=F32)
    base = (CAP * me_y).astype(F32)
    key = jnp.where(named > 0.0, before + base, -1.0)
    eye = jnp.where(iota((rows, rows), 0) == iota((rows, rows), 1), 1.0, 0.0)
    key_all[me_y] = lax.dot_general(
        eye.astype(BF16), key.astype(BF16), NT, preferred_element_type=F32).astype(BF16)
    to_y_peers(KEY, lambda y: key_all.at[me_y], key_all.at[me_y])
    weights = [rw[pl.ds(k, 1), :] for k in range(2)]
    total = weights[0] + weights[1]
    spots = iota((n * SLOT, rows), 0)
    share_t = jnp.zeros((n * SLOT, rows), F32)
    for r, w in zip(route_rows, weights):
        slot = jnp.sum(jnp.where(lanes_e == r, before, 0.0), axis=0, keepdims=True)
        hit = (spots.astype(F32) == r.astype(F32) * SLOT + slot)
        share_t = share_t + jnp.where(hit, w / total, 0.0)
    ret_w[...] = lax.dot_general(eye, share_t, NT, precision=HIGHEST, preferred_element_type=F32)

    loads[1].wait()
    squares = jnp.zeros((rows, block), F32)
    for k in range(n):
        part = tok[:, k * block:(k + 1) * block].astype(F32)
        squares = squares + part * part
    scale = lax.rsqrt(jnp.sum(squares, axis=1, keepdims=True) / width + EPS)
    loads[6].wait()
    loads[7].wait()
    gate = jnp.zeros((rows, 2 * n), F32)
    for k in range(n):
        cols = slice(k * block, (k + 1) * block)
        gain = mgain[:, cols]
        normed = (tok[:, cols].astype(F32) * scale * gain).astype(BF16)
        gate = gate + lax.dot_general(normed, wgates[:, cols], NT, preferred_element_type=F32)
    for k in range(8, 11):
        loads[k].wait()
    lane = iota((rows, 2 * n), 1)
    gate_in = jnp.sum(jnp.where(lane == me_t, gate, 0.0), axis=1, keepdims=True)
    gate_forget = jnp.sum(jnp.where(lane == me_t + n, gate, 0.0), axis=1, keepdims=True)
    bias = jnp.sum(jnp.where(iota((1, n), 1) == me_t, fbias[...], 0.0), axis=1, keepdims=True)
    gate_forget = gate_forget + bias
    log_keep = jnp.minimum(gate_forget, 0.0) - jnp.log1p(jnp.exp(-jnp.abs(gate_forget)))
    old_max = to_column(smax[...], rows)
    new_max = jnp.maximum(log_keep + old_max, gate_in)
    keep = jnp.exp(log_keep + old_max - new_max)
    write = jnp.exp(gate_in - new_max)
    nmax[...] = to_row(new_max, rows)

    await_blocks(TOK, tok_all.at[rest])
    for k in range(11, 15):
        loads[k].wait()
    gain_m = mgain[:, pl.ds(pl.multiple_of(me_e * block, block), block)]

    def project(dy):
        at = pl.multiple_of(side * lax.rem(me_y + dy, side), side)
        x = tok_all[pl.ds(at, side)].reshape(quarter, block).astype(F32) * gain_m
        y = jnp.dot(x.astype(BF16), wqkv[...], preferred_element_type=F32)
        qkv_part[pl.ds(at, side)] = y.astype(BF16).reshape(side, rows, 4 * head)
        for dx in far_first:
            if dy or dx:
                peer = ep_at(dy, dx)
                ep_copy(QKV, qkv_part.at[peer], qkv_in.at[me_e], peer, 0).start()

    for dy in far_first:
        project(dy)
    give_weights(1)

    loads[15].wait()
    await_blocks(QKV, qkv_in.at[rest])
    y = others(me_e, n, qkv_in, qkv_part[me_e].astype(F32)) * scale
    query = y[:, :head]
    keys = y[:, head:2 * head] * head ** (-0.5)
    value = y[:, 2 * head:3 * head]
    outgate = y[:, 3 * head:]
    written = write * keys
    new_norm = keep * sn[...] + written
    nn[...] = new_norm
    denom = jnp.sum(query * new_norm, axis=1, keepdims=True)
    qt[...] = query.T
    wkt[...] = written.T
    vrow[...] = value
    keep_rows[...] = jnp.broadcast_to(keep, (rows, head))
    for b in range(rows):
        numer[pl.ds(b, 1), :] = jnp.sum(qt[:, b:b + 1] * sm[b], axis=0, keepdims=True)
    dots = jnp.sum(query * written, axis=1, keepdims=True)
    num = keep * numer[...] + dots * value
    cell = num / jnp.maximum(jnp.abs(denom), 1.0)
    mix_own[...] = (jax.nn.sigmoid(outgate) * cell).astype(BF16)

    def head_place(h):
        return mix_in.at[:, pl.ds(pl.multiple_of(h * head, head), head)]

    for dy, dx in steps(True):
        j = ep_at(dy, dx)
        over(j, lax.rem(me_e + j, n), MIX, mix_own, head_place(me_t), 0).start()

    @pl.when(owned != me_e)
    def _():
        over(me_e, lax.rem(2 * me_e, n), MIX, mix_own, head_place(me_t), 0).start()

    @pl.when(owned == me_e)
    def _():
        mix_in[:, pl.ds(pl.multiple_of(me_t * head, head), head)] = mix_own[...]

    give_weights(2)
    loads[22].wait()
    near(NEAR_DOWN, dd_all, me_y, along_y, 0, hid_d, 0)
    pass_over_tp(PROJ, projection)
    pass_weights(0)
    pass_weights(1)
    for b in range(rows):
        nm[b] = keep_rows[pl.ds(b, 1), :] * sm[b] + wkt[:, b:b + 1] * vrow[pl.ds(b, 1), :]

    await_blocks(KEY, key_all.at[few])
    key_t = lax.dot_general(
        jnp.where(iota((n, 128), 0) == iota((n, 128), 1), 1.0, 0.0).astype(BF16),
        key_all[...].reshape(quarter, 128), NT, preferred_element_type=F32)
    places = iota((few_rows, quarter), 0).astype(F32)
    for e in range(0, n, 2):
        both = [jnp.where(places == key_t[k:k + 1, :], 1.0, 0.0) for k in (e, e + 1)]
        pick[pl.ds(e * few_rows, 2 * few_rows), :] = jnp.concatenate(both, axis=0).astype(BF16)

    take_over_tp(PROJ, proj_all.at[pl.ds(0, chips)])

    @pl.when(owned != me_e)
    def _():
        await_blocks(MIX, mix_in)

    @pl.when(owned == me_e)
    def _():
        await_blocks(MIX, mix_in.at[:, pl.ds(0, (n - 1) * head)])

    mixed = jnp.dot(mix_in[...], proj_all[...].reshape(n * head, block), preferred_element_type=F32)
    residual = (tok_all[owned].astype(F32) + mixed).astype(BF16)
    res_own[...] = residual

    def to_final():
        return pltpu.make_async_remote_copy(
            src_ref=res_own, dst_ref=res_fin, send_sem=res_sem.at[0], recv_sem=res_sem.at[1],
            device_id=(owned, me_e), device_id_type=MESH)

    corner = (owned == me_e) & (me_e == me_t)

    gather_quarter()

    @pl.when(jnp.logical_not(corner))
    def _():
        to_final().start()

    @pl.when(corner)
    def _():
        res_fin[...] = res_own[...]

    loads[2].wait()
    loads[3].wait()

    def pass_rows(peer):
        part = row_in.at[core * n + peer]
        tp_copy(ROW, part, part, partner, n + lax.div(peer, side)).start()

    half_side = side // 2
    res_half = jnp.concatenate(
        [res_all[pl.ds((core * half_side + k) * side, side)].reshape(quarter, block)
         for k in range(half_side)], axis=1)

    def dispatch(dy):
        at = pl.multiple_of(side * lax.rem(me_y + dy, side), side)
        y = jnp.dot(pick[pl.ds(pl.multiple_of(at * few_rows, side * few_rows), side * few_rows), :],
                    res_half, preferred_element_type=F32)
        y = y.reshape(side, few_rows, half_side * block)
        row_out[pl.ds(at, side)] = jnp.concatenate(
            [y[:, :, k * block:(k + 1) * block] for k in range(half_side)], axis=1).astype(BF16)
        for dx in far_first:
            if dy or dx:
                peer, spot = ep_at(dy, dx), core * n + me_e
                ep_copy(ROW, row_out.at[peer], row_in.at[spot], peer, me_e).start()

    for dy in far_first:
        dispatch(dy)
    row_in[core * n + me_e] = row_out[me_e]
    pass_rows(me_e)

    wbr_wide[...] = wbr[...].astype(F32)
    lines = block // 128
    squares = [jnp.zeros((rows, 1), F32)] * side
    branches = [jnp.zeros((rows, 1), F32)] * side
    for k in range(side):
        j = side * me_y + k
        gain_f = fgain[:, pl.ds(pl.multiple_of(j * block, block), block)]
        gain_b = gain_f * jnp.concatenate(
            [wbr_wide[pl.ds(j * lines + i, 1), :] for i in range(lines)], axis=1)
        for g in range(side):
            r = res_all[k * side + g].astype(F32)
            squares[g] = squares[g] + jnp.sum(r * r, axis=1, keepdims=True)
            branches[g] = branches[g] + jnp.sum(r * gain_b, axis=1, keepdims=True)
            x_cat[pl.ds(g * rows, rows), k * block:(k + 1) * block] = (r * gain_f).astype(BF16)
    for g in range(side):
        sta_out[g] = jnp.where(iota((8, 128), 0) == 0, to_row(squares[g], 128), to_row(branches[g], 128))
    to_y_peers(STA, lambda y: sta_out.at[y], sta_in.at[me_y])

    for part, (first, many) in enumerate(PARTS):
        far(FAR, dgu_all, me_x, along_x, first, many, part, "wait")
    weights = dgu_all[...].reshape(side * block, 2 * hid_d)
    x = x_cat[...]
    for k in range(2 * hid_d // block):
        y = jnp.dot(x, weights[:, k * block:(k + 1) * block], preferred_element_type=F32)
        den_part[:, :, k * block:(k + 1) * block] = y.astype(BF16).reshape(side, rows, block)
    to_y_peers(DEN, lambda y: den_part.at[y], den_in.at[me_y])

    loads[19].wait()
    loads[20].wait()

    deep = half_side * block

    def expert_in(y, half, ss):
        x = row_in[pl.ds(half * n + y * side, side)].astype(F32)
        x = jnp.concatenate(
            [x[:, k * few_rows:(k + 1) * few_rows].reshape(cap_rows, block) for k in range(half_side)], axis=1)
        at = pl.multiple_of(y * side * block + half * deep, deep)
        xg = (x * fgain[:, pl.ds(at, deep)]).astype(BF16)
        gu_acc[:, pl.ds(0, hid_e)] += jnp.dot(xg, eg[pl.ds(at, deep), :], preferred_element_type=F32)
        gu_acc[:, pl.ds(hid_e, hid_e)] += jnp.dot(xg, eu[pl.ds(at, deep), :], preferred_element_type=F32)
        return ss + jnp.sum(x * x, axis=1, keepdims=True)

    def expert_first(d, ss):
        y = lax.rem(me_y + side - d, side)

        def one(k, _):
            peer = side * y + lax.rem(me_x + k, side)
            spot = core * n + peer

            @pl.when(peer != me_e)
            def _():
                ep_copy(ROW, row_in.at[spot], row_in.at[spot], peer, peer).wait_recv()
                pass_rows(peer)

            return 0

        lax.fori_loop(0, side, one, 0)
        return expert_in(y, core, ss)

    def expert_second(d, ss):
        y = lax.rem(me_y + side - d, side)

        part = row_in.at[pl.ds((1 - core) * n + side * y, side)]
        tp_copy(ROW, part, part, partner, n + y).wait_recv()
        return expert_in(y, 1 - core, ss)

    gu_acc[...] = jnp.zeros_like(gu_acc)
    ss = expert_first(0, jnp.zeros((cap_rows, 1), F32))
    ss = loop(1, side, lambda d, ss: expert_second(d - 1, expert_first(d, ss)), ss)
    ss = expert_second(side - 1, ss)
    row_scale = lax.rsqrt(ss / width + EPS)
    g = gu_acc[:, :hid_e] * row_scale
    u = gu_acc[:, hid_e:] * row_scale
    hidden_e[...] = (g / (1.0 + jnp.exp(-g)) * u).astype(BF16)
    loads[21].wait()

    def expert_out(at):
        return jnp.dot(hidden_e[...], ed[:, pl.ds(pl.multiple_of(at * block, block), block)],
                       preferred_element_type=F32).astype(BF16)

    routed_sum = sum_over_tp(
        EXP_PAIR, EXP, exp_part, exp_pair, exp_sum, exp_in, expert_out)

    await_blocks(STA, sta_in.at[few])
    sums = others(me_y, side, sta_in, sta_out[me_y])
    dense_scale = lax.rsqrt(to_column(sums[0:1, :], rows) / width + EPS)
    branch = jax.nn.sigmoid(to_column(sums[1:2, :], rows) * dense_scale)
    await_blocks(DEN, den_in.at[few])
    y = others(me_y, side, den_in, den_part[me_y].astype(F32)) * dense_scale
    g, u = y[:, :hid_d], y[:, hid_d:]
    hid_all[me_x] = (g / (1.0 + jnp.exp(-g)) * u * branch).astype(BF16)

    def spread_hidden(d, _):
        over(along_x(d), me_t, HID, hid_all.at[me_x], hid_all.at[me_x], me_x).start()
        return 0

    lax.fori_loop(1, side, spread_hidden, 0)

    far(FAR_DOWN, dd_all, me_y, along_y, 0, hid_d, 0, "wait")

    def hidden_of(d, _):
        x = lax.rem(me_x + side - d, side)
        over(along_x(-d), me_t, HID, hid_all.at[x], hid_all.at[x], x).wait_recv()
        return 0

    lax.fori_loop(1, side, hidden_of, 0)
    x = hid_all[...].reshape(quarter, hid_d)
    for k in range(side):
        y = jnp.dot(x, dd_all[k], preferred_element_type=F32)
        dwn_part[pl.ds(k * side, side)] = y.astype(BF16).reshape(side, rows, block)
    end_core = lax.rem(me_x, 2)
    home = lax.rem(me_t, side) == me_x

    @pl.when(core != end_core)
    def _():
        tp_copy(DWN_PAIR, dwn_part, dwn_pair, partner, 0).start()

    @pl.when(core == end_core)
    def _():
        tp_copy(DWN_PAIR, dwn_pair, dwn_pair, partner, 0).wait_recv()
        for dx in far_first:
            def to_end(c, _):
                x = lax.rem(me_x + dx, side)
                k = side * c + x
                dwn_sum[k] = (dwn_part[k].astype(F32) + dwn_pair[k].astype(F32)).astype(BF16)
                z = 2 * c + lax.div(me_x, 2)
                here = (x == me_x) & (z == me_z)

                @pl.when(jnp.logical_not(here))
                def _():
                    over(side * me_y + x, 2 * z + core, DWN, dwn_sum.at[k], dwn_in.at[me_z], 0).start()

                @pl.when(here)
                def _():
                    dwn_in[me_z] = dwn_sum[k]

                return 0

            lax.fori_loop(0, side, to_end, 0)

    y = summed_over_tp(EXP, exp_in, routed_sum)
    spot, col = iota((n * SLOT, cap_rows), 0), iota((n * SLOT, cap_rows), 1)
    within = jnp.bitwise_and(spot, SLOT - 1)
    shift = side.bit_length() - 1
    from_e = jnp.right_shift(spot, SLOT.bit_length() - 1)
    source = few_rows * jnp.bitwise_and(from_e, side - 1) + CAP * jnp.right_shift(from_e, shift) + within
    spread = jnp.where((source == col) & (within < CAP), 1.0, 0.0).astype(BF16)
    ret_out[...] = jnp.dot(
        spread, y.astype(BF16), preferred_element_type=F32).reshape(n, SLOT, block).astype(BF16)

    to_ep_peers(RET, lambda peer: ret_out.at[peer], ret_in.at[me_e])
    ret_in[me_e] = ret_out[me_e]

    await_blocks(RET, ret_in.at[rest])

    @pl.when(jnp.logical_not(corner))
    def _():
        to_final().wait()

    routed = jnp.dot(ret_w[...], ret_in[...].astype(F32).reshape(n * SLOT, block), precision=HIGHEST,
                     preferred_element_type=F32)
    known = res_fin[...].astype(F32) + routed

    @pl.when(home)
    def _():
        await_blocks(DWN, dwn_in.at[pl.ds(0, chips - 1)])

    @pl.when(jnp.logical_not(home))
    def _():
        await_blocks(DWN, dwn_in)

    y = others(me_z, chips, dwn_in, dwn_in[me_z].astype(F32))
    out_own[...] = (known + y).astype(BF16)

    def columns(j):
        return out.at[:, pl.ds(pl.multiple_of(j * block, block), block)]

    give_over_tp(OUT, out_own, columns)
    out[:, pl.ds(pl.multiple_of(me_t * block, block), block)] = out_own[...]
    pass_over_tp(OUT, columns)
    take_over_tp(OUT, out.at[:, pl.ds(0, chips * block)])
    sent(ep_copy, TOK, tok_all.at[rest])
    sent(ep_copy, KEY, key_all.at[few])
    sent(ep_copy, QKV, qkv_part.at[rest])
    some = pl.ds(0, chips - 1)

    @pl.when(owned != me_e)
    def _():
        sent(ep_copy, MIX, mix_in)

    @pl.when(owned == me_e)
    def _():
        sent(ep_copy, MIX, mix_in.at[:, pl.ds(0, (n - 1) * head)])

    sent(tp_copy, PROJ, proj_all.at[rest])
    sent(ep_copy, ROW, row_in.at[pl.ds(0, 2 * n - 1)])
    sent(ep_copy, STA, sta_out.at[few])
    sent(ep_copy, DEN, den_part.at[few])
    sent(ep_copy, HID, hid_all.at[few])
    for phase, buffer, rows_of in (
        (NEAR, dgu_all, block), (FAR, dgu_all, block // 2),
        (NEAR_DOWN, dd_all, hid_d), (FAR_DOWN, dd_all, hid_d // 2)):
        sent(ep_copy, phase, buffer.at[pl.ds(0, 2), pl.ds(0, rows_of), :])
    sent(tp_copy, EXP_PAIR, exp_pair)
    sent(tp_copy, EXP, exp_sum.at[some])
    sent(ep_copy, RET, ret_out.at[rest])
    sent(tp_copy, OUT, tok_all.at[rest])

    @pl.when(core != end_core)
    def _():
        sent(tp_copy, DWN_PAIR, dwn_part)

    @pl.when(home)
    def _():
        sent(ep_copy, DWN, dwn_sum.at[rest])

    @pl.when((core == end_core) & jnp.logical_not(home))
    def _():
        sent(ep_copy, DWN, dwn_sum)

    own_column = lax.rem(owned, side) == me_x

    @pl.when(jnp.logical_not(own_column))
    def _():
        sent(ep_copy, RES, res_all)

    @pl.when(own_column)
    def _():
        sent(ep_copy, RES, res_all.at[rest])


def put_out(*refs):
    *arrays, sem = refs
    copies = [pltpu.make_async_copy(arrays[k], arrays[4 + k], sem.at[k]) for k in range(4)]
    for copy in copies:
        copy.start()
    for copy in copies:
        copy.wait()


def on_device(
    n, tokens, state_matrix, state_norm, state_max, mixer_gain, w_query, w_key, w_value, w_outgate,
    w_ingate, w_forget, forget_bias, w_proj, ffn_gain, w_branch, routes, route_weight,
    expert_gate, expert_up, expert_down, dense_gate, dense_up, dense_down,
):
    rows, width = tokens.shape
    head = state_norm.shape[-1]
    block = width // n
    hid_e, hid_d = expert_gate.shape[2], dense_gate.shape[1]
    cap_rows = CAP * n
    args = (
        tokens,
        state_matrix.reshape(rows, head, head),
        state_norm.reshape(rows, head),
        state_max.T,
        mixer_gain.reshape(1, width),
        w_query, w_key, w_value, w_outgate,
        w_ingate.T, w_forget.T,
        forget_bias.reshape(1, n),
        w_proj,
        ffn_gain.reshape(1, width),
        w_branch.reshape(width // 128, 128),
        routes.T, route_weight.T,
        expert_gate.reshape(width, hid_e), expert_up.reshape(width, hid_e),
        expert_down.reshape(hid_e, width),
        dense_gate, dense_up, dense_down,
    )
    vm = pltpu.VMEM
    dma = pltpu.SemaphoreType.DMA
    few_rows, side = CAP * math.isqrt(n), math.isqrt(n)

    def hier(tall):
        return [vm((n, tall, block), BF16)] + [vm((n // 2, tall, block), BF16)] * 3

    scratch = [
        vm((rows, width), BF16), vm((rows, head, head), F32), vm((rows, head), F32), vm((1, rows), F32),
        vm((1, width), F32), vm((block, 4 * head), BF16), vm((2 * n, width), BF16), vm((1, n), F32),
        vm((n, head, block), BF16), vm((1, width), F32), vm((width // 128, 128), BF16), vm((2, rows), jnp.int32),
        vm((2, rows), F32), vm((width, hid_e), BF16), vm((width, hid_e), BF16), vm((hid_e, width), BF16),
        vm((side, block, 2 * hid_d), BF16), vm((side, hid_d, block), BF16),
        vm((n, rows, block), BF16), vm((side, rows, 128), BF16),
        vm((n, rows, 4 * head), BF16), vm((n, rows, 4 * head), BF16),
        vm((rows, head), BF16), vm((rows, n * head), BF16),
        vm((rows, block), BF16), vm((n, rows, block), BF16), vm((rows, block), BF16),
        vm((n, few_rows * side // 2, block), BF16), vm((2 * n, few_rows * side // 2, block), BF16),
        vm((side, 8, 128), F32), vm((side, 8, 128), F32),
        vm((side, rows, 2 * hid_d), BF16), vm((side, rows, 2 * hid_d), BF16),
        vm((side, rows, hid_d), BF16), *[vm((n, rows, block), BF16)] * 3, vm((n // 2, rows, block), BF16),
        *hier(cap_rows),
        vm((n, SLOT, block), BF16), vm((n, SLOT, block), BF16),
        vm((rows, block), BF16),
        vm((width // 128, 128), F32),
        vm((n * few_rows, side * rows), BF16), vm((side * rows, side * block), BF16), vm((cap_rows, hid_e), BF16), vm((cap_rows, 2 * hid_e), F32), vm((rows, 2 * n), F32),
        vm((head, rows), F32), vm((head, rows), F32), vm((rows, head), F32), vm((rows, head), F32),
        vm((rows, head), F32), vm((rows, n * SLOT), F32),
        dma((len(args),)), dma((PHASES,)), dma((landing_spots(n)[1],)), dma((2,)),
    ]
    any_space = pl.BlockSpec(memory_space=pl.ANY)
    layer_out, new_matrix, new_norm, new_max = pl.pallas_call(
        functools.partial(layer_kernel, n),
        out_shape=(
            vm((rows, width), BF16), vm((rows, head, head), F32), vm((rows, head), F32), vm((1, rows), F32),
        ),
        in_specs=[any_space] * len(args),
        out_specs=[pl.BlockSpec(memory_space=vm)] * 4,
        scratch_shapes=scratch,
        compiler_params=pltpu.CompilerParams(
            collective_id=0, has_side_effects=True, vmem_limit_bytes=56 * 1024 * 1024),
        name="layer",
    )(*args)
    results = (layer_out, new_matrix, new_norm, new_max)
    results = tuple(pltpu.with_memory_space_constraint(r, vm) for r in results)
    layer_out, new_matrix, new_norm, new_max = pl.pallas_call(
        put_out,
        out_shape=tuple(jax.ShapeDtypeStruct(r.shape, r.dtype) for r in results),
        in_specs=[pl.BlockSpec(memory_space=vm)] * 4,
        out_specs=[any_space] * 4,
        scratch_shapes=[dma((4,))],
        name="put_out",
    )(*results)
    return (layer_out, new_matrix.reshape(rows, 1, head, head), new_norm.reshape(rows, 1, head), new_max.T)


def solution(mesh):
    n = mesh.shape["ep"]
    in_specs = (
        P("ep", None),
        P("ep", "tp", None, None),
        P("ep", "tp", None),
        P("ep", "tp"),
        P(),
        P("ep", "tp"),
        P("ep", "tp"),
        P("ep", "tp"),
        P("ep", "tp"),
        P(),
        P(),
        P(),
        P("tp", "ep"),
        P(),
        P(),
        P("ep", None),
        P("ep", None),
        P("ep", None, "tp"),
        P("ep", None, "tp"),
        P("ep", "tp", None),
        P("ep", "tp"),
        P("ep", "tp"),
        P("tp", "ep"),
    )
    out_specs = (P("ep", None), P("ep", "tp", None, None), P("ep", "tp", None), P("ep", "tp"))
    return jax.shard_map(
        functools.partial(on_device, n), mesh=mesh, in_specs=in_specs, out_specs=out_specs,
        check_vma=False)
```
